256 devices in a mesh: sp: 64 (over z, y, core), tp: 4 (over x).
Axes of the slice: x: 4, y: 4, z: 8, core: 2. Of those that a mesh axis runs over, the one named last changes fastest.
Arguments:
- queries: bfloat16 [8192, 1280], P('sp', 'tp'), may hold values from -4000 to 4000
- latents: bfloat16 [8192, 512], P('sp'), may hold values from -6 to 6
- shared_key: bfloat16 [8192, 64], P('sp'), may hold values from -4 to 4
- expand_weight: bfloat16 [512, 1536], P(None, 'tp'), may hold values from -0.25 to 0.25
- residual: bfloat16 [8192, 2048], P('sp'), may hold values from -3 to 3
- out_weight: bfloat16 [768, 2048], replicated, may hold values from -0.21875 to 0.21875
- norm_gain: bfloat16 [2048], replicated, may hold values from 0.099609375 to 1.8984375
- gate_weight: bfloat16 [2048, 3072], P('sp', 'tp'), may hold values from -0.125 to 0.125
- value_weight: bfloat16 [2048, 3072], P('sp', 'tp'), may hold values from -0.125 to 0.125
- conv_weight: bfloat16 [3, 3072], P(None, 'tp'), may hold values from -3.5 to 3.5
- down_weight: bfloat16 [3072, 2048], P('tp', 'sp'), may hold values from -0.109375 to 0.109375
Outputs:
- output: bfloat16 [8192, 2048], P(('sp', 'tp'))
The draws below stay inside these ranges and needn't reach their ends.
All inputs are finite; a program needn't handle non-finite values.
Results may differ from the reference program's by a relative error of at most 0.018.
Values may be sent and summed in bfloat16 or wider, within the bound.
A program may use at most 128 MiB of HBM per device.

```python
import jax
import jax.numpy as jnp
from jax import lax

D = 2048
HEADS = 4
NOPE_A = 128
VAL_A = 128
NOPE_B = 64
VAL_B = 64
ROPE = 64
RANK = 512
FF = 3072
CONV = 3
TOK_DEV = 128
TOKENS = 8192


def shared_rows(key):
    drawn = jax.random.normal(jax.random.fold_in(key, 11), (TOKENS, ROPE), jnp.float32)
    return jnp.clip(drawn, -4.0, 4.0).astype(jnp.float32)


def draw_shared_key(key, part):
    return shared_rows(key).reshape(TOKENS, ROPE).astype(jnp.bfloat16)


def draw_queries(key, part):
    q_width = NOPE_A + NOPE_B + 2 * ROPE
    base_draw = jnp.clip(3.0 * jax.random.normal(jax.random.fold_in(key, 23), (TOKENS, HEADS, q_width), jnp.float32), -18.0, 18.0)
    return jnp.clip(base_draw, -4000.0, 4000.0).reshape(TOKENS, HEADS * q_width).astype(jnp.bfloat16)


def steps_of(own_key, extent, pieces, low, high):
    gain, own = 1.0, jax.random.fold_in(own_key, 6)
    for dim, parts in pieces:
        heights = jnp.exp(jax.random.uniform(jax.random.fold_in(own, dim), (parts,), jnp.float32, low / len(pieces), high / len(pieces)))
        gain = gain * jnp.repeat(heights, extent[dim] // parts).reshape([-1 if axis == dim else 1 for axis in range(len(extent))])
    return gain


def noise(stream_key, shape, deviation, limit, pieces=(), held_as=jnp.bfloat16):
    array = jax.random.normal(stream_key, shape, jnp.float32) * deviation
    if len(pieces) > 0:
        array = steps_of(stream_key, shape, pieces, -0.22, 0.18) * array
    return jnp.clip(array, min=-limit, max=limit).astype(held_as)


def setup_inputs(seed: int = 0) -> dict:
    key_of = jax.random.split(jax.random.key(seed), 12)
    return {
        "queries": draw_queries(jax.random.fold_in(key_of[11], 71), 0),
        "latents": noise(key_of[1], (TOKENS, RANK), 1.0, 6.0, ((0, 64),)),
        "shared_key": draw_shared_key(jax.random.fold_in(key_of[11], 71), 0),
        "expand_weight": noise(key_of[3], (RANK, HEADS * (NOPE_A + VAL_A + NOPE_B + VAL_B)), RANK ** -0.5, 0.25, ((1, 4),)),
        "residual": noise(key_of[4], (TOKENS, D), 0.5, 3.0, ((0, 64),)),
        "out_weight": noise(key_of[5], (HEADS * (VAL_A + VAL_B), D), (HEADS * (VAL_A + VAL_B)) ** -0.5, 0.21875),
        "norm_gain": jnp.clip(1.0 + 0.18 * jax.random.normal(key_of[6], (D,), jnp.float32), 0.099609375, 1.8984375).astype(jnp.bfloat16),
        "gate_weight": noise(key_of[7], (D, FF), D ** -0.5, 0.125, ((0, 64), (1, 4))),
        "value_weight": noise(key_of[8], (D, FF), D ** -0.5, 0.125, ((0, 64), (1, 4))),
        "conv_weight": noise(key_of[9], (CONV, FF), CONV ** -0.5, 3.5, ((1, 4),)),
        "down_weight": noise(key_of[10], (FF, D), FF ** -0.5, 0.109375, ((0, 4), (1, 64))),
    }


def tables(positions, width):
    half_width = width // 2
    frequency = 10000.0 ** (-jnp.arange(half_width, dtype=jnp.float32) / half_width)
    angles = positions.astype(jnp.float32)[:, None] * frequency[None, :]
    return (jnp.cos(angles), jnp.sin(angles))

def rotate(vectors, cos_table, sine_table):
    half_width = vectors.shape[-1] // 2
    first_half = vectors[:, :half_width].astype(jnp.float32)
    second_half = vectors[:, half_width:].astype(jnp.float32)
    turned = jnp.concatenate([first_half * cos_table - second_half * sine_table, second_half * cos_table + first_half * sine_table], axis=1)
    return turned.astype(jnp.bfloat16)

def attend_head(q_content, q_turned, k_content, k_turned, values, score_scale):
    tokens = q_content.shape[0]
    blocks = tokens // TOK_DEV

    def one_block(block_index):
        first_row = (block_index * TOK_DEV).astype(jnp.int32)
        content = lax.dynamic_slice_in_dim(q_content, first_row, TOK_DEV, 0)
        rotary = lax.dynamic_slice_in_dim(q_turned, first_row, TOK_DEV, 0)
        scores = (jnp.dot(content, k_content.T, preferred_element_type=jnp.float32) + jnp.dot(rotary, k_turned.T, preferred_element_type=jnp.float32)) * score_scale
        row_max = lax.optimization_barrier(jnp.max(scores, axis=1, keepdims=True))
        weights = jnp.exp(scores - row_max)
        row_sum = lax.optimization_barrier(jnp.sum(weights, axis=1, keepdims=True))
        weighted = jnp.dot(weights.astype(jnp.bfloat16), values, preferred_element_type=jnp.float32)
        return (weighted / row_sum).astype(jnp.bfloat16)
    result = lax.map(one_block, jnp.arange(blocks, dtype=jnp.int32))
    return result.reshape(tokens, values.shape[1])

def reference(queries, latents, shared_key, expand_weight, residual, out_weight, norm_gain, gate_weight, value_weight, conv_weight, down_weight):
    tokens = queries.shape[0]
    q_width = NOPE_A + NOPE_B + 2 * ROPE
    kv_width = NOPE_A + VAL_A + NOPE_B + VAL_B
    cos_table, sine_table = tables(jnp.arange(tokens, dtype=jnp.int32), ROPE)
    key_turned = rotate(shared_key, cos_table, sine_table)
    expanded = jnp.dot(latents, expand_weight, preferred_element_type=jnp.float32).astype(jnp.bfloat16)
    scale_wide = (NOPE_A + ROPE) ** (-0.5)
    scale_narrow = (NOPE_B + ROPE) ** (-0.5)
    outputs = []
    for pair_index in range(HEADS):
        q_base = pair_index * q_width
        kv_base = pair_index * kv_width
        wide_content = queries[:, q_base:q_base + NOPE_A]
        narrow_content = queries[:, q_base + NOPE_A:q_base + NOPE_A + NOPE_B]
        rotary_base = q_base + NOPE_A + NOPE_B
        wide_turned = rotate(queries[:, rotary_base:rotary_base + ROPE], cos_table, sine_table)
        narrow_turned = rotate(queries[:, rotary_base + ROPE:rotary_base + 2 * ROPE], cos_table, sine_table)
        wide_keys = expanded[:, kv_base:kv_base + NOPE_A]
        wide_values = expanded[:, kv_base + NOPE_A:kv_base + NOPE_A + VAL_A]
        narrow_base = kv_base + NOPE_A + VAL_A
        narrow_keys = expanded[:, narrow_base:narrow_base + NOPE_B]
        narrow_values = expanded[:, narrow_base + NOPE_B:narrow_base + NOPE_B + VAL_B]
        outputs.append(attend_head(wide_content, wide_turned, wide_keys, key_turned, wide_values, scale_wide))
        outputs.append(attend_head(narrow_content, narrow_turned, narrow_keys, key_turned, narrow_values, scale_narrow))
    attended = jnp.concatenate(outputs, axis=1)
    projected = jnp.dot(attended, out_weight, preferred_element_type=jnp.float32)
    stream = (residual.astype(jnp.float32) + projected).astype(jnp.bfloat16)
    stream_f = stream.astype(jnp.float32)
    scaled = stream_f * lax.rsqrt(lax.optimization_barrier(jnp.mean(stream_f * stream_f, axis=1, keepdims=True)) + 1e-06)
    normed = (scaled * norm_gain.astype(jnp.float32)).astype(jnp.bfloat16)
    gate_pre = jnp.dot(normed, gate_weight, preferred_element_type=jnp.float32).astype(jnp.bfloat16)
    value_pre = jnp.dot(normed, value_weight, preferred_element_type=jnp.float32).astype(jnp.bfloat16)
    reach = CONV // 2
    padded = jnp.pad(gate_pre, ((reach, reach), (0, 0)))
    mixed_gate = jnp.zeros(gate_pre.shape, jnp.float32)
    for tap in range(CONV):
        mixed_gate = mixed_gate + padded[tap:tap + tokens].astype(jnp.float32) * conv_weight[tap].astype(jnp.float32)
    active = (jax.nn.silu(mixed_gate) * value_pre.astype(jnp.float32)).astype(jnp.bfloat16)
    down = jnp.dot(active, down_weight, preferred_element_type=jnp.float32)
    return (stream.astype(jnp.float32) + down).astype(jnp.bfloat16)
```

```python
import functools

import jax
import jax.numpy as jnp
from jax import lax
from jax.experimental import pallas as pl
from jax.experimental.pallas import tpu as pltpu
from jax.sharding import Mesh
from jax.sharding import PartitionSpec as P

NOPE_A = 128
VAL_A = 128
NOPE_B = 64
VAL_B = 64
ROPE = 64
SP = ("sp_0", "sp_1", "sp_2")
SP_TP = ("sp_0", "sp_1", "sp_2", "tp")
NZ, NY, NX = 8, 4, 4
TOK = 128
D = 2048
FFD = 768
MESH = pl.DeviceIdType.MESH
LOG2E = 1.4426950408889634
F32 = jnp.float32
BF = jnp.bfloat16


def tables(positions, width):
    half_width = width // 2
    frequency = 10000.0 ** (-jnp.arange(half_width, dtype=jnp.float32) / half_width)
    angles = positions.astype(jnp.float32)[:, None] * frequency[None, :]
    return (jnp.cos(angles), jnp.sin(angles))


def rotate(vectors, cos_table, sine_table):
    half_width = vectors.shape[-1] // 2
    first_half = vectors[:, :half_width].astype(jnp.float32)
    second_half = vectors[:, half_width:].astype(jnp.float32)
    turned = jnp.concatenate(
        [
            first_half * cos_table - second_half * sine_table,
            second_half * cos_table + first_half * sine_table,
        ],
        axis=1,
    )
    return turned.astype(jnp.bfloat16)


def split3(v):
    hi = v.astype(BF).astype(F32)
    rest = v - hi
    mid = rest.astype(BF).astype(F32)
    return hi, mid, rest - mid


def kernel(
    q_own, kv_own, gv_own, dn_own, gain, conv_w, resid_hbm, ow_hbm,
    out_ref,
    kvb, qb, gv, dn, ow, resid, s_ref, macc, mrow, accw, accn,
    part, ob, att, stream, normed, gate, value, hp, hn, act, fp, fr,
    kvz_s, kvz_r, q_s, q_r, gvz_s, gvz_r, gvy_s, gvy_r, dny_s, dny_r, dnz_s, dnz_r,
    pk_s, pk_r, pg_s, pg_r, pd_s, pd_r, o_s, o_r, x_s, x_r, h_s, h_r, f_s, f_r, loc,
):
    z = lax.axis_index("sp_0")
    y = lax.axis_index("sp_1")
    c = lax.axis_index("sp_2")
    x = lax.axis_index("tp")
    other = 1 - c

    def zat(k):
        return lax.rem(z + (k + NZ), NZ)

    def yat(k):
        return lax.rem(y + (k + NY), NY)

    def xat(k):
        return lax.rem(x + (k + NX), NX)

    right_z, left_z = {"sp_0": zat(1)}, {"sp_0": zat(-1)}
    right_y, left_y = {"sp_1": yat(1)}, {"sp_1": yat(-1)}
    partner = {"sp_2": other}
    place = (z * NY + y) * 2 + c
    after = lax.rem(place + 1, 64)
    before = lax.rem(place + 63, 64)

    def device_of(i):
        return {"sp_0": i // 8, "sp_1": lax.rem(i // 2, 4), "sp_2": lax.rem(i, 2)}

    def send(src, dst, ssem, rsem, dev):
        pltpu.make_async_remote_copy(
            src_ref=src, dst_ref=dst, send_sem=ssem, recv_sem=rsem, device_id=dev, device_id_type=MESH
        ).start()

    def wait_recv(ref, sem):
        pltpu.make_async_remote_copy(
            src_ref=ref, dst_ref=ref, send_sem=sem, recv_sem=sem, device_id=partner, device_id_type=MESH
        ).wait_recv()

    def wait_send(ref, sem):
        pltpu.make_async_remote_copy(
            src_ref=ref, dst_ref=ref, send_sem=sem, recv_sem=sem, device_id=partner, device_id_type=MESH
        ).wait_send()

    load_ow = pltpu.make_async_copy(ow_hbm, ow, loc.at[0])
    load_ow.start()
    load_res = pltpu.make_async_copy(resid_hbm, resid, loc.at[1])
    load_res.start()

    barrier = pltpu.get_barrier_semaphore()
    greeted = [
        partner, right_z, left_z, right_y, left_y, {"sp_1": yat(2)},
        {"tp": xat(1)}, {"tp": xat(2)}, {"tp": xat(3)}, device_of(after), device_of(before),
    ]
    for dev in greeted:
        pl.semaphore_signal(barrier, inc=1, device_id=dev, device_id_type=MESH)
    pl.semaphore_wait(barrier, len(greeted))

    send(kv_own, kvb.at[z, c], kvz_s, kvz_r.at[0, 0], right_z)
    send(kv_own, kvb.at[z, c], kvz_s, kvz_r.at[1, 0], left_z)
    send(q_own, qb.at[y], q_s, q_r.at[0, 0], right_y)
    send(q_own, qb.at[y], q_s, q_r.at[1, 0], left_y)
    send(gv_own, gv.at[z, y, c], gvz_s, gvz_r.at[0, 0], right_z)
    send(gv_own, gv.at[z, y, c], gvz_s, gvz_r.at[1, 0], left_z)
    send(dn_own, dn.at[z, y, c], dny_s, dny_r.at[0, 0], right_y)
    send(dn_own, dn.at[z, y, c], dny_s, dny_r.at[1, 0], left_y)
    send(kv_own, kvb.at[z, c], pk_s, pk_r, partner)
    send(gv_own, gv.at[z, y, c], gvy_s, gvy_r.at[0, 0, 0], right_y)
    send(gv_own, gv.at[z, y, c], gvy_s, gvy_r.at[1, 0, 0], left_y)
    send(gv_own, gv.at[z, y, c], pg_s, pg_r, partner)
    kvb[z, c] = kv_own[...]
    qb[y] = q_own[...]
    gv[z, y, c] = gv_own[...]
    dn[z, y, c] = dn_own[...]

    offsets = [0, -1, 1, -2, 2, -3, 3, 4]

    def kvz(s):
        lo, hi = zat(-s), zat(s)
        if s < 4:
            wait_recv(kvb.at[lo, c], kvz_r.at[0, s - 1])
            if s < 3:
                send(kvb.at[lo, c], kvb.at[lo, c], kvz_s, kvz_r.at[0, s], right_z)
            else:
                send(kvb.at[lo, c, pl.ds(0, 64)], kvb.at[lo, c, pl.ds(0, 64)], kvz_s, kvz_r.at[0, s], right_z)
            wait_recv(kvb.at[hi, c], kvz_r.at[1, s - 1])
            if s < 3:
                send(kvb.at[hi, c], kvb.at[hi, c], kvz_s, kvz_r.at[1, s], left_z)
            else:
                send(kvb.at[hi, c, pl.ds(64, 64)], kvb.at[hi, c, pl.ds(64, 64)], kvz_s, kvz_r.at[1, s], left_z)
            send(kvb.at[lo, c], kvb.at[lo, c], pk_s, pk_r, partner)
            send(kvb.at[hi, c], kvb.at[hi, c], pk_s, pk_r, partner)
        else:
            wait_recv(kvb.at[lo, c, pl.ds(0, 64)], kvz_r.at[0, 3])
            wait_recv(kvb.at[lo, c, pl.ds(64, 64)], kvz_r.at[1, 3])
            send(kvb.at[lo, c], kvb.at[lo, c], pk_s, pk_r, partner)

    def q_relay(s):
        a, b, far = yat(-1), yat(1), yat(2)
        if s == 1:
            wait_recv(qb.at[a], q_r.at[0, 0])
            send(qb.at[a, pl.ds(0, 64)], qb.at[a, pl.ds(0, 64)], q_s, q_r.at[0, 1], right_y)
            wait_recv(qb.at[b], q_r.at[1, 0])
            send(qb.at[b, pl.ds(64, 64)], qb.at[b, pl.ds(64, 64)], q_s, q_r.at[1, 1], left_y)
        else:
            wait_recv(qb.at[far, pl.ds(0, 64)], q_r.at[0, 1])
            wait_recv(qb.at[far, pl.ds(64, 64)], q_r.at[1, 1])

    def gv_out(zz, j):
        block = gv.at[zz, y, c]
        send(block, block, gvy_s, gvy_r.at[0, 0, j], right_y)
        send(block, block, gvy_s, gvy_r.at[1, 0, j], left_y)
        send(block, block, pg_s, pg_r, partner)

    def gvz(s):
        lo, hi = zat(-s), zat(s)
        if s < 4:
            wait_recv(gv.at[lo, y, c], gvz_r.at[0, s - 1])
            src = gv.at[lo, y, c] if s < 3 else gv.at[lo, y, c, pl.ds(0, 32)]
            send(src, src, gvz_s, gvz_r.at[0, s], right_z)
            wait_recv(gv.at[hi, y, c], gvz_r.at[1, s - 1])
            src = gv.at[hi, y, c] if s < 3 else gv.at[hi, y, c, pl.ds(32, 32)]
            send(src, src, gvz_s, gvz_r.at[1, s], left_z)
            gv_out(lo, 2 * s - 1)
            gv_out(hi, 2 * s)
        else:
            wait_recv(gv.at[lo, y, c, pl.ds(0, 32)], gvz_r.at[0, 3])
            wait_recv(gv.at[lo, y, c, pl.ds(32, 32)], gvz_r.at[1, 3])
            gv_out(lo, 7)

    def gvy(s, j):
        zz = zat(offsets[j])
        a, b, far = yat(-1), yat(1), yat(2)
        if s == 1:
            wait_recv(gv.at[zz, a, c], gvy_r.at[0, 0, j])
            src = gv.at[zz, a, c, pl.ds(0, 32)]
            send(src, src, gvy_s, gvy_r.at[0, 1, j], right_y)
            wait_recv(gv.at[zz, b, c], gvy_r.at[1, 0, j])
            src = gv.at[zz, b, c, pl.ds(32, 32)]
            send(src, src, gvy_s, gvy_r.at[1, 1, j], left_y)
            send(gv.at[zz, a, c], gv.at[zz, a, c], pg_s, pg_r, partner)
            send(gv.at[zz, b, c], gv.at[zz, b, c], pg_s, pg_r, partner)
        else:
            wait_recv(gv.at[zz, far, c, pl.ds(0, 32)], gvy_r.at[0, 1, j])
            wait_recv(gv.at[zz, far, c, pl.ds(32, 32)], gvy_r.at[1, 1, j])
            send(gv.at[zz, far, c], gv.at[zz, far, c], pg_s, pg_r, partner)

    def dny(s):
        a, b, far = yat(-1), yat(1), yat(2)
        if s == 1:
            wait_recv(dn.at[z, a, c], dny_r.at[0, 0])
            src = dn.at[z, a, c, pl.ds(0, 16)]
            send(src, src, dny_s, dny_r.at[0, 1], right_y)
            wait_recv(dn.at[z, b, c], dny_r.at[1, 0])
            src = dn.at[z, b, c, pl.ds(16, 16)]
            send(src, src, dny_s, dny_r.at[1, 1], left_y)
        else:
            wait_recv(dn.at[z, far, c, pl.ds(0, 16)], dny_r.at[0, 1])
            wait_recv(dn.at[z, far, c, pl.ds(16, 16)], dny_r.at[1, 1])

    def dnz(s):
        lo, hi = zat(-s), zat(s)
        if s == 0:
            bundle = dn.at[z, :, c]
            send(bundle, bundle, dnz_s, dnz_r.at[0, 0], right_z)
            send(bundle, bundle, dnz_s, dnz_r.at[1, 0], left_z)
            send(bundle, bundle, pd_s, pd_r, partner)
        elif s < 4:
            wait_recv(dn.at[lo, :, c], dnz_r.at[0, s - 1])
            src = dn.at[lo, :, c] if s < 3 else dn.at[lo, pl.ds(0, 2), c]
            send(src, src, dnz_s, dnz_r.at[0, s], right_z)
            wait_recv(dn.at[hi, :, c], dnz_r.at[1, s - 1])
            src = dn.at[hi, :, c] if s < 3 else dn.at[hi, pl.ds(2, 2), c]
            send(src, src, dnz_s, dnz_r.at[1, s], left_z)
            send(dn.at[lo, :, c], dn.at[lo, :, c], pd_s, pd_r, partner)
            send(dn.at[hi, :, c], dn.at[hi, :, c], pd_s, pd_r, partner)
        else:
            wait_recv(dn.at[lo, pl.ds(0, 2), c], dnz_r.at[0, 3])
            wait_recv(dn.at[lo, pl.ds(2, 2), c], dnz_r.at[1, 3])
            send(dn.at[lo, :, c], dn.at[lo, :, c], pd_s, pd_r, partner)

    heads = (
        (0, 256, 0, 256, 256, 512, (NOPE_A + ROPE) ** (-0.5) * LOG2E, accw),
        (256, 384, 128, 256, 384, 512, (NOPE_B + ROPE) ** (-0.5) * LOG2E, accn),
    )

    def scores(head):
        q0, q1, k0, k1 = heads[head][:4]
        macc[...] = jnp.full((512, 128), -3e38, F32)

        def step(k, carry):
            qs = qb[:, :, q0:q1].reshape(512, q1 - q0)
            ks = kvb[k, :, :, k0:k1].reshape(256, k1 - k0)
            s = lax.dot_general(qs, ks, (((1,), (1,)), ((), ())), preferred_element_type=F32)
            s_ref[k] = s
            macc[...] = jnp.maximum(macc[...], jnp.maximum(s[:, :128], s[:, 128:]))
            return carry

        lax.fori_loop(0, NZ, step, 0)

    def weigh(head):
        v0, v1, factor, acc = heads[head][4:]
        m = jnp.max(macc[...], axis=1, keepdims=True)
        mrow[head] = jnp.broadcast_to(m, (512, 128))
        acc[...] = jnp.zeros(acc.shape, F32)

        def step(k, carry):
            mb = mrow[head]
            s = s_ref[k]
            p = jnp.exp2((s - jnp.concatenate([mb, mb], axis=1)) * factor).astype(BF)
            vs = kvb[k, :, :, v0:v1].reshape(256, v1 - v0)
            acc[...] += jnp.dot(p, vs, preferred_element_type=F32)
            return carry

        lax.fori_loop(0, NZ, step, 0)

    def pack():
        def step(b, carry):
            rows = pl.ds(pl.multiple_of(b * TOK, TOK), TOK)
            wide, narrow = accw[rows, :], accn[rows, :]
            lane = lax.broadcasted_iota(jnp.int32, (TOK, 128), 1)
            tile = narrow
            stats = (
                mrow[0, rows, :], mrow[1, rows, :],
                jnp.broadcast_to(wide[:, 192:193], (TOK, 128)), jnp.broadcast_to(narrow[:, 64:65], (TOK, 128)),
            )
            at = 64
            for stat in stats:
                for piece in split3(stat):
                    tile = jnp.where(lane == at, piece, tile)
                    at += 1
            tile = jnp.where(lane >= at, 0.0, tile)
            part[b, :, 0:128] = wide[:, 0:128].astype(BF)
            part[b, :, 128:256] = tile.astype(BF)
            return carry

        lax.fori_loop(0, NY, step, 0)

    def merge():
        ob[y] = part[y]

        def stat(g, at):
            t = ob[g, :, 128:256].astype(F32)
            return t[:, at : at + 1] + t[:, at + 1 : at + 2] + t[:, at + 2 : at + 3]

        for head in range(2):
            factor = heads[head][6]
            ms = [stat(g, 64 + 3 * head) for g in range(NY)]
            top = jnp.maximum(jnp.maximum(ms[0], ms[1]), jnp.maximum(ms[2], ms[3]))
            lanes = slice(0, 128) if head == 0 else slice(128, 256)
            total = jnp.zeros((TOK, 1), F32)
            value_sum = jnp.zeros((TOK, 128), F32)
            for g in range(NY):
                share = jnp.exp2((ms[g] - top) * factor)
                total = total + share * stat(g, 70 + 3 * head)
                value_sum = value_sum + share * ob[g, :, lanes].astype(F32)
            att[x, :, lanes] = (value_sum / total).astype(BF)

    kvz(1)
    q_relay(1)
    dny(1)
    gvz(1)
    gvy(1, 0)
    kvz(2)
    q_relay(2)
    dny(2)
    gvz(2)
    gvy(2, 0)
    gvy(1, 1)
    gvy(1, 2)
    kvz(3)
    gvz(3)
    dnz(0)
    kvz(4)
    gvz(4)
    wait_recv(kvb.at[:, other], pk_r)
    scores(0)
    gvy(2, 1)
    gvy(2, 2)
    gvy(1, 3)
    gvy(1, 4)
    weigh(0)
    gvy(2, 3)
    gvy(2, 4)
    gvy(1, 5)
    dnz(1)
    scores(1)
    gvy(1, 6)
    gvy(2, 5)
    weigh(1)
    pack()
    for o in (2, 1, 3):
        peer = yat(o)
        send(part.at[peer], ob.at[y], o_s, o_r.at[o - 1], {"sp_1": peer})
    gvy(1, 7)
    gvy(2, 6)
    dnz(2)
    for o in (2, 1, 3):
        wait_recv(ob.at[yat(-o)], o_r.at[o - 1])
    merge()
    for o in (2, 1, 3):
        send(att.at[x], att.at[x], x_s, x_r.at[o - 1], {"tp": xat(o)})
    gvy(2, 7)
    dnz(3)
    load_ow.wait()
    load_res.wait()
    for o in (2, 1, 3):
        wait_recv(att.at[xat(-o)], x_r.at[o - 1])

    def project(n, ss):
        cols = pl.ds(pl.multiple_of(n * 256, 256), 256)
        total = resid[:, cols].astype(F32)
        for h in range(NX):
            total = total + jnp.dot(
                att[h, :, 0:192], ow[pl.ds(h * 192, 192), cols], preferred_element_type=F32
            )
        rounded = total.astype(BF)
        stream[:, cols] = rounded
        wide = rounded.astype(F32)
        return ss + jnp.sum(wide * wide, axis=1, keepdims=True)

    ss = lax.fori_loop(0, 8, project, jnp.zeros((TOK, 1), F32))
    scale = lax.rsqrt(ss * (1.0 / D) + 1e-06)

    def norm(n, carry):
        cols = pl.ds(pl.multiple_of(n * 256, 256), 256)
        scaled = stream[:, cols].astype(F32) * scale
        normed[:, cols] = (scaled * gain[:, cols].astype(F32)).astype(BF)
        return carry

    lax.fori_loop(0, 8, norm, 0)
    dnz(4)
    wait_recv(gv.at[:, :, other], pg_r)

    def up(lo, dst):
        def step(n, carry):
            cols = pl.ds(pl.multiple_of(n * 256, 256), 256)
            w = gv[:, :, :, lo : lo + 32, cols].reshape(D, 256)
            dst[:, cols] = jnp.dot(normed[...], w, preferred_element_type=F32).astype(BF)
            return carry

        lax.fori_loop(0, 3, step, 0)

    up(0, gate)
    send(gate.at[pl.ds(112, 16)], hp, h_s.at[0], h_r.at[0], device_of(after))
    send(gate.at[pl.ds(0, 16)], hn, h_s.at[1], h_r.at[1], device_of(before))
    up(32, value)
    wait_recv(hp, h_r.at[0])
    wait_recv(hn, h_r.at[1])

    row = lax.broadcasted_iota(jnp.int32, (TOK, 256), 0)
    for n in range(3):
        cols = slice(n * 256, n * 256 + 256)
        g = gate[:, cols].astype(F32)
        first = jnp.where(place > 0, hp[:, cols].astype(F32)[15:16], 0.0)
        last = jnp.where(place < 63, hn[:, cols].astype(F32)[0:1], 0.0)
        low = jnp.where(row == 0, first, pltpu.roll(g, 1, 0))
        high = jnp.where(row == TOK - 1, last, pltpu.roll(g, TOK - 1, 0))
        cw = conv_w[:, cols].astype(F32)
        mixed = low * cw[0:1] + g * cw[1:2] + high * cw[2:3]
        silu = mixed / (1.0 + jnp.exp(-mixed))
        act[:, cols] = (silu * value[:, cols].astype(F32)).astype(BF)

    wait_recv(dn.at[:, :, other], pd_r)

    for half in range(2):

        def down(n, carry):
            w = dn[half * 4 + n].reshape(256, FFD)
            d = lax.dot_general(act[...], w, (((1,), (1,)), ((), ())), preferred_element_type=F32)
            cols = pl.ds(pl.multiple_of(n * 256, 256), 256)
            fp[half, :, :, cols] = d.astype(BF).reshape(NX, 32, 256)
            return carry

        lax.fori_loop(0, 4, down, 0)
        for o in (2, 1, 3):
            peer = xat(o)
            send(fp.at[half, peer], fr.at[half, x], f_s, f_r.at[half, o - 1], {"tp": peer})

    for half in range(2):
        cols = slice(half * 1024, half * 1024 + 1024)
        rows = pl.ds(pl.multiple_of(x * 32, 32), 32)
        total = stream[rows, cols].astype(F32) + fp[half, x].astype(F32)
        for o in (1, 3, 2):
            wait_recv(fr.at[half, xat(-o)], f_r.at[half, o - 1])
            total = total + fr[half, xat(-o)].astype(F32)
        out_ref[:, cols] = total.astype(BF)

    wait_send(kvb.at[pl.ds(0, 7), 0], kvz_s)
    wait_send(qb.at[pl.ds(0, 3)], q_s)
    wait_send(gv.at[pl.ds(0, 7), 0, 0], gvz_s)
    wait_send(gv.at[:, pl.ds(0, 3), 0], gvy_s)
    wait_send(dn.at[0, pl.ds(0, 3), 0], dny_s)
    wait_send(dn.at[pl.ds(0, 7), :, 0], dnz_s)
    wait_send(kvb.at[:, 0], pk_s)
    wait_send(gv.at[:, :, 0], pg_s)
    wait_send(dn.at[:, :, 0], pd_s)
    wait_send(part.at[pl.ds(0, 3)], o_s)
    wait_send(att.at[pl.ds(0, 3)], x_s)
    wait_send(hp, h_s.at[0])
    wait_send(hn, h_s.at[1])
    wait_send(fp.at[:, pl.ds(0, 3)], f_s)


def layer(q_own, kv_own, gv_own, dn_own, gain, conv_w, residual, out_weight):
    vmem = pl.BlockSpec(memory_space=pltpu.VMEM)
    hbm = pl.BlockSpec(memory_space=pltpu.HBM)
    dma = pltpu.SemaphoreType.DMA
    scratch = [
        pltpu.VMEM((NZ, 2, TOK, 512), BF),
        pltpu.VMEM((NY, TOK, 384), BF),
        pltpu.VMEM((NZ, NY, 2, 64, FFD), BF),
        pltpu.VMEM((NZ, NY, 2, 32, FFD), BF),
        pltpu.VMEM((768, D), BF),
        pltpu.VMEM((TOK, D), BF),
        pltpu.VMEM((NZ, 512, 256), F32),
        pltpu.VMEM((512, 128), F32),
        pltpu.VMEM((2, 512, 128), F32),
        pltpu.VMEM((512, 256), F32),
        pltpu.VMEM((512, 128), F32),
        pltpu.VMEM((NY, TOK, 256), BF),
        pltpu.VMEM((NY, TOK, 256), BF),
        pltpu.VMEM((NX, TOK, 256), BF),
        pltpu.VMEM((TOK, D), BF),
        pltpu.VMEM((TOK, D), BF),
        pltpu.VMEM((TOK, FFD), BF),
        pltpu.VMEM((TOK, FFD), BF),
        pltpu.VMEM((16, FFD), BF),
        pltpu.VMEM((16, FFD), BF),
        pltpu.VMEM((TOK, FFD), BF),
        pltpu.VMEM((2, NX, 32, 1024), BF),
        pltpu.VMEM((2, NX, 32, 1024), BF),
        dma, dma((2, 4)), dma, dma((2, 2)), dma, dma((2, 4)), dma, dma((2, 2, 8)),
        dma, dma((2, 2)), dma, dma((2, 4)),
        dma, dma, dma, dma, dma, dma, dma, dma((3,)), dma, dma((3,)), dma((2,)), dma((2,)),
        dma, dma((2, 3)), dma((2,)),
    ]
    return pl.pallas_call(
        kernel,
        out_shape=jax.ShapeDtypeStruct((32, D), BF),
        in_specs=[vmem] * 6 + [hbm] * 2,
        out_specs=vmem,
        scratch_shapes=scratch,
        compiler_params=pltpu.CompilerParams(collective_id=0, has_side_effects=True),
    )(q_own, kv_own, gv_own, dn_own, gain, conv_w, residual, out_weight)


def body(
    queries, latents, shared_key, expand_weight, residual, out_weight,
    norm_gain, gate_weight, value_weight, conv_weight, down_weight,
):
    rows = queries.shape[0]
    positions = lax.axis_index(SP) * rows + jnp.arange(rows, dtype=jnp.int32)
    cos_table, sine_table = tables(positions, ROPE)
    key_turned = rotate(shared_key, cos_table, sine_table)
    wide_turned = rotate(queries[:, 192:256], cos_table, sine_table)
    narrow_turned = rotate(queries[:, 256:320], cos_table, sine_table)
    pad = jnp.zeros((rows, 64), BF)
    q_own = jnp.concatenate([queries[:, 0:128], wide_turned, pad, narrow_turned, queries[:, 128:192]], axis=1)
    expanded = jnp.dot(latents, expand_weight, preferred_element_type=F32).astype(BF)
    kv_own = jnp.concatenate(
        [
            expanded[:, 0:128], key_turned, expanded[:, 256:320],
            expanded[:, 128:256], expanded[:, 320:384], jnp.ones((rows, 64), BF),
        ],
        axis=1,
    )
    gv_own = jnp.concatenate([gate_weight, value_weight], axis=0)
    dn_own = down_weight.T
    return layer(q_own, kv_own, gv_own, dn_own, norm_gain[None, :], conv_weight, residual, out_weight)


def solution(mesh):
    split = Mesh(mesh.devices.reshape(NZ, NY, 2, mesh.shape["tp"]), ("sp_0", "sp_1", "sp_2", "tp"))
    placed = (
        P(SP, "tp"),
        P(SP, None),
        P(SP, None),
        P(None, "tp"),
        P(SP, None),
        P(),
        P(),
        P(SP, "tp"),
        P(SP, "tp"),
        P(None, "tp"),
        P("tp", SP),
    )
    return jax.shard_map(
        body, mesh=split, in_specs=placed, out_specs=P(SP_TP, None), check_vma=False
    )
```

```python
import functools

import jax
import jax.numpy as jnp
from jax import lax
from jax.experimental import pallas as pl
from jax.experimental.pallas import tpu as pltpu
from jax.sharding import Mesh
from jax.sharding import PartitionSpec as P

NOPE_A = 128
VAL_A = 128
NOPE_B = 64
VAL_B = 64
ROPE = 64
SP = ("sp_0", "sp_1", "sp_2")
SP_TP = ("sp_0", "sp_1", "sp_2", "tp")
NZ, NY, NX = 8, 4, 4
TOK = 128
D = 2048
FFD = 768
MESH = pl.DeviceIdType.MESH
LOG2E = 1.4426950408889634
F32 = jnp.float32
BF = jnp.bfloat16


def split3(v):
    hi = v.astype(BF).astype(F32)
    rest = v - hi
    mid = rest.astype(BF).astype(F32)
    return hi, mid, rest - mid


def kernel(
    q_t, lat, key_t, ew, gate_own, value_own, dn_own, freq, gain, conv_w, resid_hbm, ow_hbm,
    out_ref,
    kvb, qb, gv, dn, ow, resid, s_ref, p_ref, macc, mrow, accw, accn,
    part, ob, att, stream, normed, gate, value, hp, hn, act, fp, fr,
    kvz_s, kvz_r, q_s, q_r, gvz_s, gvz_r, gvy_s, gvy_r, dny_s, dny_r, dnz_s, dnz_r,
    pk_s, pk_r, pg_s, pg_r, pd_s, pd_r, o_s, o_r, x_s, x_r, h_s, h_r, f_s, f_r, loc,
):
    z = lax.axis_index("sp_0")
    y = lax.axis_index("sp_1")
    c = lax.axis_index("sp_2")
    x = lax.axis_index("tp")
    other = 1 - c

    def zat(k):
        return lax.rem(z + (k + NZ), NZ)

    def yat(k):
        return lax.rem(y + (k + NY), NY)

    def xat(k):
        return lax.rem(x + (k + NX), NX)

    right_z, left_z = {"sp_0": zat(1)}, {"sp_0": zat(-1)}
    right_y, left_y = {"sp_1": yat(1)}, {"sp_1": yat(-1)}
    partner = {"sp_2": other}
    place = (z * NY + y) * 2 + c
    after = lax.rem(place + 1, 64)
    before = lax.rem(place + 63, 64)

    def device_of(i):
        return {"sp_0": i // 8, "sp_1": lax.rem(i // 2, 4), "sp_2": lax.rem(i, 2)}

    def send(src, dst, ssem, rsem, dev):
        pltpu.make_async_remote_copy(
            src_ref=src, dst_ref=dst, send_sem=ssem, recv_sem=rsem, device_id=dev, device_id_type=MESH
        ).start()

    def wait_recv(ref, sem):
        pltpu.make_async_remote_copy(
            src_ref=ref, dst_ref=ref, send_sem=sem, recv_sem=sem, device_id=partner, device_id_type=MESH
        ).wait_recv()

    def wait_send(ref, sem):
        pltpu.make_async_remote_copy(
            src_ref=ref, dst_ref=ref, send_sem=sem, recv_sem=sem, device_id=partner, device_id_type=MESH
        ).wait_send()

    load_ow = pltpu.make_async_copy(ow_hbm, ow, loc.at[0])
    load_ow.start()
    load_res = pltpu.make_async_copy(resid_hbm, resid, loc.at[1])
    load_res.start()

    gv[z, y, c, 0:32] = gate_own[...]
    gv[z, y, c, 32:64] = value_own[...]
    dn[z, y, c] = dn_own[...]

    barrier = pltpu.get_barrier_semaphore()
    greeted = [
        partner, right_z, left_z, right_y, left_y, {"sp_1": yat(2)},
        {"tp": xat(1)}, {"tp": xat(2)}, {"tp": xat(3)}, device_of(after), device_of(before),
    ]
    for dev in greeted:
        pl.semaphore_signal(barrier, inc=1, device_id=dev, device_id_type=MESH)
    pl.semaphore_wait(barrier, len(greeted))

    own = gv.at[z, y, c]
    send(own, own, gvz_s, gvz_r.at[0, 0], right_z)
    send(own, own, gvz_s, gvz_r.at[1, 0], left_z)
    send(dn.at[z, y, c], dn.at[z, y, c], dny_s, dny_r.at[0, 0], right_y)
    send(dn.at[z, y, c], dn.at[z, y, c], dny_s, dny_r.at[1, 0], left_y)
    send(own, own, gvy_s, gvy_r.at[0, 0, 0], right_y)
    send(own, own, gvy_s, gvy_r.at[1, 0, 0], left_y)
    send(own, own, pg_s, pg_r, partner)

    position = (lax.broadcasted_iota(jnp.int32, (32, TOK), 1) + place * TOK).astype(F32)
    angles = position * freq[...]
    cosine, sine = jnp.cos(angles), jnp.sin(angles)

    def turned(a, b):
        a, b = a.astype(F32), b.astype(F32)
        return [a * cosine - b * sine, b * cosine + a * sine]

    def upright(pieces):
        return jnp.transpose(jnp.concatenate(pieces, axis=0), (1, 0))

    nothing = jnp.zeros((64, TOK), F32)
    expanded = jnp.dot(lat[...], ew[...], preferred_element_type=F32)
    key_rows = upright(turned(key_t[0:32, :], key_t[32:64, :]) + [nothing])
    low_lane = lax.broadcasted_iota(jnp.int32, (TOK, 128), 1) < 64
    swapped = pltpu.roll(expanded[:, 256:384], 64, 1)
    kvb[0, 0, :, 0:128] = expanded[:, 0:128].astype(BF)
    kvb[0, 0, :, 128:256] = jnp.where(low_lane, key_rows, swapped).astype(BF)
    kvb[0, 0, :, 256:384] = expanded[:, 128:256].astype(BF)
    kvb[0, 0, :, 384:512] = jnp.where(low_lane, swapped, 1.0).astype(BF)
    qb[0, :, 0:128] = upright([q_t[0:128, :].astype(F32)]).astype(BF)
    qb[0, :, 128:256] = upright(turned(q_t[192:224, :], q_t[224:256, :]) + [nothing]).astype(BF)
    qb[0, :, 256:384] = upright(
        turned(q_t[256:288, :], q_t[288:320, :]) + [q_t[128:192, :].astype(F32)]
    ).astype(BF)

    def rows_of(slot, h):
        return kvb.at[slot, 0, pl.ds(64 * h, 64)]

    def slot_of(s, ahead):
        return 0 if s == 0 else 7 if s == 4 else 2 * s - 1 + ahead

    def kv_out(s, h):
        if s < 3 or h == 0:
            send(rows_of(slot_of(s, 0), h), rows_of(slot_of(s + 1, 0), h), kvz_s, kvz_r.at[0, s, h], right_z)
        if s < 3 or h == 1:
            send(rows_of(slot_of(s, 1), h), rows_of(slot_of(s + 1, 1), h), kvz_s, kvz_r.at[1, s, h], left_z)

    def kv_across(slot):
        send(kvb.at[slot, 0], kvb.at[slot, 1], pk_s, pk_r.at[slot], partner)

    def kvz(s, h):
        if s < 4:
            wait_recv(rows_of(slot_of(s, 0), h), kvz_r.at[0, s - 1, h])
            wait_recv(rows_of(slot_of(s, 1), h), kvz_r.at[1, s - 1, h])
            kv_out(s, h)
            if h == 1:
                kv_across(2 * s - 1)
                kv_across(2 * s)
        else:
            wait_recv(rows_of(7, 0), kvz_r.at[0, 3, 0])
            wait_recv(rows_of(7, 1), kvz_r.at[1, 3, 1])
            kv_across(7)

    def q_relay(s):
        if s == 1:
            wait_recv(qb.at[1], q_r.at[0, 0])
            send(qb.at[1, pl.ds(0, 64)], qb.at[3, pl.ds(0, 64)], q_s, q_r.at[0, 1], right_y)
            wait_recv(qb.at[2], q_r.at[1, 0])
            send(qb.at[2, pl.ds(64, 64)], qb.at[3, pl.ds(64, 64)], q_s, q_r.at[1, 1], left_y)
        else:
            wait_recv(qb.at[3, pl.ds(0, 64)], q_r.at[0, 1])
            wait_recv(qb.at[3, pl.ds(64, 64)], q_r.at[1, 1])

    kv_out(0, 0)
    kv_out(0, 1)
    send(qb.at[0], qb.at[1], q_s, q_r.at[0, 0], right_y)
    send(qb.at[0], qb.at[2], q_s, q_r.at[1, 0], left_y)
    kv_across(0)
    macc[...] = jnp.full((2, 512, 128), -3e38, F32)

    offsets = [0, -1, 1, -2, 2, -3, 3, 4]

    def gv_out(zz, j):
        block = gv.at[zz, y, c]
        send(block, block, gvy_s, gvy_r.at[0, 0, j], right_y)
        send(block, block, gvy_s, gvy_r.at[1, 0, j], left_y)
        send(block, block, pg_s, pg_r, partner)

    def gvz(s):
        lo, hi = zat(-s), zat(s)
        if s < 4:
            wait_recv(gv.at[lo, y, c], gvz_r.at[0, s - 1])
            src = gv.at[lo, y, c] if s < 3 else gv.at[lo, y, c, pl.ds(0, 32)]
            send(src, src, gvz_s, gvz_r.at[0, s], right_z)
            wait_recv(gv.at[hi, y, c], gvz_r.at[1, s - 1])
            src = gv.at[hi, y, c] if s < 3 else gv.at[hi, y, c, pl.ds(32, 32)]
            send(src, src, gvz_s, gvz_r.at[1, s], left_z)
            gv_out(lo, 2 * s - 1)
            gv_out(hi, 2 * s)
        else:
            wait_recv(gv.at[lo, y, c, pl.ds(0, 32)], gvz_r.at[0, 3])
            wait_recv(gv.at[lo, y, c, pl.ds(32, 32)], gvz_r.at[1, 3])
            gv_out(lo, 7)

    def gvy(s, j):
        zz = zat(offsets[j])
        a, b, far = yat(-1), yat(1), yat(2)
        if s == 1:
            wait_recv(gv.at[zz, a, c], gvy_r.at[0, 0, j])
            src = gv.at[zz, a, c, pl.ds(0, 32)]
            send(src, src, gvy_s, gvy_r.at[0, 1, j], right_y)
            wait_recv(gv.at[zz, b, c], gvy_r.at[1, 0, j])
            src = gv.at[zz, b, c, pl.ds(32, 32)]
            send(src, src, gvy_s, gvy_r.at[1, 1, j], left_y)
            send(gv.at[zz, a, c], gv.at[zz, a, c], pg_s, pg_r, partner)
            send(gv.at[zz, b, c], gv.at[zz, b, c], pg_s, pg_r, partner)
        else:
            wait_recv(gv.at[zz, far, c, pl.ds(0, 32)], gvy_r.at[0, 1, j])
            wait_recv(gv.at[zz, far, c, pl.ds(32, 32)], gvy_r.at[1, 1, j])
            send(gv.at[zz, far, c], gv.at[zz, far, c], pg_s, pg_r, partner)

    def dny(s):
        a, b, far = yat(-1), yat(1), yat(2)
        if s == 1:
            wait_recv(dn.at[z, a, c], dny_r.at[0, 0])
            src = dn.at[z, a, c, pl.ds(0, 16)]
            send(src, src, dny_s, dny_r.at[0, 1], right_y)
            wait_recv(dn.at[z, b, c], dny_r.at[1, 0])
            src = dn.at[z, b, c, pl.ds(16, 16)]
            send(src, src, dny_s, dny_r.at[1, 1], left_y)
        else:
            wait_recv(dn.at[z, far, c, pl.ds(0, 16)], dny_r.at[0, 1])
            wait_recv(dn.at[z, far, c, pl.ds(16, 16)], dny_r.at[1, 1])

    def dnz(s, r):
        yy = yat((0, -1, 1, 2)[r])
        lo, hi = zat(-s), zat(s)
        if s == 0:
            block = dn.at[z, yy, c]
            send(block, block, dnz_s, dnz_r.at[0, 0, r], right_z)
            send(block, block, dnz_s, dnz_r.at[1, 0, r], left_z)
        elif s < 4:
            wait_recv(dn.at[lo, yy, c], dnz_r.at[0, s - 1, r])
            src = dn.at[lo, yy, c] if s < 3 else dn.at[lo, yy, c, pl.ds(0, 16)]
            send(src, src, dnz_s, dnz_r.at[0, s, r], right_z)
            wait_recv(dn.at[hi, yy, c], dnz_r.at[1, s - 1, r])
            src = dn.at[hi, yy, c] if s < 3 else dn.at[hi, yy, c, pl.ds(16, 16)]
            send(src, src, dnz_s, dnz_r.at[1, s, r], left_z)
        else:
            wait_recv(dn.at[lo, yy, c, pl.ds(0, 16)], dnz_r.at[0, 3, r])
            wait_recv(dn.at[lo, yy, c, pl.ds(16, 16)], dnz_r.at[1, 3, r])
        if r == 3:
            send(dn.at[lo, :, c], dn.at[lo, :, c], pd_s, pd_r, partner)
            if 0 < s < 4:
                send(dn.at[hi, :, c], dn.at[hi, :, c], pd_s, pd_r, partner)

    heads = (
        (0, 256, 0, 256, 256, 512, (NOPE_A + ROPE) ** (-0.5) * LOG2E, accw),
        (256, 384, 128, 256, 384, 512, (NOPE_B + ROPE) ** (-0.5) * LOG2E, accn),
    )

    def scores(j):
        wait_recv(kvb.at[j, 1], pk_r.at[j])
        for head in range(2):
            q0, q1, k0, k1 = heads[head][:4]
            qs = qb[:, :, q0:q1].reshape(512, q1 - q0)
            ks = kvb[j, :, :, k0:k1].reshape(256, k1 - k0)
            s = lax.dot_general(qs, ks, (((1,), (1,)), ((), ())), preferred_element_type=F32)
            s_ref[head, j] = s
            macc[head] = jnp.maximum(macc[head], jnp.maximum(s[:, :128], s[:, 128:]))

    def weigh(head):
        v0, v1, factor, acc = heads[head][4:]
        m = jnp.broadcast_to(jnp.max(macc[head], axis=1, keepdims=True), (512, 128))
        mrow[head] = m
        for j in range(NZ):
            for half in range(2):
                s = s_ref[head, j, :, half * 128 : half * 128 + 128]
                at = j * 256 + half * 128
                p_ref[head, :, at : at + 128] = jnp.exp2((s - m) * factor).astype(BF)
        vs = kvb[:, :, :, v0:v1].reshape(2048, v1 - v0)
        acc[...] = jnp.dot(p_ref[head], vs, preferred_element_type=F32)

    def pack():
        def step(b, carry):
            rows = pl.ds(pl.multiple_of(b * TOK, TOK), TOK)
            wide, narrow = accw[rows, :], accn[rows, :]
            lane = lax.broadcasted_iota(jnp.int32, (TOK, 128), 1)
            tile = narrow
            stats = (
                mrow[0, rows, :], mrow[1, rows, :],
                jnp.broadcast_to(wide[:, 192:193], (TOK, 128)), jnp.broadcast_to(narrow[:, 64:65], (TOK, 128)),
            )
            at = 64
            for stat in stats:
                for piece in split3(stat):
                    tile = jnp.where(lane == at, piece, tile)
                    at += 1
            tile = jnp.where(lane >= at, 0.0, tile)
            part[b, :, 0:128] = wide[:, 0:128].astype(BF)
            part[b, :, 128:256] = tile.astype(BF)
            return carry

        lax.fori_loop(0, NY, step, 0)

    def merge():
        ob[0] = part[0]

        def stat(g, at):
            t = ob[g, :, 128:256].astype(F32)
            return t[:, at : at + 1] + t[:, at + 1 : at + 2] + t[:, at + 2 : at + 3]

        for head in range(2):
            factor = heads[head][6]
            ms = [stat(g, 64 + 3 * head) for g in range(NY)]
            top = jnp.maximum(jnp.maximum(ms[0], ms[1]), jnp.maximum(ms[2], ms[3]))
            lanes = slice(0, 128) if head == 0 else slice(128, 256)
            total = jnp.zeros((TOK, 1), F32)
            value_sum = jnp.zeros((TOK, 128), F32)
            for g in range(NY):
                share = jnp.exp2((ms[g] - top) * factor)
                total = total + share * stat(g, 70 + 3 * head)
                value_sum = value_sum + share * ob[g, :, lanes].astype(F32)
            att[x, :, lanes] = (value_sum / total).astype(BF)

    def part_out():
        send(part.at[3], ob.at[3], o_s, o_r.at[2], {"sp_1": yat(2)})
        send(part.at[1], ob.at[2], o_s, o_r.at[1], left_y)
        send(part.at[2], ob.at[1], o_s, o_r.at[0], right_y)

    def part_in():
        for o in (1, 2, 3):
            wait_recv(ob.at[o], o_r.at[o - 1])

    def att_out():
        for o in (2, 1, 3):
            send(att.at[x], att.at[x], x_s, x_r.at[o - 1], {"tp": xat(o)})

    dny(1)
    gvy(1, 0)
    gvz(1)
    kvz(1, 0)
    q_relay(1)
    dny(2)
    kvz(1, 1)
    gvy(2, 0)
    gvz(2)
    gvy(1, 1)
    kvz(2, 0)
    kvz(2, 1)
    gvy(1, 2)
    q_relay(2)
    scores(0)
    scores(1)
    scores(2)
    gvz(3)
    scores(3)
    scores(4)
    gvy(1, 3)
    kvz(3, 0)
    kvz(3, 1)
    dnz(0, 0)
    dnz(0, 1)
    dnz(0, 2)
    gvy(1, 4)
    dnz(0, 3)
    gvz(4)
    gvy(2, 1)
    scores(5)
    scores(6)
    gvy(2, 2)
    kvz(4, 0)
    gvy(1, 5)
    dnz(1, 0)
    scores(7)
    weigh(0)
    gvy(1, 6)
    gvy(2, 3)
    dnz(1, 1)
    dnz(1, 2)
    dnz(1, 3)
    weigh(1)
    pack()
    part_out()
    gvy(2, 4)
    dnz(2, 0)
    gvy(1, 7)
    dnz(2, 1)
    gvy(2, 5)
    dnz(2, 2)
    gvy(2, 6)
    dnz(2, 3)
    dnz(3, 0)
    part_in()
    merge()
    att_out()
    dnz(3, 1)
    gvy(2, 7)
    dnz(3, 2)
    dnz(3, 3)
    dnz(4, 0)
    dnz(4, 1)
    dnz(4, 2)
    load_ow.wait()
    load_res.wait()
    for o in (2, 1, 3):
        wait_recv(att.at[xat(-o)], x_r.at[o - 1])

    def project(n, ss):
        cols = pl.ds(pl.multiple_of(n * 256, 256), 256)
        total = resid[:, cols].astype(F32)
        for h in range(NX):
            total = total + jnp.dot(
                att[h, :, 0:192], ow[pl.ds(h * 192, 192), cols], preferred_element_type=F32
            )
        rounded = total.astype(BF)
        stream[:, cols] = rounded
        wide = rounded.astype(F32)
        return ss + jnp.sum(wide * wide, axis=1, keepdims=True)

    ss = lax.fori_loop(0, 8, project, jnp.zeros((TOK, 1), F32))
    scale = lax.rsqrt(ss * (1.0 / D) + 1e-06)

    def norm(n, carry):
        cols = pl.ds(pl.multiple_of(n * 256, 256), 256)
        scaled = stream[:, cols].astype(F32) * scale
        normed[:, cols] = (scaled * gain[:, cols].astype(F32)).astype(BF)
        return carry

    lax.fori_loop(0, 8, norm, 0)
    dnz(4, 3)
    wait_recv(gv.at[:, :, other], pg_r)

    def up(lo, dst):
        def step(n, carry):
            cols = pl.ds(pl.multiple_of(n * 256, 256), 256)
            w = gv[:, :, :, lo : lo + 32, cols].reshape(D, 256)
            dst[:, cols] = jnp.dot(normed[...], w, preferred_element_type=F32).astype(BF)
            return carry

        lax.fori_loop(0, 3, step, 0)

    up(0, gate)
    send(gate.at[pl.ds(112, 16)], hp, h_s.at[0], h_r.at[0], device_of(after))
    send(gate.at[pl.ds(0, 16)], hn, h_s.at[1], h_r.at[1], device_of(before))
    up(32, value)
    wait_recv(hp, h_r.at[0])
    wait_recv(hn, h_r.at[1])

    row = lax.broadcasted_iota(jnp.int32, (TOK, 256), 0)
    for n in range(3):
        cols = slice(n * 256, n * 256 + 256)
        g = gate[:, cols].astype(F32)
        first = jnp.where(place > 0, hp[:, cols].astype(F32)[15:16], 0.0)
        last = jnp.where(place < 63, hn[:, cols].astype(F32)[0:1], 0.0)
        low = jnp.where(row == 0, first, pltpu.roll(g, 1, 0))
        high = jnp.where(row == TOK - 1, last, pltpu.roll(g, TOK - 1, 0))
        cw = conv_w[:, cols].astype(F32)
        mixed = low * cw[0:1] + g * cw[1:2] + high * cw[2:3]
        silu = mixed / (1.0 + jnp.exp(-mixed))
        act[:, cols] = (silu * value[:, cols].astype(F32)).astype(BF)

    wait_recv(dn.at[:, :, other], pd_r)

    for half in range(2):

        def down(n, carry):
            w = dn[half * 4 + n].reshape(256, FFD)
            d = lax.dot_general(act[...], w, (((1,), (1,)), ((), ())), preferred_element_type=F32)
            cols = pl.ds(pl.multiple_of(n * 256, 256), 256)
            fp[half, :, :, cols] = d.astype(BF).reshape(NX, 32, 256)
            return carry

        lax.fori_loop(0, 4, down, 0)
        for o in (2, 1, 3):
            peer = xat(o)
            send(fp.at[half, peer], fr.at[half, x], f_s, f_r.at[half, o - 1], {"tp": peer})

    for half in range(2):
        cols = slice(half * 1024, half * 1024 + 1024)
        rows = pl.ds(pl.multiple_of(x * 32, 32), 32)
        total = stream[rows, cols].astype(F32) + fp[half, x].astype(F32)
        for o in (1, 3, 2):
            wait_recv(fr.at[half, xat(-o)], f_r.at[half, o - 1])
            total = total + fr[half, xat(-o)].astype(F32)
        out_ref[:, cols] = total.astype(BF)

    wait_send(kvb.at[pl.ds(0, 7), 0], kvz_s)
    wait_send(qb.at[pl.ds(0, 3)], q_s)
    wait_send(gv.at[pl.ds(0, 7), 0, 0], gvz_s)
    wait_send(gv.at[:, pl.ds(0, 3), 0], gvy_s)
    wait_send(dn.at[0, pl.ds(0, 3), 0], dny_s)
    wait_send(dn.at[pl.ds(0, 7), :, 0], dnz_s)
    wait_send(kvb.at[:, 0], pk_s)
    wait_send(gv.at[:, :, 0], pg_s)
    wait_send(dn.at[:, :, 0], pd_s)
    wait_send(part.at[pl.ds(0, 3)], o_s)
    wait_send(att.at[pl.ds(0, 3)], x_s)
    wait_send(hp, h_s.at[0])
    wait_send(hn, h_s.at[1])
    wait_send(fp.at[:, pl.ds(0, 3)], f_s)


def layer(*operands):
    vmem = pl.BlockSpec(memory_space=pltpu.VMEM)
    hbm = pl.BlockSpec(memory_space=pltpu.HBM)
    dma = pltpu.SemaphoreType.DMA
    scratch = [
        pltpu.VMEM((NZ, 2, TOK, 512), BF),
        pltpu.VMEM((NY, TOK, 384), BF),
        pltpu.VMEM((NZ, NY, 2, 64, FFD), BF),
        pltpu.VMEM((NZ, NY, 2, 32, FFD), BF),
        pltpu.VMEM((768, D), BF),
        pltpu.VMEM((TOK, D), BF),
        pltpu.VMEM((2, NZ, 512, 256), F32),
        pltpu.VMEM((2, 512, 2048), BF),
        pltpu.VMEM((2, 512, 128), F32),
        pltpu.VMEM((2, 512, 128), F32),
        pltpu.VMEM((512, 256), F32),
        pltpu.VMEM((512, 128), F32),
        pltpu.VMEM((NY, TOK, 256), BF),
        pltpu.VMEM((NY, TOK, 256), BF),
        pltpu.VMEM((NX, TOK, 256), BF),
        pltpu.VMEM((TOK, D), BF),
        pltpu.VMEM((TOK, D), BF),
        pltpu.VMEM((TOK, FFD), BF),
        pltpu.VMEM((TOK, FFD), BF),
        pltpu.VMEM((16, FFD), BF),
        pltpu.VMEM((16, FFD), BF),
        pltpu.VMEM((TOK, FFD), BF),
        pltpu.VMEM((2, NX, 32, 1024), BF),
        pltpu.VMEM((2, NX, 32, 1024), BF),
        dma, dma((2, 4, 2)), dma, dma((2, 2)), dma, dma((2, 4)), dma, dma((2, 2, 8)),
        dma, dma((2, 2)), dma, dma((2, 4, 4)),
        dma, dma((8,)), dma, dma, dma, dma, dma, dma((3,)), dma, dma((3,)), dma((2,)), dma((2,)),
        dma, dma((2, 3)), dma((2,)),
    ]
    return pl.pallas_call(
        kernel,
        out_shape=jax.ShapeDtypeStruct((32, D), BF),
        in_specs=[vmem] * 10 + [hbm] * 2,
        out_specs=vmem,
        scratch_shapes=scratch,
        compiler_params=pltpu.CompilerParams(collective_id=0, has_side_effects=True),
    )(*operands)


def body(
    queries, latents, shared_key, expand_weight, residual, out_weight,
    norm_gain, gate_weight, value_weight, conv_weight, down_weight,
):
    frequency = 10000.0 ** (-jnp.arange(ROPE // 2, dtype=F32) / (ROPE // 2))
    return layer(
        queries.T, latents, shared_key.T, expand_weight, gate_weight, value_weight, down_weight.T,
        jnp.broadcast_to(frequency[:, None], (ROPE // 2, TOK)), norm_gain[None, :], conv_weight,
        residual, out_weight,
    )


def solution(mesh):
    split = Mesh(mesh.devices.reshape(NZ, NY, 2, mesh.shape["tp"]), ("sp_0", "sp_1", "sp_2", "tp"))
    placed = (
        P(SP, "tp"),
        P(SP, None),
        P(SP, None),
        P(None, "tp"),
        P(SP, None),
        P(),
        P(),
        P(SP, "tp"),
        P(SP, "tp"),
        P(None, "tp"),
        P("tp", SP),
    )
    return jax.shard_map(
        body, mesh=split, in_specs=placed, out_specs=P(SP_TP, None), check_vma=False
    )
```

```python
import functools

import jax
import jax.numpy as jnp
import numpy as np
from jax import lax
from jax.experimental import pallas as pl
from jax.experimental.pallas import tpu as pltpu
from jax.sharding import Mesh
from jax.sharding import PartitionSpec as P

NOPE_A = 128
VAL_A = 128
NOPE_B = 64
VAL_B = 64
ROPE = 64
SP = ("sp_0", "sp_1", "sp_2")
SP_TP = ("sp_0", "sp_1", "sp_2", "tp")
NZ, NY, NX = 8, 4, 4
TOK = 128
D = 2048
FFD = 768
MESH = pl.DeviceIdType.MESH
LOG2E = 1.4426950408889634
F32 = jnp.float32
BF = jnp.bfloat16


def split3(v):
    hi = v.astype(BF).astype(F32)
    rest = v - hi
    mid = rest.astype(BF).astype(F32)
    return hi, mid, rest - mid


def kernel(
    gain, conv_w, q_hbm, lat_hbm, key_hbm, ew_hbm, gate_hbm, value_hbm, dn_hbm, freq_hbm, resid_hbm, ow_hbm,
    out_ref,
    q_t, lat, key_t, ew, freq, kvb, qb, gv, dn, ow, resid, s_ref, p_ref, macc, mrow, accw, accn,
    part, ob, att, stream, normed, gate, value, hp, hn, act, fp, fr,
    kvz_s, kvz_r, q_s, q_r, gvz_s, gvz_r, gvy_s, gvy_r, dny_s, dny_r, dnz_s, dnz_r,
    pk_s, pk_r, pg_s, pg_r, pd_s, pd_r, o_s, o_r, x_s, x_r, h_s, h_r, f_s, f_r, loc,
):
    z = lax.axis_index("sp_0")
    y = lax.axis_index("sp_1")
    c = lax.axis_index("sp_2")
    x = lax.axis_index("tp")
    other = 1 - c

    def zat(k):
        return lax.rem(z + (k + NZ), NZ)

    def yat(k):
        return lax.rem(y + (k + NY), NY)

    def xat(k):
        return lax.rem(x + (k + NX), NX)

    right_z, left_z = {"sp_0": zat(1)}, {"sp_0": zat(-1)}
    right_y, left_y = {"sp_1": yat(1)}, {"sp_1": yat(-1)}
    partner = {"sp_2": other}
    place = (z * NY + y) * 2 + c
    after = lax.rem(place + 1, 64)
    before = lax.rem(place + 63, 64)

    def device_of(i):
        return {"sp_0": i // 8, "sp_1": lax.rem(i // 2, 4), "sp_2": lax.rem(i, 2)}

    def send(src, dst, ssem, rsem, dev):
        pltpu.make_async_remote_copy(
            src_ref=src, dst_ref=dst, send_sem=ssem, recv_sem=rsem, device_id=dev, device_id_type=MESH
        ).start()

    def wait_recv(ref, sem):
        pltpu.make_async_remote_copy(
            src_ref=ref, dst_ref=ref, send_sem=sem, recv_sem=sem, device_id=partner, device_id_type=MESH
        ).wait_recv()

    def wait_send(ref, sem):
        pltpu.make_async_remote_copy(
            src_ref=ref, dst_ref=ref, send_sem=sem, recv_sem=sem, device_id=partner, device_id_type=MESH
        ).wait_send()

    barrier = pltpu.get_barrier_semaphore()
    greeted = [
        partner, right_z, left_z, right_y, left_y, {"sp_1": yat(2)},
        {"tp": xat(1)}, {"tp": xat(2)}, {"tp": xat(3)}, device_of(after), device_of(before),
    ]
    for dev in greeted:
        pl.semaphore_signal(barrier, inc=1, device_id=dev, device_id_type=MESH)

    def load(src, dst, i):
        copy = pltpu.make_async_copy(src, dst, loc.at[i])
        copy.start()
        return copy

    first_loads = [
        load(lat_hbm, lat, 0), load(ew_hbm, ew, 1), load(key_hbm, key_t, 2), load(freq_hbm, freq, 3),
        load(q_hbm, q_t, 4),
    ]
    weight_loads = [
        load(gate_hbm, gv.at[z, y, c, pl.ds(0, 32)], 5), load(value_hbm, gv.at[z, y, c, pl.ds(32, 32)], 6),
        load(dn_hbm, dn.at[z, y, c], 7),
    ]
    load_res = load(resid_hbm, resid, 8)
    load_ow = load(ow_hbm, ow, 9)
    pl.semaphore_wait(barrier, len(greeted))
    for copy in first_loads:
        copy.wait()

    position = (lax.broadcasted_iota(jnp.int32, (32, TOK), 1) + place * TOK).astype(F32)
    angles = position * freq[...]
    cosine, sine = jnp.cos(angles), jnp.sin(angles)

    def turned(a, b):
        a, b = a.astype(F32), b.astype(F32)
        return [a * cosine - b * sine, b * cosine + a * sine]

    def upright(pieces):
        return jnp.transpose(jnp.concatenate(pieces, axis=0), (1, 0))

    nothing = jnp.zeros((64, TOK), F32)
    expanded = jnp.dot(lat[...], ew[...], preferred_element_type=F32)
    key_rows = upright(turned(key_t[0:32, :], key_t[32:64, :]) + [nothing])
    low_lane = lax.broadcasted_iota(jnp.int32, (TOK, 128), 1) < 64
    swapped = pltpu.roll(expanded[:, 256:384], 64, 1)
    kvb[0, 0, :, 0:128] = expanded[:, 0:128].astype(BF)
    kvb[0, 0, :, 128:256] = jnp.where(low_lane, key_rows, swapped).astype(BF)
    kvb[0, 0, :, 256:384] = expanded[:, 128:256].astype(BF)
    kvb[0, 0, :, 384:512] = jnp.where(low_lane, swapped, 1.0).astype(BF)
    qb[0, :, 0:128] = upright([q_t[0:128, :].astype(F32)]).astype(BF)
    qb[0, :, 128:256] = upright(turned(q_t[192:224, :], q_t[224:256, :]) + [nothing]).astype(BF)
    qb[0, :, 256:384] = upright(
        turned(q_t[256:288, :], q_t[288:320, :]) + [q_t[128:192, :].astype(F32)]
    ).astype(BF)

    def rows_of(slot, h):
        return kvb.at[slot, 0, pl.ds(64 * h, 64)]

    def slot_of(s, ahead):
        return 0 if s == 0 else 7 if s == 4 else 2 * s - 1 + ahead

    def kv_out(s, h):
        if s < 3 or h == 0:
            send(rows_of(slot_of(s, 0), h), rows_of(slot_of(s + 1, 0), h), kvz_s, kvz_r.at[0, s, h], right_z)
        if s < 3 or h == 1:
            send(rows_of(slot_of(s, 1), h), rows_of(slot_of(s + 1, 1), h), kvz_s, kvz_r.at[1, s, h], left_z)

    def kv_across(slot):
        send(kvb.at[slot, 0], kvb.at[slot, 1], pk_s, pk_r.at[slot], partner)

    def kvz(s, h):
        if s < 4:
            wait_recv(rows_of(slot_of(s, 0), h), kvz_r.at[0, s - 1, h])
            wait_recv(rows_of(slot_of(s, 1), h), kvz_r.at[1, s - 1, h])
            kv_out(s, h)
            if h == 1:
                kv_across(2 * s - 1)
                kv_across(2 * s)
        else:
            wait_recv(rows_of(7, 0), kvz_r.at[0, 3, 0])
            wait_recv(rows_of(7, 1), kvz_r.at[1, 3, 1])
            kv_across(7)

    def q_relay(s):
        if s == 1:
            wait_recv(qb.at[1], q_r.at[0, 0])
            send(qb.at[1, pl.ds(0, 64)], qb.at[3, pl.ds(0, 64)], q_s, q_r.at[0, 1], right_y)
            wait_recv(qb.at[2], q_r.at[1, 0])
            send(qb.at[2, pl.ds(64, 64)], qb.at[3, pl.ds(64, 64)], q_s, q_r.at[1, 1], left_y)
        else:
            wait_recv(qb.at[3, pl.ds(0, 64)], q_r.at[0, 1])
            wait_recv(qb.at[3, pl.ds(64, 64)], q_r.at[1, 1])

    kv_out(0, 0)
    kv_out(0, 1)
    send(qb.at[0], qb.at[1], q_s, q_r.at[0, 0], right_y)
    send(qb.at[0], qb.at[2], q_s, q_r.at[1, 0], left_y)
    kv_across(0)
    macc[...] = jnp.full((2, 512, 128), -3e38, F32)

    def gvz_own():
        own = gv.at[z, y, c]
        send(own, own, gvz_s, gvz_r.at[0, 0], right_z)
        send(own, own, gvz_s, gvz_r.at[1, 0], left_z)

    def dny_own():
        own = dn.at[z, y, c]
        send(own, own, dny_s, dny_r.at[0, 0], right_y)
        send(own, own, dny_s, dny_r.at[1, 0], left_y)

    def gvy_own():
        own = gv.at[z, y, c]
        send(own, own, gvy_s, gvy_r.at[0, 0, 0], right_y)
        send(own, own, gvy_s, gvy_r.at[1, 0, 0], left_y)
        send(own, own, pg_s, pg_r, partner)

    for copy in weight_loads:
        copy.wait()

    offsets = [0, -1, 1, -2, 2, -3, 3, 4]

    def gv_out(zz, j):
        block = gv.at[zz, y, c]
        send(block, block, gvy_s, gvy_r.at[0, 0, j], right_y)
        send(block, block, gvy_s, gvy_r.at[1, 0, j], left_y)
        send(block, block, pg_s, pg_r, partner)

    def gvz(s):
        lo, hi = zat(-s), zat(s)
        if s < 4:
            wait_recv(gv.at[lo, y, c], gvz_r.at[0, s - 1])
            src = gv.at[lo, y, c] if s < 3 else gv.at[lo, y, c, pl.ds(0, 32)]
            send(src, src, gvz_s, gvz_r.at[0, s], right_z)
            wait_recv(gv.at[hi, y, c], gvz_r.at[1, s - 1])
            src = gv.at[hi, y, c] if s < 3 else gv.at[hi, y, c, pl.ds(32, 32)]
            send(src, src, gvz_s, gvz_r.at[1, s], left_z)
            gv_out(lo, 2 * s - 1)
            gv_out(hi, 2 * s)
        else:
            wait_recv(gv.at[lo, y, c, pl.ds(0, 32)], gvz_r.at[0, 3])
            wait_recv(gv.at[lo, y, c, pl.ds(32, 32)], gvz_r.at[1, 3])
            gv_out(lo, 7)

    def gvy(s, j):
        zz = zat(offsets[j])
        a, b, far = yat(-1), yat(1), yat(2)
        if s == 1:
            wait_recv(gv.at[zz, a, c], gvy_r.at[0, 0, j])
            src = gv.at[zz, a, c, pl.ds(0, 32)]
            send(src, src, gvy_s, gvy_r.at[0, 1, j], right_y)
            wait_recv(gv.at[zz, b, c], gvy_r.at[1, 0, j])
            src = gv.at[zz, b, c, pl.ds(32, 32)]
            send(src, src, gvy_s, gvy_r.at[1, 1, j], left_y)
            send(gv.at[zz, a, c], gv.at[zz, a, c], pg_s, pg_r, partner)
            send(gv.at[zz, b, c], gv.at[zz, b, c], pg_s, pg_r, partner)
        else:
            wait_recv(gv.at[zz, far, c, pl.ds(0, 32)], gvy_r.at[0, 1, j])
            wait_recv(gv.at[zz, far, c, pl.ds(32, 32)], gvy_r.at[1, 1, j])
            send(gv.at[zz, far, c], gv.at[zz, far, c], pg_s, pg_r, partner)

    def dny(s):
        a, b, far = yat(-1), yat(1), yat(2)
        if s == 1:
            wait_recv(dn.at[z, a, c], dny_r.at[0, 0])
            src = dn.at[z, a, c, pl.ds(0, 16)]
            send(src, src, dny_s, dny_r.at[0, 1], right_y)
            wait_recv(dn.at[z, b, c], dny_r.at[1, 0])
            src = dn.at[z, b, c, pl.ds(16, 16)]
            send(src, src, dny_s, dny_r.at[1, 1], left_y)
        else:
            wait_recv(dn.at[z, far, c, pl.ds(0, 16)], dny_r.at[0, 1])
            wait_recv(dn.at[z, far, c, pl.ds(16, 16)], dny_r.at[1, 1])

    def dnz(s, r):
        yy = yat((0, -1, 1, 2)[r])
        lo, hi = zat(-s), zat(s)
        if s == 0:
            block = dn.at[z, yy, c]
            send(block, block, dnz_s, dnz_r.at[0, 0, r], right_z)
            send(block, block, dnz_s, dnz_r.at[1, 0, r], left_z)
        elif s < 4:
            wait_recv(dn.at[lo, yy, c], dnz_r.at[0, s - 1, r])
            src = dn.at[lo, yy, c] if s < 3 else dn.at[lo, yy, c, pl.ds(0, 16)]
            send(src, src, dnz_s, dnz_r.at[0, s, r], right_z)
            wait_recv(dn.at[hi, yy, c], dnz_r.at[1, s - 1, r])
            src = dn.at[hi, yy, c] if s < 3 else dn.at[hi, yy, c, pl.ds(16, 16)]
            send(src, src, dnz_s, dnz_r.at[1, s, r], left_z)
        else:
            wait_recv(dn.at[lo, yy, c, pl.ds(0, 16)], dnz_r.at[0, 3, r])
            wait_recv(dn.at[lo, yy, c, pl.ds(16, 16)], dnz_r.at[1, 3, r])
        if r == 3:
            send(dn.at[lo, :, c], dn.at[lo, :, c], pd_s, pd_r, partner)
            if 0 < s < 4:
                send(dn.at[hi, :, c], dn.at[hi, :, c], pd_s, pd_r, partner)

    heads = (
        (0, 256, 0, 256, 256, 512, (NOPE_A + ROPE) ** (-0.5) * LOG2E, accw),
        (256, 384, 128, 256, 384, 512, (NOPE_B + ROPE) ** (-0.5) * LOG2E, accn),
    )

    def scores(j):
        wait_recv(kvb.at[j, 1], pk_r.at[j])
        for head in range(2):
            q0, q1, k0, k1 = heads[head][:4]
            qs = qb[:, :, q0:q1].reshape(512, q1 - q0)
            ks = kvb[j, :, :, k0:k1].reshape(256, k1 - k0)
            s = lax.dot_general(qs, ks, (((1,), (1,)), ((), ())), preferred_element_type=F32)
            s_ref[head, j] = s
            macc[head] = jnp.maximum(macc[head], jnp.maximum(s[:, :128], s[:, 128:]))

    def weigh(head):
        v0, v1, factor, acc = heads[head][4:]
        m = jnp.broadcast_to(jnp.max(macc[head], axis=1, keepdims=True), (512, 128))
        mrow[head] = m
        for j in range(NZ):
            for half in range(2):
                s = s_ref[head, j, :, half * 128 : half * 128 + 128]
                at = j * 256 + half * 128
                p_ref[head, :, at : at + 128] = jnp.exp2((s - m) * factor).astype(BF)
        vs = kvb[:, :, :, v0:v1].reshape(2048, v1 - v0)
        acc[...] = jnp.dot(p_ref[head], vs, preferred_element_type=F32)

    def pack():
        def step(b, carry):
            rows = pl.ds(pl.multiple_of(b * TOK, TOK), TOK)
            wide, narrow = accw[rows, :], accn[rows, :]
            lane = lax.broadcasted_iota(jnp.int32, (TOK, 128), 1)
            tile = narrow
            stats = (
                mrow[0, rows, :], mrow[1, rows, :],
                jnp.broadcast_to(wide[:, 192:193], (TOK, 128)), jnp.broadcast_to(narrow[:, 64:65], (TOK, 128)),
            )
            at = 64
            for stat in stats:
                for piece in split3(stat):
                    tile = jnp.where(lane == at, piece, tile)
                    at += 1
            tile = jnp.where(lane >= at, 0.0, tile)
            part[b, :, 0:128] = wide[:, 0:128].astype(BF)
            part[b, :, 128:256] = tile.astype(BF)
            return carry

        lax.fori_loop(0, NY, step, 0)

    def merge():
        ob[0] = part[0]

        def stat(g, at):
            t = ob[g, :, 128:256].astype(F32)
            return t[:, at : at + 1] + t[:, at + 1 : at + 2] + t[:, at + 2 : at + 3]

        for head in range(2):
            factor = heads[head][6]
            ms = [stat(g, 64 + 3 * head) for g in range(NY)]
            top = jnp.maximum(jnp.maximum(ms[0], ms[1]), jnp.maximum(ms[2], ms[3]))
            lanes = slice(0, 128) if head == 0 else slice(128, 256)
            total = jnp.zeros((TOK, 1), F32)
            value_sum = jnp.zeros((TOK, 128), F32)
            for g in range(NY):
                share = jnp.exp2((ms[g] - top) * factor)
                total = total + share * stat(g, 70 + 3 * head)
                value_sum = value_sum + share * ob[g, :, lanes].astype(F32)
            att[x, :, lanes] = (value_sum / total).astype(BF)

    def part_out():
        send(part.at[3], ob.at[3], o_s, o_r.at[2], {"sp_1": yat(2)})
        send(part.at[1], ob.at[2], o_s, o_r.at[1], left_y)
        send(part.at[2], ob.at[1], o_s, o_r.at[0], right_y)

    def part_in():
        for o in (1, 2, 3):
            wait_recv(ob.at[o], o_r.at[o - 1])

    def att_out():
        for o in (2, 1, 3):
            send(att.at[x], att.at[x], x_s, x_r.at[o - 1], {"tp": xat(o)})

    gvz_own()
    dny_own()
    gvy_own()
    q_relay(1)
    kvz(1, 0)
    dny(1)
    kvz(1, 1)
    gvy(1, 0)
    gvz(1)
    q_relay(2)
    scores(0)
    scores(1)
    dny(2)
    scores(2)
    kvz(2, 0)
    gvy(2, 0)
    kvz(2, 1)
    gvy(1, 1)
    scores(3)
    scores(4)
    gvz(2)
    kvz(3, 0)
    gvy(2, 1)
    kvz(3, 1)
    dnz(0, 1)
    dnz(0, 0)
    gvy(1, 2)
    dnz(0, 2)
    scores(5)
    scores(6)
    gvz(3)
    kvz(4, 0)
    gvy(1, 3)
    dnz(0, 3)
    gvy(2, 2)
    dnz(1, 1)
    scores(7)
    weigh(0)
    weigh(1)
    pack()
    part_out()
    dnz(1, 2)
    dnz(1, 0)
    gvz(4)
    gvy(1, 4)
    gvy(1, 5)
    gvy(1, 6)
    dnz(1, 3)
    gvy(2, 3)
    dnz(2, 1)
    dnz(2, 2)
    part_in()
    merge()
    att_out()
    dnz(2, 0)
    dnz(2, 3)
    gvy(1, 7)
    dnz(3, 1)
    gvy(2, 4)
    dnz(3, 2)
    gvy(2, 5)
    dnz(3, 0)
    load_ow.wait()
    load_res.wait()
    for o in (2, 1, 3):
        wait_recv(att.at[xat(-o)], x_r.at[o - 1])

    ss = jnp.zeros((TOK, 1), F32)
    for n in range(8):
        cols = slice(n * 256, n * 256 + 256)
        total = resid[:, cols].astype(F32)
        for h in range(NX):
            total = total + jnp.dot(att[h, :, 0:192], ow[h * 192 : h * 192 + 192, cols], preferred_element_type=F32)
        rounded = total.astype(BF)
        stream[:, cols] = rounded
        wide = rounded.astype(F32)
        ss = ss + jnp.sum(wide * wide, axis=1, keepdims=True)
    scale = lax.rsqrt(ss * (1.0 / D) + 1e-06)
    for n in range(8):
        cols = slice(n * 256, n * 256 + 256)
        scaled = stream[:, cols].astype(F32) * scale
        normed[:, cols] = (scaled * gain[cols].astype(F32).reshape(1, 256)).astype(BF)
    gvy(2, 6)
    dnz(3, 3)
    gvy(2, 7)
    dnz(4, 1)
    dnz(4, 2)
    dnz(4, 0)
    dnz(4, 3)
    wait_recv(gv.at[:, :, other], pg_r)

    def up(lo, dst):
        for n in range(3):
            cols = slice(n * 256, n * 256 + 256)
            w = gv[:, :, :, lo : lo + 32, cols].reshape(D, 256)
            dst[:, cols] = jnp.dot(normed[...], w, preferred_element_type=F32).astype(BF)

    up(0, gate)
    send(gate.at[pl.ds(112, 16)], hp, h_s.at[0], h_r.at[0], device_of(after))
    send(gate.at[pl.ds(0, 16)], hn, h_s.at[1], h_r.at[1], device_of(before))
    up(32, value)
    wait_recv(hp, h_r.at[0])
    wait_recv(hn, h_r.at[1])

    row = lax.broadcasted_iota(jnp.int32, (TOK, 256), 0)
    for n in range(3):
        cols = slice(n * 256, n * 256 + 256)
        g = gate[:, cols].astype(F32)
        first = jnp.where(place > 0, hp[:, cols].astype(F32)[15:16], 0.0)
        last = jnp.where(place < 63, hn[:, cols].astype(F32)[0:1], 0.0)
        low = jnp.where(row == 0, first, pltpu.roll(g, 1, 0))
        high = jnp.where(row == TOK - 1, last, pltpu.roll(g, TOK - 1, 0))
        cw = conv_w[:, cols].astype(F32)
        mixed = low * cw[0:1] + g * cw[1:2] + high * cw[2:3]
        silu = mixed / (1.0 + jnp.exp(-mixed))
        act[:, cols] = (silu * value[:, cols].astype(F32)).astype(BF)

    wait_recv(dn.at[:, :, other], pd_r)

    for n in range(NZ):
        w = dn[n].reshape(256, FFD)
        d = lax.dot_general(act[...], w, (((1,), (1,)), ((), ())), preferred_element_type=F32)
        fp[n] = d.astype(BF).reshape(NX, 32, 256)
        for o in (2, 1, 3):
            peer = xat(o)
            send(fp.at[n, peer], fr.at[n, x], f_s, f_r.at[n, o - 1], {"tp": peer})

    rows = pl.ds(pl.multiple_of(x * 32, 32), 32)
    for n in range(NZ):
        cols = slice(n * 256, n * 256 + 256)
        total = stream[rows, cols].astype(F32) + fp[n, x].astype(F32)
        for o in (1, 3, 2):
            wait_recv(fr.at[n, xat(-o)], f_r.at[n, o - 1])
            total = total + fr[n, xat(-o)].astype(F32)
        out_ref[:, cols] = total.astype(BF)

    wait_send(kvb.at[pl.ds(0, 7), 0], kvz_s)
    wait_send(qb.at[pl.ds(0, 3)], q_s)
    wait_send(gv.at[pl.ds(0, 7), 0, 0], gvz_s)
    wait_send(gv.at[:, pl.ds(0, 3), 0], gvy_s)
    wait_send(dn.at[0, pl.ds(0, 3), 0], dny_s)
    wait_send(dn.at[pl.ds(0, 7), :, 0], dnz_s)
    wait_send(kvb.at[:, 0], pk_s)
    wait_send(gv.at[:, :, 0], pg_s)
    wait_send(dn.at[:, :, 0], pd_s)
    wait_send(part.at[pl.ds(0, 3)], o_s)
    wait_send(att.at[pl.ds(0, 3)], x_s)
    wait_send(hp, h_s.at[0])
    wait_send(hn, h_s.at[1])
    wait_send(fp.at[:, pl.ds(0, 3)], f_s)


def layer(*operands):
    vmem = pl.BlockSpec(memory_space=pltpu.VMEM)
    hbm = pl.BlockSpec(memory_space=pltpu.HBM)
    dma = pltpu.SemaphoreType.DMA
    scratch = [
        pltpu.VMEM((320, TOK), BF),
        pltpu.VMEM((TOK, 512), BF),
        pltpu.VMEM((64, TOK), BF),
        pltpu.VMEM((512, 384), BF),
        pltpu.VMEM((32, TOK), F32),
        pltpu.VMEM((NZ, 2, TOK, 512), BF),
        pltpu.VMEM((NY, TOK, 384), BF),
        pltpu.VMEM((NZ, NY, 2, 64, FFD), BF),
        pltpu.VMEM((NZ, NY, 2, 32, FFD), BF),
        pltpu.VMEM((768, D), BF),
        pltpu.VMEM((TOK, D), BF),
        pltpu.VMEM((2, NZ, 512, 256), F32),
        pltpu.VMEM((2, 512, 2048), BF),
        pltpu.VMEM((2, 512, 128), F32),
        pltpu.VMEM((2, 512, 128), F32),
        pltpu.VMEM((512, 256), F32),
        pltpu.VMEM((512, 128), F32),
        pltpu.VMEM((NY, TOK, 256), BF),
        pltpu.VMEM((NY, TOK, 256), BF),
        pltpu.VMEM((NX, TOK, 256), BF),
        pltpu.VMEM((TOK, D), BF),
        pltpu.VMEM((TOK, D), BF),
        pltpu.VMEM((TOK, FFD), BF),
        pltpu.VMEM((TOK, FFD), BF),
        pltpu.VMEM((16, FFD), BF),
        pltpu.VMEM((16, FFD), BF),
        pltpu.VMEM((TOK, FFD), BF),
        pltpu.VMEM((NZ, NX, 32, 256), BF),
        pltpu.VMEM((NZ, NX, 32, 256), BF),
        dma, dma((2, 4, 2)), dma, dma((2, 2)), dma, dma((2, 4)), dma, dma((2, 2, 8)),
        dma, dma((2, 2)), dma, dma((2, 4, 4)),
        dma, dma((8,)), dma, dma, dma, dma, dma, dma((3,)), dma, dma((3,)), dma((2,)), dma((2,)),
        dma, dma((NZ, 3)), dma((10,)),
    ]
    return pl.pallas_call(
        kernel,
        out_shape=pltpu.VMEM((32, D), BF),
        in_specs=[vmem] * 2 + [hbm] * 10,
        out_specs=vmem,
        scratch_shapes=scratch,
        compiler_params=pltpu.CompilerParams(collective_id=0, has_side_effects=True),
    )(*operands)


def body(
    queries, latents, shared_key, expand_weight, residual, out_weight,
    norm_gain, gate_weight, value_weight, conv_weight, down_weight,
):
    frequency = (10000.0 ** (-np.arange(ROPE // 2) / (ROPE // 2))).astype(np.float32)
    return layer(
        norm_gain, conv_weight, queries.T, latents, shared_key.T, expand_weight, gate_weight, value_weight,
        down_weight.T, np.ascontiguousarray(np.broadcast_to(frequency[:, None], (ROPE // 2, TOK))),
        residual, out_weight,
    )


def solution(mesh):
    split = Mesh(mesh.devices.reshape(NZ, NY, 2, mesh.shape["tp"]), ("sp_0", "sp_1", "sp_2", "tp"))
    placed = (
        P(SP, "tp"),
        P(SP, None),
        P(SP, None),
        P(None, "tp"),
        P(SP, None),
        P(),
        P(),
        P(SP, "tp"),
        P(SP, "tp"),
        P(None, "tp"),
        P("tp", SP),
    )
    return jax.shard_map(
        body, mesh=split, in_specs=placed, out_specs=P(SP_TP, None), check_vma=False
    )
```

```python
import functools

import jax
import jax.numpy as jnp
import numpy as np
from jax import lax
from jax.experimental import pallas as pl
from jax.experimental.pallas import tpu as pltpu
from jax.sharding import Mesh
from jax.sharding import PartitionSpec as P

NOPE_A = 128
VAL_A = 128
NOPE_B = 64
VAL_B = 64
ROPE = 64
SP = ("sp_0", "sp_1", "sp_2")
SP_TP = ("sp_0", "sp_1", "sp_2", "tp")
NZ, NY, NX = 8, 4, 4
TOK = 128
ROWS = TOK + 32
D = 2048
FFD = 768
MESH = pl.DeviceIdType.MESH
LOG2E = 1.4426950408889634
F32 = jnp.float32
BF = jnp.bfloat16


def split3(v):
    hi = v.astype(BF).astype(F32)
    rest = v - hi
    mid = rest.astype(BF).astype(F32)
    return hi, mid, rest - mid


def kernel(
    gain, conv_w, q_hbm, lat_hbm, key_hbm, ew_hbm, gate_hbm, value_hbm, dn_hbm, freq_hbm, resid_hbm, ow_hbm,
    out_ref,
    q_t, lat, key_t, ew, freq, kvb, qb, gv, dn, ow, resid, s_ref, p_ref, macc, mrow, accw, accn,
    part, ob, att, stream, normed, gate, value, act, fp, fr,
    kvz_s, kvz_r, q_s, q_r, gvz_s, gvz_r, gvy_s, gvy_r, dny_s, dny_r, dnz_s, dnz_r,
    pk_s, pk_r, pg_s, pg_r, pd_s, pd_r, o_s, o_r, x_s, x_r, e_s, e_r, h_s, h_r, f_s, f_r, loc,
):
    z = lax.axis_index("sp_0")
    y = lax.axis_index("sp_1")
    c = lax.axis_index("sp_2")
    x = lax.axis_index("tp")
    other = 1 - c

    def zat(k):
        return lax.rem(z + (k + NZ), NZ)

    def yat(k):
        return lax.rem(y + (k + NY), NY)

    def xat(k):
        return lax.rem(x + (k + NX), NX)

    right_z, left_z = {"sp_0": zat(1)}, {"sp_0": zat(-1)}
    right_y, left_y = {"sp_1": yat(1)}, {"sp_1": yat(-1)}
    partner = {"sp_2": other}
    place = (z * NY + y) * 2 + c
    after = lax.rem(place + 1, 64)
    before = lax.rem(place + 63, 64)

    def device_of(i):
        return {"sp_0": i // 8, "sp_1": lax.rem(i // 2, 4), "sp_2": lax.rem(i, 2)}

    def send(src, dst, ssem, rsem, dev):
        pltpu.make_async_remote_copy(
            src_ref=src, dst_ref=dst, send_sem=ssem, recv_sem=rsem, device_id=dev, device_id_type=MESH
        ).start()

    def wait_recv(ref, sem):
        pltpu.make_async_remote_copy(
            src_ref=ref, dst_ref=ref, send_sem=sem, recv_sem=sem, device_id=partner, device_id_type=MESH
        ).wait_recv()

    def wait_send(ref, sem):
        pltpu.make_async_remote_copy(
            src_ref=ref, dst_ref=ref, send_sem=sem, recv_sem=sem, device_id=partner, device_id_type=MESH
        ).wait_send()

    barrier = pltpu.get_barrier_semaphore()
    greeted = [
        partner, right_z, left_z, right_y, left_y, {"sp_1": yat(2)},
        {"tp": xat(1)}, {"tp": xat(2)}, {"tp": xat(3)},
    ]
    greeted += [device_of(i) | {"tp": xat(o)} for i in (after, before) for o in range(NX)]
    for dev in greeted:
        pl.semaphore_signal(barrier, inc=1, device_id=dev, device_id_type=MESH)

    def load(src, dst, i):
        copy = pltpu.make_async_copy(src, dst, loc.at[i])
        copy.start()
        return copy

    first_loads = [
        load(lat_hbm, lat, 0), load(ew_hbm, ew, 1), load(key_hbm, key_t, 2), load(freq_hbm, freq, 3),
        load(q_hbm, q_t, 4),
    ]
    weight_loads = [
        load(gate_hbm, gv.at[z, y, c, pl.ds(0, 32)], 5), load(value_hbm, gv.at[z, y, c, pl.ds(32, 32)], 6),
        load(dn_hbm, dn.at[z, y, c], 7),
    ]
    load_res = load(resid_hbm, resid.at[pl.ds(0, TOK)], 8)
    load_ow = load(ow_hbm, ow, 9)
    pl.semaphore_wait(barrier, len(greeted))
    for copy in first_loads:
        copy.wait()

    position = (lax.broadcasted_iota(jnp.int32, (32, TOK), 1) + place * TOK).astype(F32)
    angles = position * freq[...]
    cosine, sine = jnp.cos(angles), jnp.sin(angles)

    def turned(a, b):
        a, b = a.astype(F32), b.astype(F32)
        return [a * cosine - b * sine, b * cosine + a * sine]

    def upright(pieces):
        return jnp.transpose(jnp.concatenate(pieces, axis=0), (1, 0))

    nothing = jnp.zeros((64, TOK), F32)
    expanded = jnp.dot(lat[...], ew[...], preferred_element_type=F32)
    key_rows = upright(turned(key_t[0:32, :], key_t[32:64, :]) + [nothing])
    low_lane = lax.broadcasted_iota(jnp.int32, (TOK, 128), 1) < 64
    swapped = pltpu.roll(expanded[:, 256:384], 64, 1)
    kvb[0, 0, :, 0:128] = expanded[:, 0:128].astype(BF)
    kvb[0, 0, :, 128:256] = jnp.where(low_lane, key_rows, swapped).astype(BF)
    kvb[0, 0, :, 256:384] = expanded[:, 128:256].astype(BF)
    kvb[0, 0, :, 384:512] = jnp.where(low_lane, swapped, 1.0).astype(BF)
    qb[0, :, 0:128] = upright([q_t[0:128, :].astype(F32)]).astype(BF)
    qb[0, :, 128:256] = upright(turned(q_t[192:224, :], q_t[224:256, :]) + [nothing]).astype(BF)
    qb[0, :, 256:384] = upright(
        turned(q_t[256:288, :], q_t[288:320, :]) + [q_t[128:192, :].astype(F32)]
    ).astype(BF)

    def rows_of(slot, h):
        return kvb.at[slot, 0, pl.ds(64 * h, 64)]

    def slot_of(s, ahead):
        return 0 if s == 0 else 7 if s == 4 else 2 * s - 1 + ahead

    def kv_out(s, h):
        if s < 3 or h == 0:
            send(rows_of(slot_of(s, 0), h), rows_of(slot_of(s + 1, 0), h), kvz_s, kvz_r.at[0, s, h], right_z)
        if s < 3 or h == 1:
            send(rows_of(slot_of(s, 1), h), rows_of(slot_of(s + 1, 1), h), kvz_s, kvz_r.at[1, s, h], left_z)

    def kv_across(slot):
        send(kvb.at[slot, 0], kvb.at[slot, 1], pk_s, pk_r.at[slot], partner)

    def kvz(s, h):
        if s < 4:
            wait_recv(rows_of(slot_of(s, 0), h), kvz_r.at[0, s - 1, h])
            wait_recv(rows_of(slot_of(s, 1), h), kvz_r.at[1, s - 1, h])
            kv_out(s, h)
            if h == 1:
                kv_across(2 * s - 1)
                kv_across(2 * s)
        else:
            wait_recv(rows_of(7, 0), kvz_r.at[0, 3, 0])
            wait_recv(rows_of(7, 1), kvz_r.at[1, 3, 1])
            kv_across(7)

    def q_relay(s):
        if s == 1:
            wait_recv(qb.at[1], q_r.at[0, 0])
            send(qb.at[1, pl.ds(0, 64)], qb.at[3, pl.ds(0, 64)], q_s, q_r.at[0, 1], right_y)
            wait_recv(qb.at[2], q_r.at[1, 0])
            send(qb.at[2, pl.ds(64, 64)], qb.at[3, pl.ds(64, 64)], q_s, q_r.at[1, 1], left_y)
        else:
            wait_recv(qb.at[3, pl.ds(0, 64)], q_r.at[0, 1])
            wait_recv(qb.at[3, pl.ds(64, 64)], q_r.at[1, 1])

    kv_out(0, 0)
    kv_out(0, 1)
    send(qb.at[0], qb.at[1], q_s, q_r.at[0, 0], right_y)
    send(qb.at[0], qb.at[2], q_s, q_r.at[1, 0], left_y)
    kv_across(0)
    macc[...] = jnp.full((2, 512, 128), -3e38, F32)

    def gvz_own():
        own = gv.at[z, y, c]
        send(own, own, gvz_s, gvz_r.at[0, 0], right_z)
        send(own, own, gvz_s, gvz_r.at[1, 0], left_z)

    def dny_own():
        own = dn.at[z, y, c]
        send(own, own, dny_s, dny_r.at[0, 0], right_y)
        send(own, own, dny_s, dny_r.at[1, 0], left_y)

    def gvy_own():
        own = gv.at[z, y, c]
        send(own, own, gvy_s, gvy_r.at[0, 0, 0], right_y)
        send(own, own, gvy_s, gvy_r.at[1, 0, 0], left_y)
        send(own, own, pg_s, pg_r, partner)

    for copy in weight_loads:
        copy.wait()

    offsets = [0, -1, 1, -2, 2, -3, 3, 4]

    def gv_out(zz, j):
        block = gv.at[zz, y, c]
        send(block, block, gvy_s, gvy_r.at[0, 0, j], right_y)
        send(block, block, gvy_s, gvy_r.at[1, 0, j], left_y)
        send(block, block, pg_s, pg_r, partner)

    def gvz(s):
        lo, hi = zat(-s), zat(s)
        if s < 4:
            wait_recv(gv.at[lo, y, c], gvz_r.at[0, s - 1])
            src = gv.at[lo, y, c] if s < 3 else gv.at[lo, y, c, pl.ds(0, 32)]
            send(src, src, gvz_s, gvz_r.at[0, s], right_z)
            wait_recv(gv.at[hi, y, c], gvz_r.at[1, s - 1])
            src = gv.at[hi, y, c] if s < 3 else gv.at[hi, y, c, pl.ds(32, 32)]
            send(src, src, gvz_s, gvz_r.at[1, s], left_z)
            gv_out(lo, 2 * s - 1)
            gv_out(hi, 2 * s)
        else:
            wait_recv(gv.at[lo, y, c, pl.ds(0, 32)], gvz_r.at[0, 3])
            wait_recv(gv.at[lo, y, c, pl.ds(32, 32)], gvz_r.at[1, 3])
            gv_out(lo, 7)

    def gvy(s, j):
        zz = zat(offsets[j])
        a, b, far = yat(-1), yat(1), yat(2)
        if s == 1:
            wait_recv(gv.at[zz, a, c], gvy_r.at[0, 0, j])
            src = gv.at[zz, a, c, pl.ds(0, 32)]
            send(src, src, gvy_s, gvy_r.at[0, 1, j], right_y)
            wait_recv(gv.at[zz, b, c], gvy_r.at[1, 0, j])
            src = gv.at[zz, b, c, pl.ds(32, 32)]
            send(src, src, gvy_s, gvy_r.at[1, 1, j], left_y)
            send(gv.at[zz, a, c], gv.at[zz, a, c], pg_s, pg_r, partner)
            send(gv.at[zz, b, c], gv.at[zz, b, c], pg_s, pg_r, partner)
        else:
            wait_recv(gv.at[zz, far, c, pl.ds(0, 32)], gvy_r.at[0, 1, j])
            wait_recv(gv.at[zz, far, c, pl.ds(32, 32)], gvy_r.at[1, 1, j])
            send(gv.at[zz, far, c], gv.at[zz, far, c], pg_s, pg_r, partner)

    def dny(s):
        a, b, far = yat(-1), yat(1), yat(2)
        if s == 1:
            wait_recv(dn.at[z, a, c], dny_r.at[0, 0])
            src = dn.at[z, a, c, pl.ds(0, 16)]
            send(src, src, dny_s, dny_r.at[0, 1], right_y)
            wait_recv(dn.at[z, b, c], dny_r.at[1, 0])
            src = dn.at[z, b, c, pl.ds(16, 16)]
            send(src, src, dny_s, dny_r.at[1, 1], left_y)
        else:
            wait_recv(dn.at[z, far, c, pl.ds(0, 16)], dny_r.at[0, 1])
            wait_recv(dn.at[z, far, c, pl.ds(16, 16)], dny_r.at[1, 1])

    def dnz(s, r):
        yy = yat((0, -1, 1, 2)[r])
        lo, hi = zat(-s), zat(s)
        if s == 0:
            block = dn.at[z, yy, c]
            send(block, block, dnz_s, dnz_r.at[0, 0, r], right_z)
            send(block, block, dnz_s, dnz_r.at[1, 0, r], left_z)
        elif s < 4:
            wait_recv(dn.at[lo, yy, c], dnz_r.at[0, s - 1, r])
            src = dn.at[lo, yy, c] if s < 3 else dn.at[lo, yy, c, pl.ds(0, 16)]
            send(src, src, dnz_s, dnz_r.at[0, s, r], right_z)
            wait_recv(dn.at[hi, yy, c], dnz_r.at[1, s - 1, r])
            src = dn.at[hi, yy, c] if s < 3 else dn.at[hi, yy, c, pl.ds(16, 16)]
            send(src, src, dnz_s, dnz_r.at[1, s, r], left_z)
        else:
            wait_recv(dn.at[lo, yy, c, pl.ds(0, 16)], dnz_r.at[0, 3, r])
            wait_recv(dn.at[lo, yy, c, pl.ds(16, 16)], dnz_r.at[1, 3, r])
        if r == 3:
            send(dn.at[lo, :, c], dn.at[lo, :, c], pd_s, pd_r.at[slot_of(s, 0)], partner)
            if 0 < s < 4:
                send(dn.at[hi, :, c], dn.at[hi, :, c], pd_s, pd_r.at[slot_of(s, 1)], partner)

    heads = (
        (0, 256, 0, 256, 256, 512, (NOPE_A + ROPE) ** (-0.5) * LOG2E, accw),
        (256, 384, 128, 256, 384, 512, (NOPE_B + ROPE) ** (-0.5) * LOG2E, accn),
    )

    def scores(j):
        wait_recv(kvb.at[j, 1], pk_r.at[j])
        for head in range(2):
            q0, q1, k0, k1 = heads[head][:4]
            qs = qb[:, :, q0:q1].reshape(512, q1 - q0)
            ks = kvb[j, :, :, k0:k1].reshape(256, k1 - k0)
            s = lax.dot_general(qs, ks, (((1,), (1,)), ((), ())), preferred_element_type=F32)
            s_ref[head, j] = s
            macc[head] = jnp.maximum(macc[head], jnp.maximum(s[:, :128], s[:, 128:]))

    def weigh(head):
        v0, v1, factor, acc = heads[head][4:]
        m = jnp.broadcast_to(jnp.max(macc[head], axis=1, keepdims=True), (512, 128))
        mrow[head] = m
        for j in range(NZ):
            for half in range(2):
                s = s_ref[head, j, :, half * 128 : half * 128 + 128]
                at = j * 256 + half * 128
                p_ref[head, :, at : at + 128] = jnp.exp2((s - m) * factor).astype(BF)
        vs = kvb[:, :, :, v0:v1].reshape(2048, v1 - v0)
        acc[...] = jnp.dot(p_ref[head], vs, preferred_element_type=F32)

    def pack():
        def step(b, carry):
            rows = pl.ds(pl.multiple_of(b * TOK, TOK), TOK)
            wide, narrow = accw[rows, :], accn[rows, :]
            lane = lax.broadcasted_iota(jnp.int32, (TOK, 128), 1)
            tile = narrow
            stats = (
                mrow[0, rows, :], mrow[1, rows, :],
                jnp.broadcast_to(wide[:, 192:193], (TOK, 128)), jnp.broadcast_to(narrow[:, 64:65], (TOK, 128)),
            )
            at = 64
            for stat in stats:
                for piece in split3(stat):
                    tile = jnp.where(lane == at, piece, tile)
                    at += 1
            tile = jnp.where(lane >= at, 0.0, tile)
            part[b, :, 0:128] = wide[:, 0:128].astype(BF)
            part[b, :, 128:256] = tile.astype(BF)
            return carry

        lax.fori_loop(0, NY, step, 0)

    def merge():
        ob[0] = part[0]

        def stat(g, at):
            t = ob[g, :, 128:256].astype(F32)
            return t[:, at : at + 1] + t[:, at + 1 : at + 2] + t[:, at + 2 : at + 3]

        for head in range(2):
            factor = heads[head][6]
            ms = [stat(g, 64 + 3 * head) for g in range(NY)]
            top = jnp.maximum(jnp.maximum(ms[0], ms[1]), jnp.maximum(ms[2], ms[3]))
            lanes = slice(0, 128) if head == 0 else slice(128, 256)
            total = jnp.zeros((TOK, 1), F32)
            value_sum = jnp.zeros((TOK, 128), F32)
            for g in range(NY):
                share = jnp.exp2((ms[g] - top) * factor)
                total = total + share * stat(g, 70 + 3 * head)
                value_sum = value_sum + share * ob[g, :, lanes].astype(F32)
            att[x, 0:TOK, lanes] = (value_sum / total).astype(BF)

    def part_out():
        send(part.at[3], ob.at[3], o_s, o_r.at[2], {"sp_1": yat(2)})
        send(part.at[1], ob.at[2], o_s, o_r.at[1], left_y)
        send(part.at[2], ob.at[1], o_s, o_r.at[0], right_y)

    def part_in():
        for o in (1, 2, 3):
            wait_recv(ob.at[o], o_r.at[o - 1])

    def att_out():
        for o in (2, 1, 3):
            mine = att.at[x, pl.ds(0, TOK)]
            send(mine, mine, x_s, x_r.at[o - 1], {"tp": xat(o)})
        for o in range(NX):
            peer = {"tp": xat(o)}
            send(att.at[x, pl.ds(112, 16)], att.at[x, pl.ds(128, 16)], e_s, e_r.at[0, o], device_of(after) | peer)
            send(att.at[x, pl.ds(0, 16)], att.at[x, pl.ds(144, 16)], e_s, e_r.at[1, o], device_of(before) | peer)

    gvz_own()
    dny_own()
    gvy_own()
    load_res.wait()
    send(resid.at[pl.ds(112, 16)], resid.at[pl.ds(128, 16)], h_s, h_r.at[0], device_of(after))
    send(resid.at[pl.ds(0, 16)], resid.at[pl.ds(144, 16)], h_s, h_r.at[1], device_of(before))
    q_relay(1)
    kvz(1, 0)
    dny(1)
    kvz(1, 1)
    gvy(1, 0)
    gvz(1)
    q_relay(2)
    scores(0)
    scores(1)
    dny(2)
    scores(2)
    kvz(2, 0)
    gvy(2, 0)
    kvz(2, 1)
    gvy(1, 1)
    scores(3)
    scores(4)
    gvz(2)
    kvz(3, 0)
    gvy(2, 1)
    kvz(3, 1)
    dnz(0, 1)
    dnz(0, 0)
    gvy(1, 2)
    dnz(0, 2)
    scores(5)
    scores(6)
    gvz(3)
    kvz(4, 0)
    gvy(1, 3)
    dnz(0, 3)
    gvy(2, 2)
    dnz(1, 1)
    scores(7)
    weigh(0)
    weigh(1)
    pack()
    part_out()
    dnz(1, 2)
    dnz(1, 0)
    gvz(4)
    gvy(1, 4)
    gvy(1, 5)
    gvy(1, 6)
    dnz(1, 3)
    gvy(2, 3)
    dnz(2, 1)
    dnz(2, 2)
    part_in()
    merge()
    att_out()
    dnz(2, 0)
    dnz(2, 3)
    gvy(1, 7)
    dnz(3, 1)
    gvy(2, 4)
    dnz(3, 2)
    gvy(2, 5)
    dnz(3, 0)
    load_ow.wait()
    wait_recv(resid.at[pl.ds(128, 16)], h_r.at[0])
    wait_recv(resid.at[pl.ds(144, 16)], h_r.at[1])
    for o in (2, 1, 3):
        wait_recv(att.at[xat(-o), pl.ds(0, TOK)], x_r.at[o - 1])
    for o in range(NX):
        wait_recv(att.at[xat(-o), pl.ds(128, 16)], e_r.at[0, o])
        wait_recv(att.at[xat(-o), pl.ds(144, 16)], e_r.at[1, o])

    ss = jnp.zeros((ROWS, 1), F32)
    for n in range(8):
        cols = slice(n * 256, n * 256 + 256)
        total = resid[:, cols].astype(F32)
        for h in range(NX):
            total = total + jnp.dot(att[h, :, 0:192], ow[h * 192 : h * 192 + 192, cols], preferred_element_type=F32)
        rounded = total.astype(BF)
        stream[:, cols] = rounded
        wide = rounded.astype(F32)
        ss = ss + jnp.sum(wide * wide, axis=1, keepdims=True)
    scale = lax.rsqrt(ss * (1.0 / D) + 1e-06)
    for n in range(8):
        cols = slice(n * 256, n * 256 + 256)
        scaled = stream[:, cols].astype(F32) * scale
        normed[:, cols] = (scaled * gain[cols].astype(F32).reshape(1, 256)).astype(BF)
    gvy(2, 6)
    dnz(3, 3)
    gvy(2, 7)
    wait_recv(gv.at[:, :, other], pg_r)

    def up(lo, rows, dst):
        for n in range(3):
            cols = slice(n * 256, n * 256 + 256)
            w = gv[:, :, :, lo : lo + 32, cols].reshape(D, 256)
            dst[:, cols] = jnp.dot(normed[0:rows], w, preferred_element_type=F32).astype(BF)

    up(0, ROWS, gate)
    up(32, TOK, value)

    row = lax.broadcasted_iota(jnp.int32, (TOK, 256), 0)
    for n in range(3):
        cols = slice(n * 256, n * 256 + 256)
        g = gate[0:TOK, cols].astype(F32)
        edge = gate[TOK:ROWS, cols].astype(F32)
        first = jnp.where(place > 0, edge[15:16], 0.0)
        last = jnp.where(place < 63, edge[16:17], 0.0)
        low = jnp.where(row == 0, first, pltpu.roll(g, 1, 0))
        high = jnp.where(row == TOK - 1, last, pltpu.roll(g, TOK - 1, 0))
        cw = conv_w[:, cols].astype(F32)
        mixed = low * cw[0:1] + g * cw[1:2] + high * cw[2:3]
        silu = mixed / (1.0 + jnp.exp(-mixed))
        act[:, cols] = (silu * value[:, cols].astype(F32)).astype(BF)

    for j in range(NZ):
        zz = zat(offsets[j])
        if j == 7:
            for r in range(NY):
                dnz(4, r)
        wait_recv(dn.at[zz, :, other], pd_r.at[j])
        w = dn[zz].reshape(256, FFD)
        d = lax.dot_general(act[...], w, (((1,), (1,)), ((), ())), preferred_element_type=F32)
        fp[j] = d.astype(BF).reshape(NX, 32, 256)
        for o in (2, 1, 3):
            peer = xat(o)
            send(fp.at[j, peer], fr.at[j, x], f_s, f_r.at[j, o - 1], {"tp": peer})

    rows = pl.ds(pl.multiple_of(x * 32, 32), 32)
    for j in range(NZ):
        cols = pl.ds(pl.multiple_of(zat(offsets[j]) * 256, 256), 256)
        total = stream[rows, cols].astype(F32) + fp[j, x].astype(F32)
        for o in (1, 3, 2):
            wait_recv(fr.at[j, xat(-o)], f_r.at[j, o - 1])
            total = total + fr[j, xat(-o)].astype(F32)
        out_ref[:, cols] = total.astype(BF)

    wait_send(kvb.at[pl.ds(0, 7), 0], kvz_s)
    wait_send(qb.at[pl.ds(0, 3)], q_s)
    wait_send(gv.at[pl.ds(0, 7), 0, 0], gvz_s)
    wait_send(gv.at[:, pl.ds(0, 3), 0], gvy_s)
    wait_send(dn.at[0, pl.ds(0, 3), 0], dny_s)
    wait_send(dn.at[pl.ds(0, 7), :, 0], dnz_s)
    wait_send(kvb.at[:, 0], pk_s)
    wait_send(gv.at[:, :, 0], pg_s)
    wait_send(dn.at[:, :, 0], pd_s)
    wait_send(part.at[pl.ds(0, 3)], o_s)
    wait_send(att.at[pl.ds(0, 3), pl.ds(0, TOK)], x_s)
    wait_send(att.at[:, pl.ds(0, 32)], e_s)
    wait_send(resid.at[pl.ds(0, 32)], h_s)
    wait_send(fp.at[:, pl.ds(0, 3)], f_s)


def layer(*operands):
    vmem = pl.BlockSpec(memory_space=pltpu.VMEM)
    hbm = pl.BlockSpec(memory_space=pltpu.HBM)
    dma = pltpu.SemaphoreType.DMA
    scratch = [
        pltpu.VMEM((320, TOK), BF),
        pltpu.VMEM((TOK, 512), BF),
        pltpu.VMEM((64, TOK), BF),
        pltpu.VMEM((512, 384), BF),
        pltpu.VMEM((32, TOK), F32),
        pltpu.VMEM((NZ, 2, TOK, 512), BF),
        pltpu.VMEM((NY, TOK, 384), BF),
        pltpu.VMEM((NZ, NY, 2, 64, FFD), BF),
        pltpu.VMEM((NZ, NY, 2, 32, FFD), BF),
        pltpu.VMEM((768, D), BF),
        pltpu.VMEM((ROWS, D), BF),
        pltpu.VMEM((2, NZ, 512, 256), F32),
        pltpu.VMEM((2, 512, 2048), BF),
        pltpu.VMEM((2, 512, 128), F32),
        pltpu.VMEM((2, 512, 128), F32),
        pltpu.VMEM((512, 256), F32),
        pltpu.VMEM((512, 128), F32),
        pltpu.VMEM((NY, TOK, 256), BF),
        pltpu.VMEM((NY, TOK, 256), BF),
        pltpu.VMEM((NX, ROWS, 256), BF),
        pltpu.VMEM((ROWS, D), BF),
        pltpu.VMEM((ROWS, D), BF),
        pltpu.VMEM((ROWS, FFD), BF),
        pltpu.VMEM((TOK, FFD), BF),
        pltpu.VMEM((TOK, FFD), BF),
        pltpu.VMEM((NZ, NX, 32, 256), BF),
        pltpu.VMEM((NZ, NX, 32, 256), BF),
        dma, dma((2, 4, 2)), dma, dma((2, 2)), dma, dma((2, 4)), dma, dma((2, 2, 8)),
        dma, dma((2, 2)), dma, dma((2, 4, 4)),
        dma, dma((8,)), dma, dma, dma, dma((8,)), dma, dma((3,)), dma, dma((3,)), dma, dma((2, 4)), dma, dma((2,)),
        dma, dma((NZ, 3)), dma((10,)),
    ]
    return pl.pallas_call(
        kernel,
        out_shape=pltpu.VMEM((32, D), BF),
        in_specs=[vmem] * 2 + [hbm] * 10,
        out_specs=vmem,
        scratch_shapes=scratch,
        compiler_params=pltpu.CompilerParams(collective_id=0, has_side_effects=True),
    )(*operands)


def body(
    queries, latents, shared_key, expand_weight, residual, out_weight,
    norm_gain, gate_weight, value_weight, conv_weight, down_weight,
):
    frequency = (10000.0 ** (-np.arange(ROPE // 2) / (ROPE // 2))).astype(np.float32)
    return layer(
        norm_gain, conv_weight, queries.T, latents, shared_key.T, expand_weight, gate_weight, value_weight,
        down_weight.T, np.ascontiguousarray(np.broadcast_to(frequency[:, None], (ROPE // 2, TOK))),
        residual, out_weight,
    )


def solution(mesh):
    split = Mesh(mesh.devices.reshape(NZ, NY, 2, mesh.shape["tp"]), ("sp_0", "sp_1", "sp_2", "tp"))
    placed = (
        P(SP, "tp"),
        P(SP, None),
        P(SP, None),
        P(None, "tp"),
        P(SP, None),
        P(),
        P(),
        P(SP, "tp"),
        P(SP, "tp"),
        P(None, "tp"),
        P("tp", SP),
    )
    return jax.shard_map(
        body, mesh=split, in_specs=placed, out_specs=P(SP_TP, None), check_vma=False
    )
```

```python
import functools

import jax
import jax.numpy as jnp
import numpy as np
from jax import lax
from jax.experimental import pallas as pl
from jax.experimental.pallas import tpu as pltpu
from jax.sharding import Mesh
from jax.sharding import PartitionSpec as P

NOPE_A = 128
VAL_A = 128
NOPE_B = 64
VAL_B = 64
ROPE = 64
SP = ("sp_0", "sp_1", "sp_2")
SP_TP = ("sp_0", "sp_1", "sp_2", "tp")
NZ, NY, NX = 8, 4, 4
TOK = 128
ROWS = TOK + 32
D = 2048
FFD = 768
MESH = pl.DeviceIdType.MESH
LOG2E = 1.4426950408889634
F32 = jnp.float32
BF = jnp.bfloat16


def split3(v):
    hi = v.astype(BF).astype(F32)
    rest = v - hi
    mid = rest.astype(BF).astype(F32)
    return hi, mid, rest - mid


def kernel(
    gain, conv_w, q_hbm, lat_hbm, key_hbm, ew_hbm, gate_hbm, value_hbm, dn_hbm, freq_hbm, resid_hbm, ow_hbm,
    out_ref,
    q_t, lat, key_t, ew, freq, kvb, qb, gv, dn, ow, resid, s_ref, p_ref, macc, mrow, accw, accn,
    part, ob, att, stream, normed, gacc, vacc, gate, value, act, fp, fr,
    kvz_s, kvz_r, q_s, q_r, gvz_s, gvz_r, gvy_s, gvy_r, dny_s, dny_r, dnz_s, dnz_r,
    pk_s, pk_r, pg_s, pg_r, pd_s, pd_r, o_s, o_r, x_s, x_r, e_s, e_r, h_s, h_r, f_s, f_r, loc,
):
    z = lax.axis_index("sp_0")
    y = lax.axis_index("sp_1")
    c = lax.axis_index("sp_2")
    x = lax.axis_index("tp")
    other = 1 - c

    def zat(k):
        return lax.rem(z + (k + NZ), NZ)

    def yat(k):
        return lax.rem(y + (k + NY), NY)

    def xat(k):
        return lax.rem(x + (k + NX), NX)

    right_z, left_z = {"sp_0": zat(1)}, {"sp_0": zat(-1)}
    right_y, left_y = {"sp_1": yat(1)}, {"sp_1": yat(-1)}
    partner = {"sp_2": other}
    place = (z * NY + y) * 2 + c
    after = lax.rem(place + 1, 64)
    before = lax.rem(place + 63, 64)

    def device_of(i):
        return {"sp_0": i // 8, "sp_1": lax.rem(i // 2, 4), "sp_2": lax.rem(i, 2)}

    def send(src, dst, ssem, rsem, dev):
        pltpu.make_async_remote_copy(
            src_ref=src, dst_ref=dst, send_sem=ssem, recv_sem=rsem, device_id=dev, device_id_type=MESH
        ).start()

    def wait_recv(ref, sem):
        pltpu.make_async_remote_copy(
            src_ref=ref, dst_ref=ref, send_sem=sem, recv_sem=sem, device_id=partner, device_id_type=MESH
        ).wait_recv()

    def wait_send(ref, sem):
        pltpu.make_async_remote_copy(
            src_ref=ref, dst_ref=ref, send_sem=sem, recv_sem=sem, device_id=partner, device_id_type=MESH
        ).wait_send()

    barrier = pltpu.get_barrier_semaphore()
    greeted = [
        partner, right_z, left_z, right_y, left_y, {"sp_1": yat(2)},
        {"tp": xat(1)}, {"tp": xat(2)}, {"tp": xat(3)},
    ]
    greeted += [device_of(i) | {"tp": xat(o)} for i in (after, before) for o in range(NX)]
    for dev in greeted:
        pl.semaphore_signal(barrier, inc=1, device_id=dev, device_id_type=MESH)

    def load(src, dst, i):
        copy = pltpu.make_async_copy(src, dst, loc.at[i])
        copy.start()
        return copy

    first_loads = [
        load(lat_hbm, lat, 0), load(ew_hbm, ew, 1), load(key_hbm, key_t, 2), load(freq_hbm, freq, 3),
        load(q_hbm, q_t, 4),
    ]
    weight_loads = [
        load(gate_hbm, gv.at[z, y, c, pl.ds(0, 32)], 5), load(value_hbm, gv.at[z, y, c, pl.ds(32, 32)], 6),
        load(dn_hbm, dn.at[z, y, c], 7),
    ]
    load_res = load(resid_hbm, resid.at[pl.ds(0, TOK)], 8)
    load_ow = load(ow_hbm, ow, 9)
    pl.semaphore_wait(barrier, len(greeted))
    for copy in first_loads:
        copy.wait()

    position = (lax.broadcasted_iota(jnp.int32, (32, TOK), 1) + place * TOK).astype(F32)
    angles = position * freq[...]
    cosine, sine = jnp.cos(angles), jnp.sin(angles)

    def turned(a, b):
        a, b = a.astype(F32), b.astype(F32)
        return [a * cosine - b * sine, b * cosine + a * sine]

    def upright(pieces):
        return jnp.transpose(jnp.concatenate(pieces, axis=0), (1, 0))

    nothing = jnp.zeros((64, TOK), F32)
    expanded = jnp.dot(lat[...], ew[...], preferred_element_type=F32)
    key_rows = upright(turned(key_t[0:32, :], key_t[32:64, :]) + [nothing])
    low_lane = lax.broadcasted_iota(jnp.int32, (TOK, 128), 1) < 64
    swapped = pltpu.roll(expanded[:, 256:384], 64, 1)
    kvb[0, 0, :, 0:128] = expanded[:, 0:128].astype(BF)
    kvb[0, 0, :, 128:256] = jnp.where(low_lane, key_rows, swapped).astype(BF)
    kvb[0, 0, :, 256:384] = expanded[:, 128:256].astype(BF)
    kvb[0, 0, :, 384:512] = jnp.where(low_lane, swapped, 1.0).astype(BF)
    qb[3, :, 0:128] = upright([q_t[0:128, :].astype(F32)]).astype(BF)
    qb[3, :, 128:256] = upright(turned(q_t[192:224, :], q_t[224:256, :]) + [nothing]).astype(BF)
    qb[3, :, 256:384] = upright(
        turned(q_t[256:288, :], q_t[288:320, :]) + [q_t[128:192, :].astype(F32)]
    ).astype(BF)

    def rows_of(slot, h):
        return kvb.at[slot, 0, pl.ds(32 * h, 32)]

    def slot_of(s, ahead):
        return 0 if s == 0 else 7 if s == 4 else 2 * s - 1 + ahead

    def kv_out(s, h):
        if s < 3 or h < 2:
            send(rows_of(slot_of(s, 0), h), rows_of(slot_of(s + 1, 0), h), kvz_s, kvz_r.at[0, s, h], right_z)
        if s < 3 or h >= 2:
            send(rows_of(slot_of(s, 1), h), rows_of(slot_of(s + 1, 1), h), kvz_s, kvz_r.at[1, s, h], left_z)

    def kv_across(slot):
        send(kvb.at[slot, 0], kvb.at[slot, 1], pk_s, pk_r.at[slot], partner)

    def kvz(s, h):
        if s < 4:
            wait_recv(rows_of(slot_of(s, 0), h), kvz_r.at[0, s - 1, h])
            wait_recv(rows_of(slot_of(s, 1), h), kvz_r.at[1, s - 1, h])
            kv_out(s, h)
            if h == 3:
                kv_across(2 * s - 1)
                kv_across(2 * s)
        else:
            for q in range(4):
                wait_recv(rows_of(7, q), kvz_r.at[q // 2, 3, q])
            kv_across(7)

    def q_relay(s):
        if s == 1:
            wait_recv(qb.at[1], q_r.at[0, 0])
            send(qb.at[1, pl.ds(0, 64)], qb.at[0, pl.ds(0, 64)], q_s, q_r.at[0, 1], right_y)
            wait_recv(qb.at[2], q_r.at[1, 0])
            send(qb.at[2, pl.ds(64, 64)], qb.at[0, pl.ds(64, 64)], q_s, q_r.at[1, 1], left_y)
        else:
            wait_recv(qb.at[0, pl.ds(0, 64)], q_r.at[0, 1])
            wait_recv(qb.at[0, pl.ds(64, 64)], q_r.at[1, 1])

    for q in range(4):
        kv_out(0, q)
    send(qb.at[3], qb.at[1], q_s, q_r.at[0, 0], right_y)
    send(qb.at[3], qb.at[2], q_s, q_r.at[1, 0], left_y)
    kv_across(0)
    macc[...] = jnp.full((2, 512, 128), -3e38, F32)

    def gvz_own():
        own = gv.at[z, y, c]
        send(own, own, gvz_s, gvz_r.at[0, 0], right_z)
        send(own, own, gvz_s, gvz_r.at[1, 0], left_z)

    def dny_own():
        own = dn.at[z, y, c]
        send(own, own, dny_s, dny_r.at[0, 0], right_y)
        send(own, own, dny_s, dny_r.at[1, 0], left_y)

    def gvy_own():
        own = gv.at[z, y, c]
        send(own, own, gvy_s, gvy_r.at[0, 0, 0], right_y)
        send(own, own, gvy_s, gvy_r.at[1, 0, 0], left_y)
        send(own, own, pg_s, pg_r.at[0], partner)

    for copy in weight_loads:
        copy.wait()

    offsets = [0, -1, 1, -2, 2, -3, 3, 4]

    def gv_out(zz, j):
        block = gv.at[zz, y, c]
        send(block, block, gvy_s, gvy_r.at[0, 0, j], right_y)
        send(block, block, gvy_s, gvy_r.at[1, 0, j], left_y)
        send(block, block, pg_s, pg_r.at[j], partner)

    def gvz(s):
        lo, hi = zat(-s), zat(s)
        if s < 4:
            wait_recv(gv.at[lo, y, c], gvz_r.at[0, s - 1])
            src = gv.at[lo, y, c] if s < 3 else gv.at[lo, y, c, pl.ds(0, 32)]
            send(src, src, gvz_s, gvz_r.at[0, s], right_z)
            wait_recv(gv.at[hi, y, c], gvz_r.at[1, s - 1])
            src = gv.at[hi, y, c] if s < 3 else gv.at[hi, y, c, pl.ds(32, 32)]
            send(src, src, gvz_s, gvz_r.at[1, s], left_z)
            gv_out(lo, 2 * s - 1)
            gv_out(hi, 2 * s)
        else:
            wait_recv(gv.at[lo, y, c, pl.ds(0, 32)], gvz_r.at[0, 3])
            wait_recv(gv.at[lo, y, c, pl.ds(32, 32)], gvz_r.at[1, 3])
            gv_out(lo, 7)

    def gvy(s, j):
        zz = zat(offsets[j])
        a, b, far = yat(-1), yat(1), yat(2)
        if s == 1:
            wait_recv(gv.at[zz, a, c], gvy_r.at[0, 0, j])
            src = gv.at[zz, a, c, pl.ds(0, 32)]
            send(src, src, gvy_s, gvy_r.at[0, 1, j], right_y)
            wait_recv(gv.at[zz, b, c], gvy_r.at[1, 0, j])
            src = gv.at[zz, b, c, pl.ds(32, 32)]
            send(src, src, gvy_s, gvy_r.at[1, 1, j], left_y)
            send(gv.at[zz, a, c], gv.at[zz, a, c], pg_s, pg_r.at[j], partner)
            send(gv.at[zz, b, c], gv.at[zz, b, c], pg_s, pg_r.at[j], partner)
        else:
            wait_recv(gv.at[zz, far, c, pl.ds(0, 32)], gvy_r.at[0, 1, j])
            wait_recv(gv.at[zz, far, c, pl.ds(32, 32)], gvy_r.at[1, 1, j])
            send(gv.at[zz, far, c], gv.at[zz, far, c], pg_s, pg_r.at[j], partner)

    def dny(s):
        a, b, far = yat(-1), yat(1), yat(2)
        if s == 1:
            wait_recv(dn.at[z, a, c], dny_r.at[0, 0])
            src = dn.at[z, a, c, pl.ds(0, 16)]
            send(src, src, dny_s, dny_r.at[0, 1], right_y)
            wait_recv(dn.at[z, b, c], dny_r.at[1, 0])
            src = dn.at[z, b, c, pl.ds(16, 16)]
            send(src, src, dny_s, dny_r.at[1, 1], left_y)
        else:
            wait_recv(dn.at[z, far, c, pl.ds(0, 16)], dny_r.at[0, 1])
            wait_recv(dn.at[z, far, c, pl.ds(16, 16)], dny_r.at[1, 1])

    def dnz(s, r):
        yy = yat((0, -1, 1, 2)[r])
        lo, hi = zat(-s), zat(s)
        if s == 0:
            block = dn.at[z, yy, c]
            send(block, block, dnz_s, dnz_r.at[0, 0, r], right_z)
            send(block, block, dnz_s, dnz_r.at[1, 0, r], left_z)
        elif s < 4:
            wait_recv(dn.at[lo, yy, c], dnz_r.at[0, s - 1, r])
            src = dn.at[lo, yy, c] if s < 3 else dn.at[lo, yy, c, pl.ds(0, 16)]
            send(src, src, dnz_s, dnz_r.at[0, s, r], right_z)
            wait_recv(dn.at[hi, yy, c], dnz_r.at[1, s - 1, r])
            src = dn.at[hi, yy, c] if s < 3 else dn.at[hi, yy, c, pl.ds(16, 16)]
            send(src, src, dnz_s, dnz_r.at[1, s, r], left_z)
        else:
            wait_recv(dn.at[lo, yy, c, pl.ds(0, 16)], dnz_r.at[0, 3, r])
            wait_recv(dn.at[lo, yy, c, pl.ds(16, 16)], dnz_r.at[1, 3, r])
        send(dn.at[lo, yy, c], dn.at[lo, yy, c], pd_s, pd_r.at[slot_of(s, 0)], partner)
        if 0 < s < 4:
            send(dn.at[hi, yy, c], dn.at[hi, yy, c], pd_s, pd_r.at[slot_of(s, 1)], partner)

    heads = (
        (0, 256, 0, 256, 256, 512, (NOPE_A + ROPE) ** (-0.5) * LOG2E, accw),
        (256, 384, 128, 256, 384, 512, (NOPE_B + ROPE) ** (-0.5) * LOG2E, accn),
    )

    def scores(j):
        wait_recv(kvb.at[j, 1], pk_r.at[j])
        for head in range(2):
            q0, q1, k0, k1 = heads[head][:4]
            qs = qb[:, :, q0:q1].reshape(512, q1 - q0)
            ks = kvb[j, :, :, k0:k1].reshape(256, k1 - k0)
            s = lax.dot_general(qs, ks, (((1,), (1,)), ((), ())), preferred_element_type=F32)
            s_ref[head, j] = s
            macc[head] = jnp.maximum(macc[head], jnp.maximum(s[:, :128], s[:, 128:]))

    def weigh(half):
        rows = slice(256 * half, 256 * half + 256)
        for head in range(2):
            v0, v1, factor, acc = heads[head][4:]
            m = jnp.broadcast_to(jnp.max(macc[head, rows], axis=1, keepdims=True), (256, 128))
            mrow[head, rows] = m
            for j in range(NZ):
                for side in range(2):
                    s = s_ref[head, j, rows, side * 128 : side * 128 + 128]
                    at = j * 256 + side * 128
                    p_ref[head, :, at : at + 128] = jnp.exp2((s - m) * factor).astype(BF)
            vs = kvb[:, :, :, v0:v1].reshape(2048, v1 - v0)
            acc[rows] = jnp.dot(p_ref[head], vs, preferred_element_type=F32)

    lane = lax.broadcasted_iota(jnp.int32, (TOK, 128), 1)

    def pack(half):
        for b in (2 * half, 2 * half + 1):
            rows = slice(b * TOK, b * TOK + TOK)
            wide, narrow = accw[rows, :], accn[rows, :]
            tile = narrow
            stats = (
                mrow[0, rows, :], mrow[1, rows, :],
                jnp.broadcast_to(wide[:, 192:193], (TOK, 128)), jnp.broadcast_to(narrow[:, 64:65], (TOK, 128)),
            )
            at = 64
            for stat in stats:
                for piece in split3(stat):
                    tile = jnp.where(lane == at, piece, tile)
                    at += 1
            tile = jnp.where(lane >= at, 0.0, tile)
            part[b, :, 0:128] = wide[:, 0:128].astype(BF)
            part[b, :, 128:256] = tile.astype(BF)
        if half == 0:
            send(part.at[0], ob.at[0], o_s, o_r.at[0], {"sp_1": yat(2)})
            send(part.at[1], ob.at[2], o_s, o_r.at[2], left_y)
        else:
            send(part.at[2], ob.at[1], o_s, o_r.at[1], right_y)

    def merge():
        blocks = [part.at[3]] + [ob.at[g] for g in range(3)]
        tiles = [block[:, 128:256].astype(F32) for block in blocks]
        stats = [s + pltpu.roll(s, 127, 1) + pltpu.roll(s, 126, 1) for s in tiles]
        top = jnp.maximum(jnp.maximum(stats[0], stats[1]), jnp.maximum(stats[2], stats[3]))
        factor = jnp.where(lane == 64, heads[0][6], heads[1][6])
        shares = [jnp.exp2((s - top) * factor) for s in stats]
        total = sum(pltpu.roll(w, 6, 1) * s for w, s in zip(shares, stats))
        inverse = pltpu.roll(1.0 / total, 122, 1)
        shares = [w * inverse for w in shares]
        wide = sum(w[:, 64:65] * block[:, 0:128].astype(F32) for w, block in zip(shares, blocks))
        narrow = sum(w[:, 67:68] * s for w, s in zip(shares, tiles))
        att[x, 0:TOK, 0:128] = wide.astype(BF)
        att[x, 0:TOK, 128:256] = narrow.astype(BF)

    def part_in():
        for o in range(3):
            wait_recv(ob.at[o], o_r.at[o])

    def att_out():
        for o in (2, 1, 3):
            mine = att.at[x, pl.ds(0, TOK)]
            send(mine, mine, x_s, x_r.at[o - 1], {"tp": xat(o)})
        for o in range(NX):
            peer = {"tp": xat(o)}
            send(att.at[x, pl.ds(112, 16)], att.at[x, pl.ds(128, 16)], e_s, e_r.at[0, o], device_of(after) | peer)
            send(att.at[x, pl.ds(0, 16)], att.at[x, pl.ds(144, 16)], e_s, e_r.at[1, o], device_of(before) | peer)

    def edges_out():
        load_res.wait()
        send(resid.at[pl.ds(112, 16)], resid.at[pl.ds(128, 16)], h_s, h_r.at[0], device_of(after))
        send(resid.at[pl.ds(0, 16)], resid.at[pl.ds(144, 16)], h_s, h_r.at[1], device_of(before))

    edges_out()
    gvy_own()
    gvz_own()
    kvz(1, 0)
    q_relay(1)
    kvz(1, 1)
    dny_own()
    kvz(1, 2)
    kvz(1, 3)
    gvy(1, 0)
    gvz(1)
    q_relay(2)
    scores(0)
    scores(1)
    kvz(2, 0)
    scores(2)
    dny(1)
    kvz(2, 1)
    kvz(2, 2)
    gvy(2, 0)
    kvz(2, 3)
    scores(3)
    gvz(2)
    scores(4)
    kvz(3, 0)
    kvz(3, 1)
    gvy(1, 2)
    kvz(3, 2)
    dny(2)
    gvy(1, 1)
    kvz(3, 3)
    dnz(0, 2)
    dnz(0, 3)
    dnz(0, 0)
    scores(5)
    gvz(3)
    scores(6)
    kvz(4, 0)
    dnz(0, 1)
    dnz(1, 2)
    gvy(2, 2)
    scores(7)
    weigh(0)
    dnz(1, 0)
    dnz(1, 3)
    gvy(2, 1)
    pack(0)
    weigh(1)
    pack(1)
    gvz(4)
    gvy(1, 5)
    dnz(1, 1)
    gvy(1, 3)
    gvy(1, 4)
    dnz(2, 2)
    gvy(1, 6)
    dnz(2, 0)
    dnz(2, 3)
    part_in()
    merge()
    att_out()
    dnz(2, 1)
    dnz(3, 2)
    gvy(1, 7)
    dnz(3, 0)
    gvy(2, 5)
    dnz(3, 3)
    gvy(2, 3)
    dnz(3, 1)
    load_ow.wait()
    wait_recv(resid.at[pl.ds(128, 16)], h_r.at[0])
    wait_recv(resid.at[pl.ds(144, 16)], h_r.at[1])
    for o in (2, 1, 3):
        wait_recv(att.at[xat(-o), pl.ds(0, TOK)], x_r.at[o - 1])
    for o in range(NX):
        wait_recv(att.at[xat(-o), pl.ds(128, 16)], e_r.at[0, o])
        wait_recv(att.at[xat(-o), pl.ds(144, 16)], e_r.at[1, o])

    ss = jnp.zeros((ROWS, 1), F32)
    for n in range(8):
        cols = slice(n * 256, n * 256 + 256)
        total = resid[:, cols].astype(F32)
        for h in range(NX):
            total = total + jnp.dot(att[h, :, 0:192], ow[h * 192 : h * 192 + 192, cols], preferred_element_type=F32)
        rounded = total.astype(BF)
        stream[:, cols] = rounded
        wide = rounded.astype(F32)
        ss = ss + jnp.sum(wide * wide, axis=1, keepdims=True)
    scale = lax.rsqrt(ss * (1.0 / D) + 1e-06)
    for n in range(8):
        cols = slice(n * 256, n * 256 + 256)
        scaled = stream[:, cols].astype(F32) * scale
        normed[n] = (scaled * gain[cols].astype(F32).reshape(1, 256)).astype(BF)
    gvy(2, 4)
    gvy(2, 6)

    def up(lo, rows, js, acc, n):
        cols = slice(n * 256, n * 256 + 256)
        total = None
        for j in js:
            zz = zat(offsets[j])
            w = gv[zz, :, :, lo : lo + 32, cols].reshape(256, 256)
            term = jnp.dot(normed[zz, 0:rows], w, preferred_element_type=F32)
            total = term if total is None else total + term
        return total if acc is None else acc[:, cols] + total

    def up_first():
        for j in range(7):
            wait_recv(gv.at[zat(offsets[j]), :, other], pg_r.at[j])
        for n in range(3):
            cols = slice(n * 256, n * 256 + 256)
            gacc[:, cols] = up(0, ROWS, range(7), None, n)
            vacc[:, cols] = up(32, TOK, range(7), None, n)

    def up_last():
        wait_recv(gv.at[zat(offsets[7]), :, other], pg_r.at[7])
        for n in range(3):
            cols = slice(n * 256, n * 256 + 256)
            gate[:, cols] = up(0, ROWS, (7,), gacc, n).astype(BF)
            value[:, cols] = up(32, TOK, (7,), vacc, n).astype(BF)

    up_first()
    gvy(2, 7)
    up_last()

    row = lax.broadcasted_iota(jnp.int32, (TOK, 256), 0)
    for n in range(3):
        cols = slice(n * 256, n * 256 + 256)
        g = gate[0:TOK, cols].astype(F32)
        edge = gate[TOK:ROWS, cols].astype(F32)
        first = jnp.where(place > 0, edge[15:16], 0.0)
        last = jnp.where(place < 63, edge[16:17], 0.0)
        low = jnp.where(row == 0, first, pltpu.roll(g, 1, 0))
        high = jnp.where(row == TOK - 1, last, pltpu.roll(g, TOK - 1, 0))
        cw = conv_w[:, cols].astype(F32)
        mixed = low * cw[0:1] + g * cw[1:2] + high * cw[2:3]
        silu = mixed / (1.0 + jnp.exp(-mixed))
        act[:, cols] = (silu * value[:, cols].astype(F32)).astype(BF)

    for j in range(NZ):
        zz = zat(offsets[j])
        if j == 7:
            for r in range(NY):
                dnz(4, r)
        wait_recv(dn.at[zz, :, other], pd_r.at[j])
        w = dn[zz].reshape(256, FFD)
        d = lax.dot_general(act[...], w, (((1,), (1,)), ((), ())), preferred_element_type=F32)
        fp[j] = d.astype(BF).reshape(NX, 32, 256)
        for o in (2, 1, 3):
            peer = xat(o)
            send(fp.at[j, peer], fr.at[j, x], f_s, f_r.at[j, o - 1], {"tp": peer})

    rows = pl.ds(pl.multiple_of(x * 32, 32), 32)
    for j in range(NZ):
        cols = pl.ds(pl.multiple_of(zat(offsets[j]) * 256, 256), 256)
        total = stream[rows, cols].astype(F32) + fp[j, x].astype(F32)
        for o in (1, 3, 2):
            wait_recv(fr.at[j, xat(-o)], f_r.at[j, o - 1])
            total = total + fr[j, xat(-o)].astype(F32)
        out_ref[:, cols] = total.astype(BF)

    wait_send(kvb.at[pl.ds(0, 7), 0], kvz_s)
    wait_send(qb.at[pl.ds(0, 3)], q_s)
    wait_send(gv.at[pl.ds(0, 7), 0, 0], gvz_s)
    wait_send(gv.at[:, pl.ds(0, 3), 0], gvy_s)
    wait_send(dn.at[0, pl.ds(0, 3), 0], dny_s)
    wait_send(dn.at[pl.ds(0, 7), :, 0], dnz_s)
    wait_send(kvb.at[:, 0], pk_s)
    wait_send(gv.at[:, :, 0], pg_s)
    wait_send(dn.at[:, :, 0], pd_s)
    wait_send(part.at[pl.ds(0, 3)], o_s)
    wait_send(att.at[pl.ds(0, 3), pl.ds(0, TOK)], x_s)
    wait_send(att.at[:, pl.ds(0, 32)], e_s)
    wait_send(resid.at[pl.ds(0, 32)], h_s)
    wait_send(fp.at[:, pl.ds(0, 3)], f_s)


def layer(*operands):
    vmem = pl.BlockSpec(memory_space=pltpu.VMEM)
    hbm = pl.BlockSpec(memory_space=pltpu.HBM)
    dma = pltpu.SemaphoreType.DMA
    scratch = [
        pltpu.VMEM((320, TOK), BF),
        pltpu.VMEM((TOK, 512), BF),
        pltpu.VMEM((64, TOK), BF),
        pltpu.VMEM((512, 384), BF),
        pltpu.VMEM((32, TOK), F32),
        pltpu.VMEM((NZ, 2, TOK, 512), BF),
        pltpu.VMEM((NY, TOK, 384), BF),
        pltpu.VMEM((NZ, NY, 2, 64, FFD), BF),
        pltpu.VMEM((NZ, NY, 2, 32, FFD), BF),
        pltpu.VMEM((768, D), BF),
        pltpu.VMEM((ROWS, D), BF),
        pltpu.VMEM((2, NZ, 512, 256), F32),
        pltpu.VMEM((2, 256, 2048), BF),
        pltpu.VMEM((2, 512, 128), F32),
        pltpu.VMEM((2, 512, 128), F32),
        pltpu.VMEM((512, 256), F32),
        pltpu.VMEM((512, 128), F32),
        pltpu.VMEM((NY, TOK, 256), BF),
        pltpu.VMEM((NY, TOK, 256), BF),
        pltpu.VMEM((NX, ROWS, 256), BF),
        pltpu.VMEM((ROWS, D), BF),
        pltpu.VMEM((NZ, ROWS, 256), BF),
        pltpu.VMEM((ROWS, FFD), F32),
        pltpu.VMEM((TOK, FFD), F32),
        pltpu.VMEM((ROWS, FFD), BF),
        pltpu.VMEM((TOK, FFD), BF),
        pltpu.VMEM((TOK, FFD), BF),
        pltpu.VMEM((NZ, NX, 32, 256), BF),
        pltpu.VMEM((NZ, NX, 32, 256), BF),
        dma, dma((2, 4, 4)), dma, dma((2, 2)), dma, dma((2, 4)), dma, dma((2, 2, 8)),
        dma, dma((2, 2)), dma, dma((2, 4, 4)),
        dma, dma((8,)), dma, dma((8,)), dma, dma((8,)), dma, dma((3,)), dma, dma((3,)), dma, dma((2, 4)), dma, dma((2,)),
        dma, dma((NZ, 3)), dma((10,)),
    ]
    return pl.pallas_call(
        kernel,
        out_shape=pltpu.VMEM((32, D), BF),
        in_specs=[vmem] * 2 + [hbm] * 10,
        out_specs=vmem,
        scratch_shapes=scratch,
        compiler_params=pltpu.CompilerParams(collective_id=0, has_side_effects=True),
    )(*operands)


def body(
    queries, latents, shared_key, expand_weight, residual, out_weight,
    norm_gain, gate_weight, value_weight, conv_weight, down_weight,
):
    frequency = (10000.0 ** (-np.arange(ROPE // 2) / (ROPE // 2))).astype(np.float32)
    return layer(
        norm_gain, conv_weight, queries.T, latents, shared_key.T, expand_weight, gate_weight, value_weight,
        down_weight.T, np.ascontiguousarray(np.broadcast_to(frequency[:, None], (ROPE // 2, TOK))),
        residual, out_weight,
    )


def solution(mesh):
    split = Mesh(mesh.devices.reshape(NZ, NY, 2, mesh.shape["tp"]), ("sp_0", "sp_1", "sp_2", "tp"))
    placed = (
        P(SP, "tp"),
        P(SP, None),
        P(SP, None),
        P(None, "tp"),
        P(SP, None),
        P(),
        P(),
        P(SP, "tp"),
        P(SP, "tp"),
        P(None, "tp"),
        P("tp", SP),
    )
    return jax.shard_map(
        body, mesh=split, in_specs=placed, out_specs=P(SP_TP, None), check_vma=False
    )
```

```python
import functools

import jax
import jax.numpy as jnp
import numpy as np
from jax import lax
from jax.experimental import pallas as pl
from jax.experimental.pallas import tpu as pltpu
from jax.sharding import Mesh
from jax.sharding import PartitionSpec as P

NOPE_A = 128
VAL_A = 128
NOPE_B = 64
VAL_B = 64
ROPE = 64
SP = ("sp_0", "sp_1", "sp_2")
SP_TP = ("sp_0", "sp_1", "sp_2", "tp")
NZ, NY, NX = 8, 4, 4
TOK = 128
ROWS = TOK + 32
D = 2048
FFD = 768
MESH = pl.DeviceIdType.MESH
LOG2E = 1.4426950408889634
F32 = jnp.float32
BF = jnp.bfloat16


def split3(v):
    hi = v.astype(BF).astype(F32)
    rest = v - hi
    mid = rest.astype(BF).astype(F32)
    return hi, mid, rest - mid


def kernel(
    gain_hbm, conv_hbm, q_hbm, lat_hbm, key_hbm, ew_hbm, gate_hbm, value_hbm, dn_hbm, freq_hbm, resid_hbm, ow_hbm,
    out_ref,
    gain, conv_w, q_t, lat, key_t, ew, freq, kvb, qb, gv, dn, ow, resid, s_ref, p_ref, macc, mrow, accw, accn,
    part, ob, att, stream, normed, gacc, vacc, gate, value, act, fp, fr,
    kvz_s, kvz_r, q_s, q_r, gvz_s, gvz_r, gvy_s, gvy_r, dny_s, dny_r, dnz_s, dnz_r,
    pk_s, pk_r, pg_s, pg_r, pd_s, pd_r, o_s, o_r, x_s, x_r, e_s, e_r, h_s, h_r, f_s, f_r, loc,
):
    z = lax.axis_index("sp_0")
    y = lax.axis_index("sp_1")
    c = lax.axis_index("sp_2")
    x = lax.axis_index("tp")
    other = 1 - c

    def zat(k):
        return lax.rem(z + (k + NZ), NZ)

    def yat(k):
        return lax.rem(y + (k + NY), NY)

    def xat(k):
        return lax.rem(x + (k + NX), NX)

    right_z, left_z = {"sp_0": zat(1)}, {"sp_0": zat(-1)}
    right_y, left_y = {"sp_1": yat(1)}, {"sp_1": yat(-1)}
    partner = {"sp_2": other}
    place = (z * NY + y) * 2 + c
    after = lax.rem(place + 1, 64)
    before = lax.rem(place + 63, 64)

    def device_of(i):
        return {"sp_0": i // 8, "sp_1": lax.rem(i // 2, 4), "sp_2": lax.rem(i, 2)}

    def send(src, dst, ssem, rsem, dev):
        pltpu.make_async_remote_copy(
            src_ref=src, dst_ref=dst, send_sem=ssem, recv_sem=rsem, device_id=dev, device_id_type=MESH
        ).start()

    def wait_recv(ref, sem):
        pltpu.make_async_remote_copy(
            src_ref=ref, dst_ref=ref, send_sem=sem, recv_sem=sem, device_id=partner, device_id_type=MESH
        ).wait_recv()

    def wait_send(ref, sem):
        pltpu.make_async_remote_copy(
            src_ref=ref, dst_ref=ref, send_sem=sem, recv_sem=sem, device_id=partner, device_id_type=MESH
        ).wait_send()

    barrier = pltpu.get_barrier_semaphore()
    greeted = [
        partner, right_z, left_z, right_y, left_y, {"sp_1": yat(2)},
        {"tp": xat(1)}, {"tp": xat(2)}, {"tp": xat(3)},
    ]
    greeted += [device_of(i) | {"tp": xat(o)} for i in (after, before) for o in range(NX)]
    for dev in greeted:
        pl.semaphore_signal(barrier, inc=1, device_id=dev, device_id_type=MESH)

    def load(src, dst, i):
        copy = pltpu.make_async_copy(src, dst, loc.at[i])
        copy.start()
        return copy

    first_loads = [
        load(lat_hbm, lat, 0), load(ew_hbm, ew, 1), load(key_hbm, key_t, 2), load(freq_hbm, freq, 3),
        load(q_hbm, q_t, 4),
    ]
    weight_loads = [
        load(gate_hbm, gv.at[z, y, c, pl.ds(0, 32)], 5), load(value_hbm, gv.at[z, y, c, pl.ds(32, 32)], 6),
        load(dn_hbm, dn.at[z, y, c], 7),
    ]
    load_res = load(resid_hbm, resid.at[pl.ds(0, TOK)], 8)
    load_ow = load(ow_hbm, ow, 9)
    load_gain = load(gain_hbm, gain, 10)
    load_conv = load(conv_hbm, conv_w, 11)
    pl.semaphore_wait(barrier, len(greeted))
    for copy in first_loads:
        copy.wait()

    position = (lax.broadcasted_iota(jnp.int32, (32, TOK), 1) + place * TOK).astype(F32)
    angles = position * freq[...]
    cosine, sine = jnp.cos(angles), jnp.sin(angles)

    def turned(a, b):
        a, b = a.astype(F32), b.astype(F32)
        return [a * cosine - b * sine, b * cosine + a * sine]

    def upright(pieces):
        return jnp.transpose(jnp.concatenate(pieces, axis=0), (1, 0))

    nothing = jnp.zeros((64, TOK), F32)
    expanded = jnp.dot(lat[...], ew[...], preferred_element_type=F32)
    key_rows = upright(turned(key_t[0:32, :], key_t[32:64, :]) + [nothing])
    low_lane = lax.broadcasted_iota(jnp.int32, (TOK, 128), 1) < 64
    swapped = pltpu.roll(expanded[:, 256:384], 64, 1)
    kvb[0, 0, :, 0:128] = expanded[:, 0:128].astype(BF)
    kvb[0, 0, :, 128:256] = jnp.where(low_lane, key_rows, swapped).astype(BF)
    kvb[0, 0, :, 256:384] = expanded[:, 128:256].astype(BF)
    kvb[0, 0, :, 384:512] = jnp.where(low_lane, swapped, 1.0).astype(BF)
    qb[3, :, 0:128] = upright([q_t[0:128, :].astype(F32)]).astype(BF)
    qb[3, :, 128:256] = upright(turned(q_t[192:224, :], q_t[224:256, :]) + [nothing]).astype(BF)
    qb[3, :, 256:384] = upright(
        turned(q_t[256:288, :], q_t[288:320, :]) + [q_t[128:192, :].astype(F32)]
    ).astype(BF)

    def rows_of(slot, h):
        return kvb.at[slot, 0, pl.ds(32 * h, 32)]

    def slot_of(s, ahead):
        return 0 if s == 0 else 7 if s == 4 else 2 * s - 1 + ahead

    def kv_out(s, h):
        if s < 3 or h < 2:
            send(rows_of(slot_of(s, 0), h), rows_of(slot_of(s + 1, 0), h), kvz_s, kvz_r.at[0, s, h], right_z)
        if s < 3 or h >= 2:
            send(rows_of(slot_of(s, 1), h), rows_of(slot_of(s + 1, 1), h), kvz_s, kvz_r.at[1, s, h], left_z)

    def kv_across(slot):
        send(kvb.at[slot, 0], kvb.at[slot, 1], pk_s, pk_r.at[slot], partner)

    def kvz(s, h):
        if s < 4:
            wait_recv(rows_of(slot_of(s, 0), h), kvz_r.at[0, s - 1, h])
            wait_recv(rows_of(slot_of(s, 1), h), kvz_r.at[1, s - 1, h])
            kv_out(s, h)
            if h == 3:
                kv_across(2 * s - 1)
                kv_across(2 * s)
        else:
            for q in range(4):
                wait_recv(rows_of(7, q), kvz_r.at[q // 2, 3, q])
            kv_across(7)

    def q_relay(s):
        if s == 1:
            wait_recv(qb.at[1], q_r.at[0, 0])
            send(qb.at[1, pl.ds(0, 64)], qb.at[0, pl.ds(0, 64)], q_s, q_r.at[0, 1], right_y)
            wait_recv(qb.at[2], q_r.at[1, 0])
            send(qb.at[2, pl.ds(64, 64)], qb.at[0, pl.ds(64, 64)], q_s, q_r.at[1, 1], left_y)
        else:
            wait_recv(qb.at[0, pl.ds(0, 64)], q_r.at[0, 1])
            wait_recv(qb.at[0, pl.ds(64, 64)], q_r.at[1, 1])

    for q in range(4):
        kv_out(0, q)
    send(qb.at[3], qb.at[1], q_s, q_r.at[0, 0], right_y)
    send(qb.at[3], qb.at[2], q_s, q_r.at[1, 0], left_y)
    kv_across(0)
    macc[...] = jnp.full((2, 512, 128), -3e38, F32)

    def gvz_own():
        own = gv.at[z, y, c]
        send(own, own, gvz_s, gvz_r.at[0, 0], right_z)
        send(own, own, gvz_s, gvz_r.at[1, 0], left_z)

    def dny_own():
        own = dn.at[z, y, c]
        send(own, own, dny_s, dny_r.at[0, 0], right_y)
        send(own, own, dny_s, dny_r.at[1, 0], left_y)

    def gvy_own():
        own = gv.at[z, y, c]
        send(own, own, gvy_s, gvy_r.at[0, 0, 0], right_y)
        send(own, own, gvy_s, gvy_r.at[1, 0, 0], left_y)
        send(own, own, pg_s, pg_r.at[0], partner)

    for copy in weight_loads:
        copy.wait()

    offsets = [0, -1, 1, -2, 2, -3, 3, 4]

    def gv_out(zz, j):
        block = gv.at[zz, y, c]
        send(block, block, gvy_s, gvy_r.at[0, 0, j], right_y)
        send(block, block, gvy_s, gvy_r.at[1, 0, j], left_y)
        send(block, block, pg_s, pg_r.at[j], partner)

    def gvz(s):
        lo, hi = zat(-s), zat(s)
        if s < 4:
            wait_recv(gv.at[lo, y, c], gvz_r.at[0, s - 1])
            src = gv.at[lo, y, c] if s < 3 else gv.at[lo, y, c, pl.ds(0, 32)]
            send(src, src, gvz_s, gvz_r.at[0, s], right_z)
            wait_recv(gv.at[hi, y, c], gvz_r.at[1, s - 1])
            src = gv.at[hi, y, c] if s < 3 else gv.at[hi, y, c, pl.ds(32, 32)]
            send(src, src, gvz_s, gvz_r.at[1, s], left_z)
            gv_out(lo, 2 * s - 1)
            gv_out(hi, 2 * s)
        else:
            wait_recv(gv.at[lo, y, c, pl.ds(0, 32)], gvz_r.at[0, 3])
            wait_recv(gv.at[lo, y, c, pl.ds(32, 32)], gvz_r.at[1, 3])
            gv_out(lo, 7)

    def gvy(s, j):
        zz = zat(offsets[j])
        a, b, far = yat(-1), yat(1), yat(2)
        if s == 1:
            wait_recv(gv.at[zz, a, c], gvy_r.at[0, 0, j])
            src = gv.at[zz, a, c, pl.ds(0, 32)]
            send(src, src, gvy_s, gvy_r.at[0, 1, j], right_y)
            wait_recv(gv.at[zz, b, c], gvy_r.at[1, 0, j])
            src = gv.at[zz, b, c, pl.ds(32, 32)]
            send(src, src, gvy_s, gvy_r.at[1, 1, j], left_y)
            send(gv.at[zz, a, c], gv.at[zz, a, c], pg_s, pg_r.at[j], partner)
            send(gv.at[zz, b, c], gv.at[zz, b, c], pg_s, pg_r.at[j], partner)
        else:
            wait_recv(gv.at[zz, far, c, pl.ds(0, 32)], gvy_r.at[0, 1, j])
            wait_recv(gv.at[zz, far, c, pl.ds(32, 32)], gvy_r.at[1, 1, j])
            send(gv.at[zz, far, c], gv.at[zz, far, c], pg_s, pg_r.at[j], partner)

    def dny(s):
        a, b, far = yat(-1), yat(1), yat(2)
        if s == 1:
            wait_recv(dn.at[z, a, c], dny_r.at[0, 0])
            src = dn.at[z, a, c, pl.ds(0, 16)]
            send(src, src, dny_s, dny_r.at[0, 1], right_y)
            wait_recv(dn.at[z, b, c], dny_r.at[1, 0])
            src = dn.at[z, b, c, pl.ds(16, 16)]
            send(src, src, dny_s, dny_r.at[1, 1], left_y)
        else:
            wait_recv(dn.at[z, far, c, pl.ds(0, 16)], dny_r.at[0, 1])
            wait_recv(dn.at[z, far, c, pl.ds(16, 16)], dny_r.at[1, 1])

    def dnz(s, r):
        yy = yat((0, -1, 1, 2)[r])
        lo, hi = zat(-s), zat(s)
        if s == 0:
            block = dn.at[z, yy, c]
            send(block, block, dnz_s, dnz_r.at[0, 0, r], right_z)
            send(block, block, dnz_s, dnz_r.at[1, 0, r], left_z)
        elif s < 4:
            wait_recv(dn.at[lo, yy, c], dnz_r.at[0, s - 1, r])
            src = dn.at[lo, yy, c] if s < 3 else dn.at[lo, yy, c, pl.ds(0, 16)]
            send(src, src, dnz_s, dnz_r.at[0, s, r], right_z)
            wait_recv(dn.at[hi, yy, c], dnz_r.at[1, s - 1, r])
            src = dn.at[hi, yy, c] if s < 3 else dn.at[hi, yy, c, pl.ds(16, 16)]
            send(src, src, dnz_s, dnz_r.at[1, s, r], left_z)
        else:
            wait_recv(dn.at[lo, yy, c, pl.ds(0, 16)], dnz_r.at[0, 3, r])
            wait_recv(dn.at[lo, yy, c, pl.ds(16, 16)], dnz_r.at[1, 3, r])
        send(dn.at[lo, yy, c], dn.at[lo, yy, c], pd_s, pd_r.at[slot_of(s, 0)], partner)
        if 0 < s < 4:
            send(dn.at[hi, yy, c], dn.at[hi, yy, c], pd_s, pd_r.at[slot_of(s, 1)], partner)

    heads = (
        (0, 256, 0, 256, 256, 512, (NOPE_A + ROPE) ** (-0.5) * LOG2E, accw),
        (256, 384, 128, 256, 384, 512, (NOPE_B + ROPE) ** (-0.5) * LOG2E, accn),
    )

    def scores(j):
        wait_recv(kvb.at[j, 1], pk_r.at[j])
        for head in range(2):
            q0, q1, k0, k1 = heads[head][:4]
            qs = qb[:, :, q0:q1].reshape(512, q1 - q0)
            ks = kvb[j, :, :, k0:k1].reshape(256, k1 - k0)
            s = lax.dot_general(qs, ks, (((1,), (1,)), ((), ())), preferred_element_type=F32)
            s_ref[head, j] = s
            macc[head] = jnp.maximum(macc[head], jnp.maximum(s[:, :128], s[:, 128:]))

    def weigh(half):
        rows = slice(256 * half, 256 * half + 256)
        for head in range(2):
            v0, v1, factor, acc = heads[head][4:]
            m = jnp.broadcast_to(jnp.max(macc[head, rows], axis=1, keepdims=True), (256, 128))
            mrow[head, rows] = m
            for j in range(NZ):
                for side in range(2):
                    s = s_ref[head, j, rows, side * 128 : side * 128 + 128]
                    at = j * 256 + side * 128
                    p_ref[head, :, at : at + 128] = jnp.exp2((s - m) * factor).astype(BF)
            vs = kvb[:, :, :, v0:v1].reshape(2048, v1 - v0)
            acc[rows] = jnp.dot(p_ref[head], vs, preferred_element_type=F32)

    lane = lax.broadcasted_iota(jnp.int32, (TOK, 128), 1)

    def pack(half):
        for b in (2 * half, 2 * half + 1):
            rows = slice(b * TOK, b * TOK + TOK)
            wide, narrow = accw[rows, :], accn[rows, :]
            tile = narrow
            stats = (
                mrow[0, rows, :], mrow[1, rows, :],
                jnp.broadcast_to(wide[:, 192:193], (TOK, 128)), jnp.broadcast_to(narrow[:, 64:65], (TOK, 128)),
            )
            at = 64
            for stat in stats:
                for piece in split3(stat):
                    tile = jnp.where(lane == at, piece, tile)
                    at += 1
            tile = jnp.where(lane >= at, 0.0, tile)
            part[b, :, 0:128] = wide[:, 0:128].astype(BF)
            part[b, :, 128:256] = tile.astype(BF)
        if half == 0:
            send(part.at[0], ob.at[0], o_s, o_r.at[0], {"sp_1": yat(2)})
            send(part.at[1], ob.at[2], o_s, o_r.at[2], left_y)
        else:
            send(part.at[2], ob.at[1], o_s, o_r.at[1], right_y)

    def merge():
        blocks = [part.at[3]] + [ob.at[g] for g in range(3)]
        tiles = [block[:, 128:256].astype(F32) for block in blocks]
        stats = [s + pltpu.roll(s, 127, 1) + pltpu.roll(s, 126, 1) for s in tiles]
        top = jnp.maximum(jnp.maximum(stats[0], stats[1]), jnp.maximum(stats[2], stats[3]))
        factor = jnp.where(lane == 64, heads[0][6], heads[1][6])
        shares = [jnp.exp2((s - top) * factor) for s in stats]
        total = sum(pltpu.roll(w, 6, 1) * s for w, s in zip(shares, stats))
        inverse = pltpu.roll(1.0 / total, 122, 1)
        shares = [w * inverse for w in shares]
        wide = sum(w[:, 64:65] * block[:, 0:128].astype(F32) for w, block in zip(shares, blocks))
        narrow = sum(w[:, 67:68] * s for w, s in zip(shares, tiles))
        att[x, 0:TOK, 0:128] = wide.astype(BF)
        att[x, 0:TOK, 128:256] = narrow.astype(BF)

    def part_in():
        for o in range(3):
            wait_recv(ob.at[o], o_r.at[o])

    def att_out():
        for o in (2, 1, 3):
            mine = att.at[x, pl.ds(0, TOK)]
            send(mine, mine, x_s, x_r.at[o - 1], {"tp": xat(o)})
        for o in range(NX):
            peer = {"tp": xat(o)}
            send(att.at[x, pl.ds(112, 16)], att.at[x, pl.ds(128, 16)], e_s, e_r.at[0, o], device_of(after) | peer)
            send(att.at[x, pl.ds(0, 16)], att.at[x, pl.ds(144, 16)], e_s, e_r.at[1, o], device_of(before) | peer)

    def edges_out():
        load_res.wait()
        send(resid.at[pl.ds(112, 16)], resid.at[pl.ds(128, 16)], h_s, h_r.at[0], device_of(after))
        send(resid.at[pl.ds(0, 16)], resid.at[pl.ds(144, 16)], h_s, h_r.at[1], device_of(before))

    edges_out()
    gvy_own()
    gvz_own()
    kvz(1, 0)
    q_relay(1)
    kvz(1, 1)
    dny_own()
    kvz(1, 2)
    kvz(1, 3)
    gvy(1, 0)
    gvz(1)
    q_relay(2)
    scores(0)
    scores(1)
    kvz(2, 0)
    scores(2)
    dny(1)
    kvz(2, 1)
    kvz(2, 2)
    gvy(2, 0)
    kvz(2, 3)
    scores(3)
    gvz(2)
    scores(4)
    kvz(3, 0)
    kvz(3, 1)
    gvy(1, 2)
    kvz(3, 2)
    dny(2)
    gvy(1, 1)
    kvz(3, 3)
    dnz(0, 2)
    dnz(0, 3)
    dnz(0, 0)
    scores(5)
    gvz(3)
    scores(6)
    kvz(4, 0)
    dnz(0, 1)
    dnz(1, 2)
    gvy(2, 2)
    scores(7)
    weigh(0)
    dnz(1, 0)
    dnz(1, 3)
    gvy(2, 1)
    pack(0)
    weigh(1)
    pack(1)
    gvz(4)
    gvy(1, 5)
    dnz(1, 1)
    gvy(1, 3)
    gvy(1, 4)
    dnz(2, 2)
    gvy(1, 6)
    dnz(2, 0)
    dnz(2, 3)
    part_in()
    merge()
    att_out()
    dnz(2, 1)
    dnz(3, 2)
    gvy(1, 7)
    dnz(3, 0)
    gvy(2, 5)
    dnz(3, 3)
    gvy(2, 3)
    dnz(3, 1)
    load_ow.wait()
    load_gain.wait()
    load_conv.wait()
    wait_recv(resid.at[pl.ds(128, 16)], h_r.at[0])
    wait_recv(resid.at[pl.ds(144, 16)], h_r.at[1])
    for o in (2, 1, 3):
        wait_recv(att.at[xat(-o), pl.ds(0, TOK)], x_r.at[o - 1])
    for o in range(NX):
        wait_recv(att.at[xat(-o), pl.ds(128, 16)], e_r.at[0, o])
        wait_recv(att.at[xat(-o), pl.ds(144, 16)], e_r.at[1, o])

    ss = jnp.zeros((ROWS, 1), F32)
    for n in range(8):
        cols = slice(n * 256, n * 256 + 256)
        total = resid[:, cols].astype(F32)
        for h in range(NX):
            total = total + jnp.dot(att[h, :, 0:192], ow[h * 192 : h * 192 + 192, cols], preferred_element_type=F32)
        rounded = total.astype(BF)
        stream[:, cols] = rounded
        wide = rounded.astype(F32)
        ss = ss + jnp.sum(wide * wide, axis=1, keepdims=True)
    scale = lax.rsqrt(ss * (1.0 / D) + 1e-06)
    for n in range(8):
        cols = slice(n * 256, n * 256 + 256)
        scaled = stream[:, cols].astype(F32) * scale
        normed[n] = (scaled * gain[cols].astype(F32).reshape(1, 256)).astype(BF)
    gvy(2, 4)
    gvy(2, 6)

    def up(lo, rows, js, acc, n):
        cols = slice(n * 256, n * 256 + 256)
        total = None
        for j in js:
            zz = zat(offsets[j])
            w = gv[zz, :, :, lo : lo + 32, cols].reshape(256, 256)
            term = jnp.dot(normed[zz, 0:rows], w, preferred_element_type=F32)
            total = term if total is None else total + term
        return total if acc is None else acc[:, cols] + total

    for j in range(7):
        wait_recv(gv.at[zat(offsets[j]), :, other], pg_r.at[j])
    for n in range(3):
        gacc[:, n * 256 : n * 256 + 256] = up(0, ROWS, range(7), None, n)
    gvy(2, 7)
    for n in range(3):
        vacc[:, n * 256 : n * 256 + 256] = up(32, TOK, range(7), None, n)
    wait_recv(gv.at[zat(offsets[7]), :, other], pg_r.at[7])
    for n in range(3):
        cols = slice(n * 256, n * 256 + 256)
        gate[:, cols] = up(0, ROWS, (7,), gacc, n).astype(BF)
        value[:, cols] = up(32, TOK, (7,), vacc, n).astype(BF)

    row = lax.broadcasted_iota(jnp.int32, (TOK, 256), 0)
    for n in range(3):
        cols = slice(n * 256, n * 256 + 256)
        g = gate[0:TOK, cols].astype(F32)
        edge = gate[TOK:ROWS, cols].astype(F32)
        first = jnp.where(place > 0, edge[15:16], 0.0)
        last = jnp.where(place < 63, edge[16:17], 0.0)
        low = jnp.where(row == 0, first, pltpu.roll(g, 1, 0))
        high = jnp.where(row == TOK - 1, last, pltpu.roll(g, TOK - 1, 0))
        cw = conv_w[:, cols].astype(F32)
        mixed = low * cw[0:1] + g * cw[1:2] + high * cw[2:3]
        silu = mixed / (1.0 + jnp.exp(-mixed))
        act[:, cols] = (silu * value[:, cols].astype(F32)).astype(BF)

    for j in range(NZ):
        zz = zat(offsets[j])
        if j == 7:
            for r in range(NY):
                dnz(4, r)
        wait_recv(dn.at[zz, :, other], pd_r.at[j])
        w = dn[zz].reshape(256, FFD)
        d = lax.dot_general(act[...], w, (((1,), (1,)), ((), ())), preferred_element_type=F32)
        fp[j] = d.astype(BF).reshape(NX, 32, 256)
        for o in (2, 1, 3):
            peer = xat(o)
            send(fp.at[j, peer], fr.at[j, x], f_s, f_r.at[j, o - 1], {"tp": peer})

    rows = pl.ds(pl.multiple_of(x * 32, 32), 32)
    for j in range(NZ):
        cols = pl.ds(pl.multiple_of(zat(offsets[j]) * 256, 256), 256)
        total = stream[rows, cols].astype(F32) + fp[j, x].astype(F32)
        for o in (1, 3, 2):
            wait_recv(fr.at[j, xat(-o)], f_r.at[j, o - 1])
            total = total + fr[j, xat(-o)].astype(F32)
        out_ref[:, cols] = total.astype(BF)

    wait_send(kvb.at[pl.ds(0, 7), 0], kvz_s)
    wait_send(qb.at[pl.ds(0, 3)], q_s)
    wait_send(gv.at[pl.ds(0, 7), 0, 0], gvz_s)
    wait_send(gv.at[:, pl.ds(0, 3), 0], gvy_s)
    wait_send(dn.at[0, pl.ds(0, 3), 0], dny_s)
    wait_send(dn.at[pl.ds(0, 7), :, 0], dnz_s)
    wait_send(kvb.at[:, 0], pk_s)
    wait_send(gv.at[:, :, 0], pg_s)
    wait_send(dn.at[:, :, 0], pd_s)
    wait_send(part.at[pl.ds(0, 3)], o_s)
    wait_send(att.at[pl.ds(0, 3), pl.ds(0, TOK)], x_s)
    wait_send(att.at[:, pl.ds(0, 32)], e_s)
    wait_send(resid.at[pl.ds(0, 32)], h_s)
    wait_send(fp.at[:, pl.ds(0, 3)], f_s)


def layer(*operands):
    vmem = pl.BlockSpec(memory_space=pltpu.VMEM)
    hbm = pl.BlockSpec(memory_space=pltpu.HBM)
    dma = pltpu.SemaphoreType.DMA
    scratch = [
        pltpu.VMEM((D,), BF),
        pltpu.VMEM((3, FFD), BF),
        pltpu.VMEM((320, TOK), BF),
        pltpu.VMEM((TOK, 512), BF),
        pltpu.VMEM((64, TOK), BF),
        pltpu.VMEM((512, 384), BF),
        pltpu.VMEM((32, TOK), F32),
        pltpu.VMEM((NZ, 2, TOK, 512), BF),
        pltpu.VMEM((NY, TOK, 384), BF),
        pltpu.VMEM((NZ, NY, 2, 64, FFD), BF),
        pltpu.VMEM((NZ, NY, 2, 32, FFD), BF),
        pltpu.VMEM((768, D), BF),
        pltpu.VMEM((ROWS, D), BF),
        pltpu.VMEM((2, NZ, 512, 256), F32),
        pltpu.VMEM((2, 256, 2048), BF),
        pltpu.VMEM((2, 512, 128), F32),
        pltpu.VMEM((2, 512, 128), F32),
        pltpu.VMEM((512, 256), F32),
        pltpu.VMEM((512, 128), F32),
        pltpu.VMEM((NY, TOK, 256), BF),
        pltpu.VMEM((NY, TOK, 256), BF),
        pltpu.VMEM((NX, ROWS, 256), BF),
        pltpu.VMEM((ROWS, D), BF),
        pltpu.VMEM((NZ, ROWS, 256), BF),
        pltpu.VMEM((ROWS, FFD), F32),
        pltpu.VMEM((TOK, FFD), F32),
        pltpu.VMEM((ROWS, FFD), BF),
        pltpu.VMEM((TOK, FFD), BF),
        pltpu.VMEM((TOK, FFD), BF),
        pltpu.VMEM((NZ, NX, 32, 256), BF),
        pltpu.VMEM((NZ, NX, 32, 256), BF),
        dma, dma((2, 4, 4)), dma, dma((2, 2)), dma, dma((2, 4)), dma, dma((2, 2, 8)),
        dma, dma((2, 2)), dma, dma((2, 4, 4)),
        dma, dma((8,)), dma, dma((8,)), dma, dma((8,)), dma, dma((3,)), dma, dma((3,)), dma, dma((2, 4)), dma, dma((2,)),
        dma, dma((NZ, 3)), dma((12,)),
    ]
    return pl.pallas_call(
        kernel,
        out_shape=pltpu.VMEM((32, D), BF),
        in_specs=[hbm] * 12,
        out_specs=vmem,
        scratch_shapes=scratch,
        compiler_params=pltpu.CompilerParams(collective_id=0, has_side_effects=True),
    )(*operands)


def body(
    queries, latents, shared_key, expand_weight, residual, out_weight,
    norm_gain, gate_weight, value_weight, conv_weight, down_weight,
):
    frequency = (10000.0 ** (-np.arange(ROPE // 2) / (ROPE // 2))).astype(np.float32)
    return layer(
        norm_gain, conv_weight, queries.T, latents, shared_key.T, expand_weight, gate_weight, value_weight,
        down_weight.T, np.ascontiguousarray(np.broadcast_to(frequency[:, None], (ROPE // 2, TOK))),
        residual, out_weight,
    )


def solution(mesh):
    split = Mesh(mesh.devices.reshape(NZ, NY, 2, mesh.shape["tp"]), ("sp_0", "sp_1", "sp_2", "tp"))
    placed = (
        P(SP, "tp"),
        P(SP, None),
        P(SP, None),
        P(None, "tp"),
        P(SP, None),
        P(),
        P(),
        P(SP, "tp"),
        P(SP, "tp"),
        P(None, "tp"),
        P("tp", SP),
    )
    return jax.shard_map(
        body, mesh=split, in_specs=placed, out_specs=P(SP_TP, None), check_vma=False
    )
```

```python
import functools

import jax
import jax.numpy as jnp
import numpy as np
from jax import lax
from jax.experimental import pallas as pl
from jax.experimental.pallas import tpu as pltpu
from jax.sharding import Mesh
from jax.sharding import PartitionSpec as P

NOPE_A = 128
VAL_A = 128
NOPE_B = 64
VAL_B = 64
ROPE = 64
SP = ("sp_0", "sp_1", "sp_2")
SP_TP = ("sp_0", "sp_1", "sp_2", "tp")
NZ, NY, NX = 8, 4, 4
TOK = 128
ROWS = TOK + 32
D = 2048
FFD = 768
MESH = pl.DeviceIdType.MESH
LOG2E = 1.4426950408889634
F32 = jnp.float32
BF = jnp.bfloat16


def split3(v):
    hi = v.astype(BF).astype(F32)
    rest = v - hi
    mid = rest.astype(BF).astype(F32)
    return hi, mid, rest - mid


def kernel(
    gain_hbm, conv_hbm, q_hbm, lat_hbm, key_hbm, ew_hbm, gate_hbm, value_hbm, dn_hbm, freq_hbm, resid_hbm, ow_hbm,
    out_ref,
    gain, conv_w, q_t, lat, key_t, ew, freq, kvb, qb, gb, va, da, db, ow, resid, s_ref, p_ref, macc, mrow, accw, accn,
    part, ob, att, stream, normed, gacc, vacc, gate, value, act, fp, fr,
    kvz_s, kvz_r, q_s, q_r, pk_s, pk_r, o_s, o_r, x_s, x_r, e_s, e_r, h_s, h_r, f_s, f_r, loc, *ring_sems,
):
    z = lax.axis_index("sp_0")
    y = lax.axis_index("sp_1")
    c = lax.axis_index("sp_2")
    x = lax.axis_index("tp")
    other = 1 - c

    def zat(k):
        return lax.rem(z + (k + NZ), NZ)

    def yat(k):
        return lax.rem(y + (k + NY), NY)

    def xat(k):
        return lax.rem(x + (k + NX), NX)

    right_z, left_z = {"sp_0": zat(1)}, {"sp_0": zat(-1)}
    right_y, left_y = {"sp_1": yat(1)}, {"sp_1": yat(-1)}
    partner = {"sp_2": other}
    place = (z * NY + y) * 2 + c
    after = lax.rem(place + 1, 64)
    before = lax.rem(place + 63, 64)

    def device_of(i):
        return {"sp_0": i // 8, "sp_1": lax.rem(i // 2, 4), "sp_2": lax.rem(i, 2)}

    def send(src, dst, ssem, rsem, dev):
        pltpu.make_async_remote_copy(
            src_ref=src, dst_ref=dst, send_sem=ssem, recv_sem=rsem, device_id=dev, device_id_type=MESH
        ).start()

    def wait_recv(ref, sem):
        pltpu.make_async_remote_copy(
            src_ref=ref, dst_ref=ref, send_sem=sem, recv_sem=sem, device_id=partner, device_id_type=MESH
        ).wait_recv()

    def wait_send(ref, sem):
        pltpu.make_async_remote_copy(
            src_ref=ref, dst_ref=ref, send_sem=sem, recv_sem=sem, device_id=partner, device_id_type=MESH
        ).wait_send()

    barrier = pltpu.get_barrier_semaphore()
    greeted = [
        partner, right_z, left_z, right_y, left_y, {"sp_1": yat(2)},
        {"tp": xat(1)}, {"tp": xat(2)}, {"tp": xat(3)},
    ]
    greeted += [device_of(i) | {"tp": xat(o)} for i in (after, before) for o in range(NX)]
    for dev in greeted:
        pl.semaphore_signal(barrier, inc=1, device_id=dev, device_id_type=MESH)

    def load(src, dst, i):
        copy = pltpu.make_async_copy(src, dst, loc.at[i])
        copy.start()
        return copy

    first_loads = [
        load(lat_hbm, lat, 0), load(ew_hbm, ew, 1), load(key_hbm, key_t, 2), load(freq_hbm, freq, 3),
        load(q_hbm, q_t, 4),
    ]
    weight_loads = [
        load(gate_hbm, gb.at[z, y, c, pl.ds(0, 32)], 5),
        load(value_hbm.at[pl.ds(0, 16)], gb.at[z, y, c, pl.ds(32, 16)], 6),
        load(value_hbm.at[pl.ds(16, 16)], va.at[z, y, c], 7),
        load(dn_hbm.at[pl.ds(0, 16)], da.at[z, y, c], 12), load(dn_hbm.at[pl.ds(16, 16)], db.at[z, y, c], 13),
    ]
    load_res = load(resid_hbm, resid.at[pl.ds(0, TOK)], 8)
    load_ow = load(ow_hbm, ow, 9)
    load_gain = load(gain_hbm, gain, 10)
    load_conv = load(conv_hbm, conv_w, 11)
    pl.semaphore_wait(barrier, len(greeted))
    for copy in first_loads:
        copy.wait()

    position = (lax.broadcasted_iota(jnp.int32, (32, TOK), 1) + place * TOK).astype(F32)
    angles = position * freq[...]
    cosine, sine = jnp.cos(angles), jnp.sin(angles)

    def turned(a, b):
        a, b = a.astype(F32), b.astype(F32)
        return [a * cosine - b * sine, b * cosine + a * sine]

    def upright(pieces):
        return jnp.transpose(jnp.concatenate(pieces, axis=0), (1, 0))

    nothing = jnp.zeros((64, TOK), F32)
    expanded = jnp.dot(lat[...], ew[...], preferred_element_type=F32)
    key_rows = upright(turned(key_t[0:32, :], key_t[32:64, :]) + [nothing])
    low_lane = lax.broadcasted_iota(jnp.int32, (TOK, 128), 1) < 64
    swapped = pltpu.roll(expanded[:, 256:384], 64, 1)
    kvb[0, 0, :, 0:128] = expanded[:, 0:128].astype(BF)
    kvb[0, 0, :, 128:256] = jnp.where(low_lane, key_rows, swapped).astype(BF)
    kvb[0, 0, :, 256:384] = expanded[:, 128:256].astype(BF)
    kvb[0, 0, :, 384:512] = jnp.where(low_lane, swapped, 1.0).astype(BF)
    qb[3, :, 0:128] = upright([q_t[0:128, :].astype(F32)]).astype(BF)
    qb[3, :, 128:256] = upright(turned(q_t[192:224, :], q_t[224:256, :]) + [nothing]).astype(BF)
    qb[3, :, 256:384] = upright(
        turned(q_t[256:288, :], q_t[288:320, :]) + [q_t[128:192, :].astype(F32)]
    ).astype(BF)

    def rows_of(slot, h):
        return kvb.at[slot, 0, pl.ds(32 * h, 32)]

    def slot_of(s, ahead):
        return 0 if s == 0 else 7 if s == 4 else 2 * s - 1 + ahead

    def kv_out(s, h):
        if s < 3 or h < 2:
            send(rows_of(slot_of(s, 0), h), rows_of(slot_of(s + 1, 0), h), kvz_s, kvz_r.at[0, s, h], right_z)
        if s < 3 or h >= 2:
            send(rows_of(slot_of(s, 1), h), rows_of(slot_of(s + 1, 1), h), kvz_s, kvz_r.at[1, s, h], left_z)

    def kv_across(slot):
        send(kvb.at[slot, 0], kvb.at[slot, 1], pk_s, pk_r.at[slot], partner)

    def kvz(s, h):
        if s < 4:
            wait_recv(rows_of(slot_of(s, 0), h), kvz_r.at[0, s - 1, h])
            wait_recv(rows_of(slot_of(s, 1), h), kvz_r.at[1, s - 1, h])
            kv_out(s, h)
            if h == 3:
                kv_across(2 * s - 1)
                kv_across(2 * s)
        else:
            for q in range(4):
                wait_recv(rows_of(7, q), kvz_r.at[q // 2, 3, q])
            kv_across(7)

    def q_relay(s):
        if s == 1:
            wait_recv(qb.at[1], q_r.at[0, 0])
            send(qb.at[1, pl.ds(0, 64)], qb.at[0, pl.ds(0, 64)], q_s, q_r.at[0, 1], right_y)
            wait_recv(qb.at[2], q_r.at[1, 0])
            send(qb.at[2, pl.ds(64, 64)], qb.at[0, pl.ds(64, 64)], q_s, q_r.at[1, 1], left_y)
        else:
            wait_recv(qb.at[0, pl.ds(0, 64)], q_r.at[0, 1])
            wait_recv(qb.at[0, pl.ds(64, 64)], q_r.at[1, 1])

    for q in range(4):
        kv_out(0, q)
    send(qb.at[3], qb.at[1], q_s, q_r.at[0, 0], right_y)
    send(qb.at[3], qb.at[2], q_s, q_r.at[1, 0], left_y)
    kv_across(0)
    macc[...] = jnp.full((2, 512, 128), -3e38, F32)

    for copy in weight_loads:
        copy.wait()

    offsets = [0, -1, 1, -2, 2, -3, 3, 4]

    def z_then_y(buf, z_s, z_r, y_s, y_r, p_s, p_r):
        def half(zz, yy, h):
            return buf.at[zz, yy, c, :, pl.ds(384 * h, 384)]

        def out(zz, j):
            block = buf.at[zz, y, c]
            send(block, block, y_s, y_r.at[0, 0, j], right_y)
            send(block, block, y_s, y_r.at[1, 0, j], left_y)
            send(block, block, p_s, p_r.at[j], partner)

        def on_z(s):
            lo, hi = zat(-s), zat(s)
            if s == 4:
                wait_recv(half(lo, y, 0), z_r.at[0, 3])
                wait_recv(half(lo, y, 1), z_r.at[1, 3])
                out(lo, 7)
                return
            for way, (zz, dev) in enumerate(((lo, right_z), (hi, left_z))):
                block = buf.at[zz, y, c]
                if s > 0:
                    wait_recv(block, z_r.at[way, s - 1])
                src = block if s < 3 else half(zz, y, way)
                send(src, src, z_s, z_r.at[way, s], dev)
            if s > 0:
                out(lo, 2 * s - 1)
                out(hi, 2 * s)

        def on_y(s, j):
            zz = zat(offsets[j])
            a, b, far = yat(-1), yat(1), yat(2)
            if s == 0:
                out(z, 0)
            elif s == 1:
                for way, (yy, dev) in enumerate(((a, right_y), (b, left_y))):
                    wait_recv(buf.at[zz, yy, c], y_r.at[way, 0, j])
                    src = half(zz, yy, way)
                    send(src, src, y_s, y_r.at[way, 1, j], dev)
                for yy in (a, b):
                    send(buf.at[zz, yy, c], buf.at[zz, yy, c], p_s, p_r.at[j], partner)
            else:
                wait_recv(half(zz, far, 0), y_r.at[0, 1, j])
                wait_recv(half(zz, far, 1), y_r.at[1, 1, j])
                send(buf.at[zz, far, c], buf.at[zz, far, c], p_s, p_r.at[j], partner)

        return on_z, on_y

    def y_then_z(buf, z_s, z_r, y_s, y_r, p_s, p_r):
        def half(zz, yy, h):
            return buf.at[zz, yy, c, :, pl.ds(384 * h, 384)]

        def on_y(s):
            a, b, far = yat(-1), yat(1), yat(2)
            if s == 2:
                wait_recv(half(z, far, 0), y_r.at[0, 1])
                wait_recv(half(z, far, 1), y_r.at[1, 1])
                return
            for way, (yy, dev) in enumerate(((a, right_y), (b, left_y))):
                if s == 0:
                    src = buf.at[z, y, c]
                else:
                    wait_recv(buf.at[z, yy, c], y_r.at[way, 0])
                    src = half(z, yy, way)
                send(src, src, y_s, y_r.at[way, s], dev)

        def on_z(s, r):
            yy = yat((0, -1, 1, 2)[r])
            lo, hi = zat(-s), zat(s)
            if s == 4:
                wait_recv(half(lo, yy, 0), z_r.at[0, 3, r])
                wait_recv(half(lo, yy, 1), z_r.at[1, 3, r])
            else:
                for way, (zz, dev) in enumerate(((lo, right_z), (hi, left_z))):
                    block = buf.at[zz, yy, c]
                    if s > 0:
                        wait_recv(block, z_r.at[way, s - 1, r])
                    src = block if s < 3 else half(zz, yy, way)
                    send(src, src, z_s, z_r.at[way, s, r], dev)
            for ahead, zz in enumerate((lo, hi) if 0 < s < 4 else (lo,)):
                send(buf.at[zz, yy, c], buf.at[zz, yy, c], p_s, p_r.at[slot_of(s, ahead)], partner)

        return on_y, on_z

    gb_z, gb_y = z_then_y(gb, *ring_sems[0:6])
    db_z, db_y = z_then_y(db, *ring_sems[6:12])
    va_y, va_z = y_then_z(va, *ring_sems[12:18])
    da_y, da_z = y_then_z(da, *ring_sems[18:24])

    heads = (
        (0, 256, 0, 256, 256, 512, (NOPE_A + ROPE) ** (-0.5) * LOG2E, accw),
        (256, 384, 128, 256, 384, 512, (NOPE_B + ROPE) ** (-0.5) * LOG2E, accn),
    )

    def scores(j):
        wait_recv(kvb.at[j, 1], pk_r.at[j])
        for head in range(2):
            q0, q1, k0, k1 = heads[head][:4]
            qs = qb[:, :, q0:q1].reshape(512, q1 - q0)
            ks = kvb[j, :, :, k0:k1].reshape(256, k1 - k0)
            s = lax.dot_general(qs, ks, (((1,), (1,)), ((), ())), preferred_element_type=F32)
            s_ref[head, j] = s
            macc[head] = jnp.maximum(macc[head], jnp.maximum(s[:, :128], s[:, 128:]))

    def weigh(half):
        rows = slice(256 * half, 256 * half + 256)
        for head in range(2):
            v0, v1, factor, acc = heads[head][4:]
            m = jnp.broadcast_to(jnp.max(macc[head, rows], axis=1, keepdims=True), (256, 128))
            mrow[head, rows] = m
            for j in range(NZ):
                for side in range(2):
                    s = s_ref[head, j, rows, side * 128 : side * 128 + 128]
                    at = j * 256 + side * 128
                    p_ref[head, :, at : at + 128] = jnp.exp2((s - m) * factor).astype(BF)
            vs = kvb[:, :, :, v0:v1].reshape(2048, v1 - v0)
            acc[rows] = jnp.dot(p_ref[head], vs, preferred_element_type=F32)

    lane = lax.broadcasted_iota(jnp.int32, (TOK, 128), 1)

    def pack(half):
        for b in (2 * half, 2 * half + 1):
            rows = slice(b * TOK, b * TOK + TOK)
            wide, narrow = accw[rows, :], accn[rows, :]
            tile = narrow
            stats = (
                mrow[0, rows, :], mrow[1, rows, :],
                jnp.broadcast_to(wide[:, 192:193], (TOK, 128)), jnp.broadcast_to(narrow[:, 64:65], (TOK, 128)),
            )
            at = 64
            for stat in stats:
                for piece in split3(stat):
                    tile = jnp.where(lane == at, piece, tile)
                    at += 1
            tile = jnp.where(lane >= at, 0.0, tile)
            part[b, :, 0:128] = wide[:, 0:128].astype(BF)
            part[b, :, 128:256] = tile.astype(BF)
        if half == 0:
            send(part.at[0], ob.at[0], o_s, o_r.at[0], {"sp_1": yat(2)})
            send(part.at[1], ob.at[2], o_s, o_r.at[2], left_y)
        else:
            send(part.at[2], ob.at[1], o_s, o_r.at[1], right_y)

    def merge():
        blocks = [part.at[3]] + [ob.at[g] for g in range(3)]
        tiles = [block[:, 128:256].astype(F32) for block in blocks]
        stats = [s + pltpu.roll(s, 127, 1) + pltpu.roll(s, 126, 1) for s in tiles]
        top = jnp.maximum(jnp.maximum(stats[0], stats[1]), jnp.maximum(stats[2], stats[3]))
        factor = jnp.where(lane == 64, heads[0][6], heads[1][6])
        shares = [jnp.exp2((s - top) * factor) for s in stats]
        total = sum(pltpu.roll(w, 6, 1) * s for w, s in zip(shares, stats))
        inverse = pltpu.roll(1.0 / total, 122, 1)
        shares = [w * inverse for w in shares]
        wide = sum(w[:, 64:65] * block[:, 0:128].astype(F32) for w, block in zip(shares, blocks))
        narrow = sum(w[:, 67:68] * s for w, s in zip(shares, tiles))
        att[x, 0:TOK, 0:128] = wide.astype(BF)
        att[x, 0:TOK, 128:256] = narrow.astype(BF)

    def part_in():
        for o in range(3):
            wait_recv(ob.at[o], o_r.at[o])

    def att_out():
        for o in (2, 1, 3):
            mine = att.at[x, pl.ds(0, TOK)]
            send(mine, mine, x_s, x_r.at[o - 1], {"tp": xat(o)})
        for o in range(NX):
            peer = {"tp": xat(o)}
            send(att.at[x, pl.ds(112, 16)], att.at[x, pl.ds(128, 16)], e_s, e_r.at[0, o], device_of(after) | peer)
            send(att.at[x, pl.ds(0, 16)], att.at[x, pl.ds(144, 16)], e_s, e_r.at[1, o], device_of(before) | peer)

    def edges_out():
        load_res.wait()
        send(resid.at[pl.ds(112, 16)], resid.at[pl.ds(128, 16)], h_s, h_r.at[0], device_of(after))
        send(resid.at[pl.ds(0, 16)], resid.at[pl.ds(144, 16)], h_s, h_r.at[1], device_of(before))

    edges_out()
    gb_z(0)
    gb_y(0, 0)
    db_y(0, 0)
    kvz(1, 0)
    q_relay(1)
    kvz(1, 1)
    kvz(1, 2)
    kvz(1, 3)
    da_y(0)
    va_y(0)
    gb_z(1)
    kvz(2, 0)
    q_relay(2)
    scores(0)
    scores(1)
    kvz(2, 1)
    scores(2)
    kvz(2, 2)
    kvz(2, 3)
    gb_y(1, 0)
    va_z(0, 0)
    gb_y(1, 1)
    gb_z(2)
    scores(3)
    scores(4)
    kvz(3, 0)
    va_y(1)
    kvz(3, 1)
    kvz(3, 2)
    gb_y(2, 0)
    gb_y(2, 1)
    kvz(3, 3)
    va_z(0, 2)
    va_z(0, 1)
    db_z(0)
    da_y(1)
    da_z(0, 2)
    da_z(0, 1)
    va_z(1, 0)
    gb_y(1, 3)
    scores(5)
    gb_z(3)
    scores(6)
    gb_y(1, 4)
    va_y(2)
    va_z(0, 3)
    da_y(2)
    da_z(0, 3)
    kvz(4, 0)
    db_y(1, 0)
    va_z(1, 2)
    gb_y(2, 3)
    va_z(1, 1)
    db_z(1)
    scores(7)
    weigh(0)
    va_z(2, 0)
    da_z(1, 1)
    pack(0)
    weigh(1)
    va_z(1, 3)
    pack(1)
    da_z(0, 0)
    gb_z(4)
    db_y(1, 1)
    va_z(2, 2)
    db_y(2, 0)
    gb_y(1, 2)
    gb_y(2, 4)
    gb_y(1, 6)
    va_z(2, 1)
    da_z(1, 3)
    gb_y(1, 5)
    db_y(1, 2)
    db_z(2)
    va_z(3, 0)
    da_z(2, 1)
    va_z(2, 3)
    part_in()
    merge()
    att_out()
    da_z(1, 2)
    da_z(1, 0)
    va_z(3, 2)
    va_z(3, 1)
    gb_y(1, 7)
    da_z(2, 3)
    db_y(2, 1)
    db_z(3)
    va_z(4, 0)
    gb_y(2, 2)
    da_z(3, 1)
    gb_y(2, 6)
    va_z(3, 3)
    da_z(2, 2)
    gb_y(2, 5)
    db_y(2, 2)
    da_z(2, 0)
    va_z(4, 2)
    db_y(1, 3)
    va_z(4, 1)
    load_ow.wait()
    load_gain.wait()
    load_conv.wait()
    wait_recv(resid.at[pl.ds(128, 16)], h_r.at[0])
    wait_recv(resid.at[pl.ds(144, 16)], h_r.at[1])
    for o in (2, 1, 3):
        wait_recv(att.at[xat(-o), pl.ds(0, TOK)], x_r.at[o - 1])
    for o in range(NX):
        wait_recv(att.at[xat(-o), pl.ds(128, 16)], e_r.at[0, o])
        wait_recv(att.at[xat(-o), pl.ds(144, 16)], e_r.at[1, o])

    ss = jnp.zeros((ROWS, 1), F32)
    for n in range(8):
        cols = slice(n * 256, n * 256 + 256)
        total = resid[:, cols].astype(F32)
        for h in range(NX):
            total = total + jnp.dot(att[h, :, 0:192], ow[h * 192 : h * 192 + 192, cols], preferred_element_type=F32)
        rounded = total.astype(BF)
        stream[:, cols] = rounded
        wide = rounded.astype(F32)
        ss = ss + jnp.sum(wide * wide, axis=1, keepdims=True)
    scale = lax.rsqrt(ss * (1.0 / D) + 1e-06)
    for n in range(8):
        cols = slice(n * 256, n * 256 + 256)
        scaled = stream[:, cols].astype(F32) * scale
        normed[n] = (scaled * gain[cols].astype(F32).reshape(1, 256)).astype(BF)
    da_z(3, 3)
    db_y(1, 4)
    db_z(4)
    da_z(4, 1)
    db_y(1, 5)
    va_z(4, 3)
    gb_y(2, 7)

    def gate_rows(zz, cols):
        return gb[zz, :, :, 0:32, cols].reshape(256, 256)

    def value_rows(zz, cols):
        return jnp.concatenate([gb[zz, :, :, 32:48, cols], va[zz, :, :, :, cols]], axis=2).reshape(256, 256)

    def up(weights, rows, js, n):
        total = None
        for j in js:
            zz = zat(offsets[j])
            w = weights(zz, slice(n * 256, n * 256 + 256))
            term = jnp.dot(normed[zz, 0:rows], w, preferred_element_type=F32)
            total = term if total is None else total + term
        return total

    def arrived(buf, sems, j):
        wait_recv(buf.at[zat(offsets[j]), :, other], sems.at[j])

    for j in range(7):
        arrived(gb, ring_sems[5], j)
    for n in range(3):
        gacc[:, n * 256 : n * 256 + 256] = up(gate_rows, ROWS, range(7), n)
    db_y(1, 6)
    da_z(3, 2)
    db_y(2, 3)
    for j in range(7):
        arrived(va, ring_sems[17], j)
    for n in range(3):
        vacc[:, n * 256 : n * 256 + 256] = up(value_rows, TOK, range(7), n)
    da_z(3, 0)
    db_y(2, 4)
    arrived(gb, ring_sems[5], 7)
    arrived(va, ring_sems[17], 7)
    for n in range(3):
        cols = slice(n * 256, n * 256 + 256)
        gate[:, cols] = (gacc[:, cols] + up(gate_rows, ROWS, (7,), n)).astype(BF)
        value[:, cols] = (vacc[:, cols] + up(value_rows, TOK, (7,), n)).astype(BF)
    db_y(1, 7)
    da_z(4, 3)

    row = lax.broadcasted_iota(jnp.int32, (TOK, 256), 0)
    for n in range(3):
        cols = slice(n * 256, n * 256 + 256)
        g = gate[0:TOK, cols].astype(F32)
        edge = gate[TOK:ROWS, cols].astype(F32)
        first = jnp.where(place > 0, edge[15:16], 0.0)
        last = jnp.where(place < 63, edge[16:17], 0.0)
        low = jnp.where(row == 0, first, pltpu.roll(g, 1, 0))
        high = jnp.where(row == TOK - 1, last, pltpu.roll(g, TOK - 1, 0))
        cw = conv_w[:, cols].astype(F32)
        mixed = low * cw[0:1] + g * cw[1:2] + high * cw[2:3]
        silu = mixed / (1.0 + jnp.exp(-mixed))
        act[:, cols] = (silu * value[:, cols].astype(F32)).astype(BF)

    for j in range(NZ):
        zz = zat(offsets[j])
        arrived(da, ring_sems[23], j)
        arrived(db, ring_sems[11], j)
        w = jnp.concatenate([da[zz], db[zz]], axis=2).reshape(256, FFD)
        d = lax.dot_general(act[...], w, (((1,), (1,)), ((), ())), preferred_element_type=F32)
        fp[j] = d.astype(BF).reshape(NX, 32, 256)
        for o in (2, 1, 3):
            peer = xat(o)
            send(fp.at[j, peer], fr.at[j, x], f_s, f_r.at[j, o - 1], {"tp": peer})
        if j == 3:
            db_y(2, 5)
        if j == 4:
            db_y(2, 6)
        if j == 5:
            da_z(4, 2)
            da_z(4, 0)
        if j == 6:
            db_y(2, 7)

    rows = pl.ds(pl.multiple_of(x * 32, 32), 32)
    for j in range(NZ):
        cols = pl.ds(pl.multiple_of(zat(offsets[j]) * 256, 256), 256)
        total = stream[rows, cols].astype(F32) + fp[j, x].astype(F32)
        for o in (1, 3, 2):
            wait_recv(fr.at[j, xat(-o)], f_r.at[j, o - 1])
            total = total + fr[j, xat(-o)].astype(F32)
        out_ref[:, cols] = total.astype(BF)

    wait_send(kvb.at[pl.ds(0, 7), 0], kvz_s)
    wait_send(qb.at[pl.ds(0, 3)], q_s)
    wait_send(kvb.at[:, 0], pk_s)
    for buf, (z_s, _, y_s, _, p_s, _) in ((gb, ring_sems[0:6]), (db, ring_sems[6:12])):
        wait_send(buf.at[pl.ds(0, 7), 0, 0], z_s)
        wait_send(buf.at[:, pl.ds(0, 3), 0], y_s)
        wait_send(buf.at[:, :, 0], p_s)
    for buf, (z_s, _, y_s, _, p_s, _) in ((va, ring_sems[12:18]), (da, ring_sems[18:24])):
        wait_send(buf.at[pl.ds(0, 7), :, 0], z_s)
        wait_send(buf.at[0, pl.ds(0, 3), 0], y_s)
        wait_send(buf.at[:, :, 0], p_s)
    wait_send(part.at[pl.ds(0, 3)], o_s)
    wait_send(att.at[pl.ds(0, 3), pl.ds(0, TOK)], x_s)
    wait_send(att.at[:, pl.ds(0, 32)], e_s)
    wait_send(resid.at[pl.ds(0, 32)], h_s)
    wait_send(fp.at[:, pl.ds(0, 3)], f_s)


def layer(*operands):
    vmem = pl.BlockSpec(memory_space=pltpu.VMEM)
    hbm = pl.BlockSpec(memory_space=pltpu.HBM)
    dma = pltpu.SemaphoreType.DMA
    scratch = [
        pltpu.VMEM((D,), BF),
        pltpu.VMEM((3, FFD), BF),
        pltpu.VMEM((320, TOK), BF),
        pltpu.VMEM((TOK, 512), BF),
        pltpu.VMEM((64, TOK), BF),
        pltpu.VMEM((512, 384), BF),
        pltpu.VMEM((32, TOK), F32),
        pltpu.VMEM((NZ, 2, TOK, 512), BF),
        pltpu.VMEM((NY, TOK, 384), BF),
        pltpu.VMEM((NZ, NY, 2, 48, FFD), BF),
        pltpu.VMEM((NZ, NY, 2, 16, FFD), BF),
        pltpu.VMEM((NZ, NY, 2, 16, FFD), BF),
        pltpu.VMEM((NZ, NY, 2, 16, FFD), BF),
        pltpu.VMEM((768, D), BF),
        pltpu.VMEM((ROWS, D), BF),
        pltpu.VMEM((2, NZ, 512, 256), F32),
        pltpu.VMEM((2, 256, 2048), BF),
        pltpu.VMEM((2, 512, 128), F32),
        pltpu.VMEM((2, 512, 128), F32),
        pltpu.VMEM((512, 256), F32),
        pltpu.VMEM((512, 128), F32),
        pltpu.VMEM((NY, TOK, 256), BF),
        pltpu.VMEM((NY, TOK, 256), BF),
        pltpu.VMEM((NX, ROWS, 256), BF),
        pltpu.VMEM((ROWS, D), BF),
        pltpu.VMEM((NZ, ROWS, 256), BF),
        pltpu.VMEM((ROWS, FFD), F32),
        pltpu.VMEM((TOK, FFD), F32),
        pltpu.VMEM((ROWS, FFD), BF),
        pltpu.VMEM((TOK, FFD), BF),
        pltpu.VMEM((TOK, FFD), BF),
        pltpu.VMEM((NZ, NX, 32, 256), BF),
        pltpu.VMEM((NZ, NX, 32, 256), BF),
        dma, dma((2, 4, 4)), dma, dma((2, 2)), dma, dma((8,)), dma, dma((3,)), dma, dma((3,)),
        dma, dma((2, 4)), dma, dma((2,)), dma, dma((NZ, 3)), dma((14,)),
    ]
    scratch += 2 * [dma, dma((2, 4)), dma, dma((2, 2, 8)), dma, dma((8,))]
    scratch += 2 * [dma, dma((2, 4, 4)), dma, dma((2, 2)), dma, dma((8,))]
    return pl.pallas_call(
        kernel,
        out_shape=pltpu.VMEM((32, D), BF),
        in_specs=[hbm] * 12,
        out_specs=vmem,
        scratch_shapes=scratch,
        compiler_params=pltpu.CompilerParams(collective_id=0, has_side_effects=True),
    )(*operands)


def body(
    queries, latents, shared_key, expand_weight, residual, out_weight,
    norm_gain, gate_weight, value_weight, conv_weight, down_weight,
):
    frequency = (10000.0 ** (-np.arange(ROPE // 2) / (ROPE // 2))).astype(np.float32)
    return layer(
        norm_gain, conv_weight, queries.T, latents, shared_key.T, expand_weight, gate_weight, value_weight,
        down_weight.T, np.ascontiguousarray(np.broadcast_to(frequency[:, None], (ROPE // 2, TOK))),
        residual, out_weight,
    )


def solution(mesh):
    split = Mesh(mesh.devices.reshape(NZ, NY, 2, mesh.shape["tp"]), ("sp_0", "sp_1", "sp_2", "tp"))
    placed = (
        P(SP, "tp"),
        P(SP, None),
        P(SP, None),
        P(None, "tp"),
        P(SP, None),
        P(),
        P(),
        P(SP, "tp"),
        P(SP, "tp"),
        P(None, "tp"),
        P("tp", SP),
    )
    return jax.shard_map(
        body, mesh=split, in_specs=placed, out_specs=P(SP_TP, None), check_vma=False
    )
```

```python
import functools

import jax
import jax.numpy as jnp
import numpy as np
from jax import lax
from jax.experimental import pallas as pl
from jax.experimental.pallas import tpu as pltpu
from jax.sharding import Mesh
from jax.sharding import PartitionSpec as P

NOPE_A = 128
VAL_A = 128
NOPE_B = 64
VAL_B = 64
ROPE = 64
SP = ("sp_0", "sp_1", "sp_2")
SP_TP = ("sp_0", "sp_1", "sp_2", "tp")
NZ, NY, NX = 8, 4, 4
TOK = 128
ROWS = TOK + 32
D = 2048
FFD = 768
MESH = pl.DeviceIdType.MESH
LOG2E = 1.4426950408889634
F32 = jnp.float32
BF = jnp.bfloat16


def split3(v):
    hi = v.astype(BF).astype(F32)
    rest = v - hi
    mid = rest.astype(BF).astype(F32)
    return hi, mid, rest - mid


def kernel(
    gain_hbm, conv_hbm, q_hbm, lat_hbm, key_hbm, ew_hbm, gate_hbm, value_hbm, dn_hbm, freq_hbm, resid_hbm, ow_hbm,
    out_ref,
    gain, conv_w, q_t, lat, key_t, ew, freq, kvb, qb, gb, va, da, db, ow, resid, s_ref, p_ref, macc, mrow, accw, accn,
    part, ob, att, stream, normed, gacc, vacc, gate, value, act, fp, fr,
    kvz_s, kvz_r, q_s, q_r, pk_s, pk_r, o_s, o_r, x_s, x_r, e_s, e_r, h_s, h_r, f_s, f_r, loc, *ring_sems,
):
    z = lax.axis_index("sp_0")
    y = lax.axis_index("sp_1")
    c = lax.axis_index("sp_2")
    x = lax.axis_index("tp")
    other = 1 - c

    def zat(k):
        return lax.rem(z + (k + NZ), NZ)

    def yat(k):
        return lax.rem(y + (k + NY), NY)

    def xat(k):
        return lax.rem(x + (k + NX), NX)

    right_z, left_z = {"sp_0": zat(1)}, {"sp_0": zat(-1)}
    right_y, left_y = {"sp_1": yat(1)}, {"sp_1": yat(-1)}
    partner = {"sp_2": other}
    place = (z * NY + y) * 2 + c
    after = lax.rem(place + 1, 64)
    before = lax.rem(place + 63, 64)

    def device_of(i):
        return {"sp_0": i // 8, "sp_1": lax.rem(i // 2, 4), "sp_2": lax.rem(i, 2)}

    def send(src, dst, ssem, rsem, dev):
        pltpu.make_async_remote_copy(
            src_ref=src, dst_ref=dst, send_sem=ssem, recv_sem=rsem, device_id=dev, device_id_type=MESH
        ).start()

    def wait_recv(ref, sem):
        pltpu.make_async_remote_copy(
            src_ref=ref, dst_ref=ref, send_sem=sem, recv_sem=sem, device_id=partner, device_id_type=MESH
        ).wait_recv()

    def wait_send(ref, sem):
        pltpu.make_async_remote_copy(
            src_ref=ref, dst_ref=ref, send_sem=sem, recv_sem=sem, device_id=partner, device_id_type=MESH
        ).wait_send()

    barrier = pltpu.get_barrier_semaphore()
    greeted = [
        partner, right_z, left_z, right_y, left_y, {"sp_1": yat(2)},
        {"tp": xat(1)}, {"tp": xat(2)}, {"tp": xat(3)},
    ]
    greeted += [device_of(i) | {"tp": xat(o)} for i in (after, before) for o in range(NX)]
    for dev in greeted:
        pl.semaphore_signal(barrier, inc=1, device_id=dev, device_id_type=MESH)

    def load(src, dst, i):
        copy = pltpu.make_async_copy(src, dst, loc.at[i])
        copy.start()
        return copy

    first_loads = [
        load(lat_hbm, lat, 0), load(ew_hbm, ew, 1), load(key_hbm, key_t, 2), load(freq_hbm, freq, 3),
        load(q_hbm, q_t, 4),
    ]
    weight_loads = [
        load(gate_hbm, gb.at[z, y, c, pl.ds(0, 32)], 5),
        load(value_hbm.at[pl.ds(0, 16)], gb.at[z, y, c, pl.ds(32, 16)], 6),
        load(value_hbm.at[pl.ds(16, 16)], va.at[z, y, c], 7),
        load(dn_hbm.at[pl.ds(0, 16)], da.at[z, y, c], 12), load(dn_hbm.at[pl.ds(16, 16)], db.at[z, y, c], 13),
    ]
    load_res = load(resid_hbm, resid.at[pl.ds(0, TOK)], 8)
    load_ow = load(ow_hbm, ow, 9)
    load_gain = load(gain_hbm, gain, 10)
    load_conv = load(conv_hbm, conv_w, 11)
    pl.semaphore_wait(barrier, len(greeted))
    for copy in first_loads:
        copy.wait()

    position = (lax.broadcasted_iota(jnp.int32, (32, TOK), 1) + place * TOK).astype(F32)
    angles = position * freq[...]
    cosine, sine = jnp.cos(angles), jnp.sin(angles)

    def turned(a, b):
        a, b = a.astype(F32), b.astype(F32)
        return [a * cosine - b * sine, b * cosine + a * sine]

    def upright(pieces):
        return jnp.transpose(jnp.concatenate(pieces, axis=0), (1, 0))

    nothing = jnp.zeros((64, TOK), F32)
    expanded = jnp.dot(lat[...], ew[...], preferred_element_type=F32)
    key_rows = upright(turned(key_t[0:32, :], key_t[32:64, :]) + [nothing])
    low_lane = lax.broadcasted_iota(jnp.int32, (TOK, 128), 1) < 64
    swapped = pltpu.roll(expanded[:, 256:384], 64, 1)
    kvb[0, 0, :, 0:128] = expanded[:, 0:128].astype(BF)
    kvb[0, 0, :, 128:256] = jnp.where(low_lane, key_rows, swapped).astype(BF)
    kvb[0, 0, :, 256:384] = expanded[:, 128:256].astype(BF)
    kvb[0, 0, :, 384:512] = jnp.where(low_lane, swapped, 1.0).astype(BF)
    qb[3, :, 0:128] = upright([q_t[0:128, :].astype(F32)]).astype(BF)
    qb[3, :, 128:256] = upright(turned(q_t[192:224, :], q_t[224:256, :]) + [nothing]).astype(BF)
    qb[3, :, 256:384] = upright(
        turned(q_t[256:288, :], q_t[288:320, :]) + [q_t[128:192, :].astype(F32)]
    ).astype(BF)

    def rows_of(slot, h):
        return kvb.at[slot, 0, pl.ds(32 * h, 32)]

    def slot_of(s, ahead):
        return 0 if s == 0 else 7 if s == 4 else 2 * s - 1 + ahead

    def kv_out(s, h):
        if s < 3 or h < 2:
            send(rows_of(slot_of(s, 0), h), rows_of(slot_of(s + 1, 0), h), kvz_s, kvz_r.at[0, s, h], right_z)
        if s < 3 or h >= 2:
            send(rows_of(slot_of(s, 1), h), rows_of(slot_of(s + 1, 1), h), kvz_s, kvz_r.at[1, s, h], left_z)

    def kv_across(slot):
        send(kvb.at[slot, 0], kvb.at[slot, 1], pk_s, pk_r.at[slot], partner)

    def kvz(s, h):
        if s < 4:
            wait_recv(rows_of(slot_of(s, 0), h), kvz_r.at[0, s - 1, h])
            wait_recv(rows_of(slot_of(s, 1), h), kvz_r.at[1, s - 1, h])
            kv_out(s, h)
            if h == 3:
                kv_across(2 * s - 1)
                kv_across(2 * s)
        else:
            for q in range(4):
                wait_recv(rows_of(7, q), kvz_r.at[q // 2, 3, q])
            kv_across(7)

    def q_relay(s):
        if s == 1:
            wait_recv(qb.at[1], q_r.at[0, 0])
            send(qb.at[1, pl.ds(0, 64)], qb.at[0, pl.ds(0, 64)], q_s, q_r.at[0, 1], right_y)
            wait_recv(qb.at[2], q_r.at[1, 0])
            send(qb.at[2, pl.ds(64, 64)], qb.at[0, pl.ds(64, 64)], q_s, q_r.at[1, 1], left_y)
        else:
            wait_recv(qb.at[0, pl.ds(0, 64)], q_r.at[0, 1])
            wait_recv(qb.at[0, pl.ds(64, 64)], q_r.at[1, 1])

    for q in range(4):
        kv_out(0, q)
    send(qb.at[3], qb.at[1], q_s, q_r.at[0, 0], right_y)
    send(qb.at[3], qb.at[2], q_s, q_r.at[1, 0], left_y)
    kv_across(0)
    macc[...] = jnp.full((2, 512, 128), -3e38, F32)

    for copy in weight_loads:
        copy.wait()

    offsets = [0, -1, 1, -2, 2, -3, 3, 4]

    def z_then_y(buf, z_s, z_r, y_s, y_r, p_s, p_r):
        def half(zz, yy, h):
            return buf.at[zz, yy, c, :, pl.ds(384 * h, 384)]

        def out(zz, j):
            block = buf.at[zz, y, c]
            send(block, block, y_s, y_r.at[0, 0, j], right_y)
            send(block, block, y_s, y_r.at[1, 0, j], left_y)
            send(block, block, p_s, p_r.at[j], partner)

        def on_z(s):
            lo, hi = zat(-s), zat(s)
            if s == 4:
                wait_recv(half(lo, y, 0), z_r.at[0, 3])
                wait_recv(half(lo, y, 1), z_r.at[1, 3])
                out(lo, 7)
                return
            for way, (zz, dev) in enumerate(((lo, right_z), (hi, left_z))):
                block = buf.at[zz, y, c]
                if s > 0:
                    wait_recv(block, z_r.at[way, s - 1])
                src = block if s < 3 else half(zz, y, way)
                send(src, src, z_s, z_r.at[way, s], dev)
            if s > 0:
                out(lo, 2 * s - 1)
                out(hi, 2 * s)

        def on_y(s, j):
            zz = zat(offsets[j])
            a, b, far = yat(-1), yat(1), yat(2)
            if s == 0:
                out(z, 0)
            elif s == 1:
                for way, (yy, dev) in enumerate(((a, right_y), (b, left_y))):
                    wait_recv(buf.at[zz, yy, c], y_r.at[way, 0, j])
                    src = half(zz, yy, way)
                    send(src, src, y_s, y_r.at[way, 1, j], dev)
                for yy in (a, b):
                    send(buf.at[zz, yy, c], buf.at[zz, yy, c], p_s, p_r.at[j], partner)
            else:
                wait_recv(half(zz, far, 0), y_r.at[0, 1, j])
                wait_recv(half(zz, far, 1), y_r.at[1, 1, j])
                send(buf.at[zz, far, c], buf.at[zz, far, c], p_s, p_r.at[j], partner)

        return on_z, on_y

    def y_then_z(buf, z_s, z_r, y_s, y_r, p_s, p_r):
        def half(zz, yy, h):
            return buf.at[zz, yy, c, :, pl.ds(384 * h, 384)]

        def on_y(s):
            a, b, far = yat(-1), yat(1), yat(2)
            if s == 2:
                wait_recv(half(z, far, 0), y_r.at[0, 1])
                wait_recv(half(z, far, 1), y_r.at[1, 1])
                return
            for way, (yy, dev) in enumerate(((a, right_y), (b, left_y))):
                if s == 0:
                    src = buf.at[z, y, c]
                else:
                    wait_recv(buf.at[z, yy, c], y_r.at[way, 0])
                    src = half(z, yy, way)
                send(src, src, y_s, y_r.at[way, s], dev)

        def on_z(s, r):
            yy = yat((0, -1, 1, 2)[r])
            lo, hi = zat(-s), zat(s)
            if s == 4:
                wait_recv(half(lo, yy, 0), z_r.at[0, 3, r])
                wait_recv(half(lo, yy, 1), z_r.at[1, 3, r])
            else:
                for way, (zz, dev) in enumerate(((lo, right_z), (hi, left_z))):
                    block = buf.at[zz, yy, c]
                    if s > 0:
                        wait_recv(block, z_r.at[way, s - 1, r])
                    src = block if s < 3 else half(zz, yy, way)
                    send(src, src, z_s, z_r.at[way, s, r], dev)
            for ahead, zz in enumerate((lo, hi) if 0 < s < 4 else (lo,)):
                send(buf.at[zz, yy, c], buf.at[zz, yy, c], p_s, p_r.at[slot_of(s, ahead)], partner)

        return on_y, on_z

    gb_z, gb_y = z_then_y(gb, *ring_sems[0:6])
    db_z, db_y = z_then_y(db, *ring_sems[6:12])
    va_y, va_z = y_then_z(va, *ring_sems[12:18])
    da_y, da_z = y_then_z(da, *ring_sems[18:24])

    heads = (
        (0, 256, 0, 256, 256, 512, (NOPE_A + ROPE) ** (-0.5) * LOG2E, accw),
        (256, 384, 128, 256, 384, 512, (NOPE_B + ROPE) ** (-0.5) * LOG2E, accn),
    )

    def scores(j):
        wait_recv(kvb.at[j, 1], pk_r.at[j])
        for head in range(2):
            q0, q1, k0, k1 = heads[head][:4]
            qs = qb[:, :, q0:q1].reshape(512, q1 - q0)
            ks = kvb[j, :, :, k0:k1].reshape(256, k1 - k0)
            s = lax.dot_general(qs, ks, (((1,), (1,)), ((), ())), preferred_element_type=F32)
            s_ref[head, j] = s
            macc[head] = jnp.maximum(macc[head], jnp.maximum(s[:, :128], s[:, 128:]))

    def weigh(half):
        rows = slice(256 * half, 256 * half + 256)
        for head in range(2):
            v0, v1, factor, acc = heads[head][4:]
            m = jnp.broadcast_to(jnp.max(macc[head, rows], axis=1, keepdims=True), (256, 128))
            mrow[head, rows] = m
            for j in range(NZ):
                for side in range(2):
                    s = s_ref[head, j, rows, side * 128 : side * 128 + 128]
                    at = j * 256 + side * 128
                    p_ref[head, :, at : at + 128] = jnp.exp2((s - m) * factor).astype(BF)
            vs = kvb[:, :, :, v0:v1].reshape(2048, v1 - v0)
            acc[rows] = jnp.dot(p_ref[head], vs, preferred_element_type=F32)

    lane = lax.broadcasted_iota(jnp.int32, (TOK, 128), 1)

    def pack(half):
        for b in (2 * half, 2 * half + 1):
            rows = slice(b * TOK, b * TOK + TOK)
            wide, narrow = accw[rows, :], accn[rows, :]
            tile = narrow
            stats = (
                mrow[0, rows, :], mrow[1, rows, :],
                jnp.broadcast_to(wide[:, 192:193], (TOK, 128)), jnp.broadcast_to(narrow[:, 64:65], (TOK, 128)),
            )
            at = 64
            for stat in stats:
                for piece in split3(stat):
                    tile = jnp.where(lane == at, piece, tile)
                    at += 1
            tile = jnp.where(lane >= at, 0.0, tile)
            part[b, :, 0:128] = wide[:, 0:128].astype(BF)
            part[b, :, 128:256] = tile.astype(BF)
        if half == 0:
            send(part.at[0], ob.at[0], o_s, o_r.at[0], {"sp_1": yat(2)})
            send(part.at[1], ob.at[2], o_s, o_r.at[2], left_y)
        else:
            send(part.at[2], ob.at[1], o_s, o_r.at[1], right_y)

    def merge():
        blocks = [part.at[3]] + [ob.at[g] for g in range(3)]
        tiles = [block[:, 128:256].astype(F32) for block in blocks]
        stats = [s + pltpu.roll(s, 127, 1) + pltpu.roll(s, 126, 1) for s in tiles]
        top = jnp.maximum(jnp.maximum(stats[0], stats[1]), jnp.maximum(stats[2], stats[3]))
        factor = jnp.where(lane == 64, heads[0][6], heads[1][6])
        shares = [jnp.exp2((s - top) * factor) for s in stats]
        total = sum(pltpu.roll(w, 6, 1) * s for w, s in zip(shares, stats))
        inverse = pltpu.roll(1.0 / total, 122, 1)
        shares = [w * inverse for w in shares]
        wide = sum(w[:, 64:65] * block[:, 0:128].astype(F32) for w, block in zip(shares, blocks))
        narrow = sum(w[:, 67:68] * s for w, s in zip(shares, tiles))
        att[x, 0:TOK, 0:128] = wide.astype(BF)
        att[x, 0:TOK, 128:256] = narrow.astype(BF)

    def part_in():
        for o in range(3):
            wait_recv(ob.at[o], o_r.at[o])

    def att_out():
        for o in (2, 1, 3):
            mine = att.at[x, pl.ds(0, TOK)]
            send(mine, mine, x_s, x_r.at[o - 1], {"tp": xat(o)})
        for o in range(NX):
            peer = {"tp": xat(o)}
            send(att.at[x, pl.ds(112, 16)], att.at[x, pl.ds(128, 16)], e_s, e_r.at[0, o], device_of(after) | peer)
            send(att.at[x, pl.ds(0, 16)], att.at[x, pl.ds(144, 16)], e_s, e_r.at[1, o], device_of(before) | peer)

    def edges_out():
        load_res.wait()
        send(resid.at[pl.ds(112, 16)], resid.at[pl.ds(128, 16)], h_s, h_r.at[0], device_of(after))
        send(resid.at[pl.ds(0, 16)], resid.at[pl.ds(144, 16)], h_s, h_r.at[1], device_of(before))

    edges_out()
    gb_z(0)
    gb_y(0, 0)
    db_y(0, 0)
    kvz(1, 0)
    q_relay(1)
    kvz(1, 1)
    kvz(1, 2)
    kvz(1, 3)
    da_y(0)
    va_y(0)
    gb_z(1)
    kvz(2, 0)
    q_relay(2)
    scores(0)
    scores(1)
    kvz(2, 1)
    scores(2)
    kvz(2, 2)
    kvz(2, 3)
    gb_y(1, 0)
    va_z(0, 0)
    gb_y(1, 1)
    gb_z(2)
    scores(3)
    scores(4)
    kvz(3, 0)
    va_y(1)
    kvz(3, 1)
    kvz(3, 2)
    gb_y(2, 0)
    gb_y(2, 1)
    kvz(3, 3)
    va_z(0, 2)
    va_z(0, 1)
    db_z(0)
    da_y(1)
    da_z(0, 2)
    da_z(0, 1)
    va_z(1, 0)
    gb_y(1, 3)
    scores(5)
    gb_z(3)
    scores(6)
    gb_y(1, 4)
    va_y(2)
    va_z(0, 3)
    da_y(2)
    da_z(0, 3)
    kvz(4, 0)
    db_y(1, 0)
    va_z(1, 2)
    gb_y(2, 3)
    va_z(1, 1)
    db_z(1)
    scores(7)
    weigh(0)
    va_z(2, 0)
    da_z(1, 1)
    pack(0)
    weigh(1)
    va_z(1, 3)
    pack(1)
    da_z(0, 0)
    gb_z(4)
    db_y(1, 1)
    va_z(2, 2)
    db_y(2, 0)
    gb_y(1, 2)
    gb_y(2, 4)
    gb_y(1, 6)
    va_z(2, 1)
    da_z(1, 3)
    gb_y(1, 5)
    db_y(1, 2)
    db_z(2)
    va_z(3, 0)
    da_z(2, 1)
    va_z(2, 3)
    part_in()
    merge()
    att_out()
    da_z(1, 2)
    da_z(1, 0)
    va_z(3, 2)
    va_z(3, 1)
    gb_y(1, 7)
    da_z(2, 3)
    db_y(2, 1)
    db_z(3)
    va_z(4, 0)
    gb_y(2, 2)
    da_z(3, 1)
    gb_y(2, 6)
    va_z(3, 3)
    da_z(2, 2)
    gb_y(2, 5)
    db_y(2, 2)
    da_z(2, 0)
    va_z(4, 2)
    db_y(1, 3)
    va_z(4, 1)
    load_ow.wait()
    load_gain.wait()
    load_conv.wait()
    wait_recv(resid.at[pl.ds(128, 16)], h_r.at[0])
    wait_recv(resid.at[pl.ds(144, 16)], h_r.at[1])
    for o in (2, 1, 3):
        wait_recv(att.at[xat(-o), pl.ds(0, TOK)], x_r.at[o - 1])
    for o in range(NX):
        wait_recv(att.at[xat(-o), pl.ds(128, 16)], e_r.at[0, o])
        wait_recv(att.at[xat(-o), pl.ds(144, 16)], e_r.at[1, o])

    ss = jnp.zeros((ROWS, 1), F32)
    for n in range(8):
        cols = slice(n * 256, n * 256 + 256)
        total = resid[:, cols].astype(F32)
        for h in range(NX):
            total = total + jnp.dot(att[h, :, 0:192], ow[h * 192 : h * 192 + 192, cols], preferred_element_type=F32)
        rounded = total.astype(BF)
        stream[:, cols] = rounded
        wide = rounded.astype(F32)
        ss = ss + jnp.sum(wide * wide, axis=1, keepdims=True)
    scale = lax.rsqrt(ss * (1.0 / D) + 1e-06)
    for n in range(8):
        cols = slice(n * 256, n * 256 + 256)
        scaled = stream[:, cols].astype(F32) * scale
        normed[n] = (scaled * gain[cols].astype(F32).reshape(1, 256)).astype(BF)
    da_z(3, 3)
    db_y(1, 4)
    db_z(4)
    va_z(4, 3)
    gb_y(2, 7)

    def gate_rows(zz, cols):
        return gb[zz, :, :, 0:32, cols].reshape(256, 256)

    def value_rows(zz, cols):
        return jnp.concatenate([gb[zz, :, :, 32:48, cols], va[zz, :, :, :, cols]], axis=2).reshape(256, 256)

    def up(weights, rows, js, n):
        total = None
        for j in js:
            zz = zat(offsets[j])
            w = weights(zz, slice(n * 256, n * 256 + 256))
            term = jnp.dot(normed[zz, 0:rows], w, preferred_element_type=F32)
            total = term if total is None else total + term
        return total

    def arrived(buf, sems, j):
        wait_recv(buf.at[zat(offsets[j]), :, other], sems.at[j])

    for j in range(7):
        arrived(gb, ring_sems[5], j)
    for n in range(3):
        gacc[:, n * 256 : n * 256 + 256] = up(gate_rows, ROWS, range(7), n)
    db_y(1, 5)
    da_z(4, 1)
    db_y(1, 6)
    da_z(3, 2)
    for j in range(7):
        arrived(va, ring_sems[17], j)
    for n in range(3):
        vacc[:, n * 256 : n * 256 + 256] = up(value_rows, TOK, range(7), n)
    da_z(3, 0)
    arrived(gb, ring_sems[5], 7)
    arrived(va, ring_sems[17], 7)
    for n in range(3):
        cols = slice(n * 256, n * 256 + 256)
        gate[:, cols] = (gacc[:, cols] + up(gate_rows, ROWS, (7,), n)).astype(BF)
        value[:, cols] = (vacc[:, cols] + up(value_rows, TOK, (7,), n)).astype(BF)
    db_y(1, 7)

    row = lax.broadcasted_iota(jnp.int32, (TOK, 256), 0)
    for n in range(3):
        cols = slice(n * 256, n * 256 + 256)
        g = gate[0:TOK, cols].astype(F32)
        edge = gate[TOK:ROWS, cols].astype(F32)
        first = jnp.where(place > 0, edge[15:16], 0.0)
        last = jnp.where(place < 63, edge[16:17], 0.0)
        low = jnp.where(row == 0, first, pltpu.roll(g, 1, 0))
        high = jnp.where(row == TOK - 1, last, pltpu.roll(g, TOK - 1, 0))
        cw = conv_w[:, cols].astype(F32)
        mixed = low * cw[0:1] + g * cw[1:2] + high * cw[2:3]
        silu = mixed / (1.0 + jnp.exp(-mixed))
        act[:, cols] = (silu * value[:, cols].astype(F32)).astype(BF)

    for j in range(NZ):
        zz = zat(offsets[j])
        arrived(da, ring_sems[23], j)
        arrived(db, ring_sems[11], j)
        w = jnp.concatenate([da[zz], db[zz]], axis=2).reshape(256, FFD)
        d = lax.dot_general(act[...], w, (((1,), (1,)), ((), ())), preferred_element_type=F32)
        fp[j] = d.astype(BF).reshape(NX, 32, 256)
        for o in (2, 1, 3):
            peer = xat(o)
            send(fp.at[j, peer], fr.at[j, x], f_s, f_r.at[j, o - 1], {"tp": peer})
        if j == 0:
            db_y(2, 3)
            da_z(4, 3)
        if j == 1:
            db_y(2, 4)
        if j == 2:
            db_y(2, 5)
        if j == 3:
            db_y(2, 6)
        if j == 4:
            da_z(4, 2)
        if j == 5:
            da_z(4, 0)
        if j == 6:
            db_y(2, 7)

    rows = pl.ds(pl.multiple_of(x * 32, 32), 32)
    for j in range(NZ):
        cols = pl.ds(pl.multiple_of(zat(offsets[j]) * 256, 256), 256)
        total = stream[rows, cols].astype(F32) + fp[j, x].astype(F32)
        for o in (1, 3, 2):
            wait_recv(fr.at[j, xat(-o)], f_r.at[j, o - 1])
            total = total + fr[j, xat(-o)].astype(F32)
        out_ref[:, cols] = total.astype(BF)

    wait_send(kvb.at[pl.ds(0, 7), 0], kvz_s)
    wait_send(qb.at[pl.ds(0, 3)], q_s)
    wait_send(kvb.at[:, 0], pk_s)
    for buf, (z_s, _, y_s, _, p_s, _) in ((gb, ring_sems[0:6]), (db, ring_sems[6:12])):
        wait_send(buf.at[pl.ds(0, 7), 0, 0], z_s)
        wait_send(buf.at[:, pl.ds(0, 3), 0], y_s)
        wait_send(buf.at[:, :, 0], p_s)
    for buf, (z_s, _, y_s, _, p_s, _) in ((va, ring_sems[12:18]), (da, ring_sems[18:24])):
        wait_send(buf.at[pl.ds(0, 7), :, 0], z_s)
        wait_send(buf.at[0, pl.ds(0, 3), 0], y_s)
        wait_send(buf.at[:, :, 0], p_s)
    wait_send(part.at[pl.ds(0, 3)], o_s)
    wait_send(att.at[pl.ds(0, 3), pl.ds(0, TOK)], x_s)
    wait_send(att.at[:, pl.ds(0, 32)], e_s)
    wait_send(resid.at[pl.ds(0, 32)], h_s)
    wait_send(fp.at[:, pl.ds(0, 3)], f_s)


def layer(*operands):
    vmem = pl.BlockSpec(memory_space=pltpu.VMEM)
    hbm = pl.BlockSpec(memory_space=pltpu.HBM)
    dma = pltpu.SemaphoreType.DMA
    scratch = [
        pltpu.VMEM((D,), BF),
        pltpu.VMEM((3, FFD), BF),
        pltpu.VMEM((320, TOK), BF),
        pltpu.VMEM((TOK, 512), BF),
        pltpu.VMEM((64, TOK), BF),
        pltpu.VMEM((512, 384), BF),
        pltpu.VMEM((32, TOK), F32),
        pltpu.VMEM((NZ, 2, TOK, 512), BF),
        pltpu.VMEM((NY, TOK, 384), BF),
        pltpu.VMEM((NZ, NY, 2, 48, FFD), BF),
        pltpu.VMEM((NZ, NY, 2, 16, FFD), BF),
        pltpu.VMEM((NZ, NY, 2, 16, FFD), BF),
        pltpu.VMEM((NZ, NY, 2, 16, FFD), BF),
        pltpu.VMEM((768, D), BF),
        pltpu.VMEM((ROWS, D), BF),
        pltpu.VMEM((2, NZ, 512, 256), F32),
        pltpu.VMEM((2, 256, 2048), BF),
        pltpu.VMEM((2, 512, 128), F32),
        pltpu.VMEM((2, 512, 128), F32),
        pltpu.VMEM((512, 256), F32),
        pltpu.VMEM((512, 128), F32),
        pltpu.VMEM((NY, TOK, 256), BF),
        pltpu.VMEM((NY, TOK, 256), BF),
        pltpu.VMEM((NX, ROWS, 256), BF),
        pltpu.VMEM((ROWS, D), BF),
        pltpu.VMEM((NZ, ROWS, 256), BF),
        pltpu.VMEM((ROWS, FFD), F32),
        pltpu.VMEM((TOK, FFD), F32),
        pltpu.VMEM((ROWS, FFD), BF),
        pltpu.VMEM((TOK, FFD), BF),
        pltpu.VMEM((TOK, FFD), BF),
        pltpu.VMEM((NZ, NX, 32, 256), BF),
        pltpu.VMEM((NZ, NX, 32, 256), BF),
        dma, dma((2, 4, 4)), dma, dma((2, 2)), dma, dma((8,)), dma, dma((3,)), dma, dma((3,)),
        dma, dma((2, 4)), dma, dma((2,)), dma, dma((NZ, 3)), dma((14,)),
    ]
    scratch += 2 * [dma, dma((2, 4)), dma, dma((2, 2, 8)), dma, dma((8,))]
    scratch += 2 * [dma, dma((2, 4, 4)), dma, dma((2, 2)), dma, dma((8,))]
    return pl.pallas_call(
        kernel,
        out_shape=pltpu.VMEM((32, D), BF),
        in_specs=[hbm] * 12,
        out_specs=vmem,
        scratch_shapes=scratch,
        compiler_params=pltpu.CompilerParams(collective_id=0, has_side_effects=True),
    )(*operands)


def body(
    queries, latents, shared_key, expand_weight, residual, out_weight,
    norm_gain, gate_weight, value_weight, conv_weight, down_weight,
):
    frequency = (10000.0 ** (-np.arange(ROPE // 2) / (ROPE // 2))).astype(np.float32)
    return layer(
        norm_gain, conv_weight, queries.T, latents, shared_key.T, expand_weight, gate_weight, value_weight,
        down_weight.T, np.ascontiguousarray(np.broadcast_to(frequency[:, None], (ROPE // 2, TOK))),
        residual, out_weight,
    )


def solution(mesh):
    split = Mesh(mesh.devices.reshape(NZ, NY, 2, mesh.shape["tp"]), ("sp_0", "sp_1", "sp_2", "tp"))
    placed = (
        P(SP, "tp"),
        P(SP, None),
        P(SP, None),
        P(None, "tp"),
        P(SP, None),
        P(),
        P(),
        P(SP, "tp"),
        P(SP, "tp"),
        P(None, "tp"),
        P("tp", SP),
    )
    return jax.shard_map(
        body, mesh=split, in_specs=placed, out_specs=P(SP_TP, None), check_vma=False
    )
```

```python
import functools

import jax
import jax.numpy as jnp
import numpy as np
from jax import lax
from jax.experimental import pallas as pl
from jax.experimental.pallas import tpu as pltpu
from jax.sharding import Mesh
from jax.sharding import PartitionSpec as P

NOPE_A = 128
VAL_A = 128
NOPE_B = 64
VAL_B = 64
ROPE = 64
SP = ("sp_0", "sp_1", "sp_2")
SP_TP = ("sp_0", "sp_1", "sp_2", "tp")
NZ, NY, NX = 8, 4, 4
TOK = 128
ROWS = TOK + 32
D = 2048
FFD = 768
MESH = pl.DeviceIdType.MESH
LOG2E = 1.4426950408889634
F32 = jnp.float32
BF = jnp.bfloat16


def split3(v):
    hi = v.astype(BF).astype(F32)
    rest = v - hi
    mid = rest.astype(BF).astype(F32)
    return hi, mid, rest - mid


def kernel(
    gain_hbm, conv_hbm, q_hbm, lat_hbm, key_hbm, ew_hbm, gate_hbm, value_hbm, dn_hbm, freq_hbm, resid_hbm, ow_hbm,
    out_ref,
    gain, conv_w, q_t, lat, key_t, ew, freq, kvb, qb, gb, va, da, db, ow, resid, s_ref, p_ref, macc, mrow, accw, accn,
    part, ob, att, stream, normed, gacc, vacc, gate, value, act, fp, fr,
    kvz_s, kvz_r, q_s, q_r, pk_s, pk_r, o_s, o_r, x_s, x_r, e_s, e_r, h_s, h_r, f_s, f_r, loc, *ring_sems,
):
    z = lax.axis_index("sp_0")
    y = lax.axis_index("sp_1")
    c = lax.axis_index("sp_2")
    x = lax.axis_index("tp")
    other = 1 - c

    def zat(k):
        return lax.rem(z + (k + NZ), NZ)

    def yat(k):
        return lax.rem(y + (k + NY), NY)

    def xat(k):
        return lax.rem(x + (k + NX), NX)

    right_z, left_z = {"sp_0": zat(1)}, {"sp_0": zat(-1)}
    right_y, left_y = {"sp_1": yat(1)}, {"sp_1": yat(-1)}
    partner = {"sp_2": other}
    place = (z * NY + y) * 2 + c
    after = lax.rem(place + 1, 64)
    before = lax.rem(place + 63, 64)

    def device_of(i):
        return {"sp_0": i // 8, "sp_1": lax.rem(i // 2, 4), "sp_2": lax.rem(i, 2)}

    def send(src, dst, ssem, rsem, dev):
        pltpu.make_async_remote_copy(
            src_ref=src, dst_ref=dst, send_sem=ssem, recv_sem=rsem, device_id=dev, device_id_type=MESH
        ).start()

    def wait_recv(ref, sem):
        pltpu.make_async_remote_copy(
            src_ref=ref, dst_ref=ref, send_sem=sem, recv_sem=sem, device_id=partner, device_id_type=MESH
        ).wait_recv()

    def wait_send(ref, sem):
        pltpu.make_async_remote_copy(
            src_ref=ref, dst_ref=ref, send_sem=sem, recv_sem=sem, device_id=partner, device_id_type=MESH
        ).wait_send()

    barrier = pltpu.get_barrier_semaphore()
    greeted = [
        partner, right_z, left_z, right_y, left_y, {"sp_1": yat(2)},
        {"tp": xat(1)}, {"tp": xat(2)}, {"tp": xat(3)},
    ]
    greeted += [device_of(i) | {"tp": xat(o)} for i in (after, before) for o in range(NX)]
    for dev in greeted:
        pl.semaphore_signal(barrier, inc=1, device_id=dev, device_id_type=MESH)

    def load(src, dst, i):
        copy = pltpu.make_async_copy(src, dst, loc.at[i])
        copy.start()
        return copy

    first_loads = [
        load(lat_hbm, lat, 0), load(ew_hbm, ew, 1), load(key_hbm, key_t, 2), load(freq_hbm, freq, 3),
        load(q_hbm, q_t, 4),
    ]
    weight_loads = [
        load(gate_hbm, gb.at[z, y, c, pl.ds(0, 32)], 5),
        load(value_hbm.at[pl.ds(0, 16)], gb.at[z, y, c, pl.ds(32, 16)], 6),
        load(value_hbm.at[pl.ds(16, 16)], va.at[z, y, c], 7),
        load(dn_hbm.at[pl.ds(0, 16)], da.at[z, y, c], 12), load(dn_hbm.at[pl.ds(16, 16)], db.at[z, y, c], 13),
    ]
    load_res = load(resid_hbm, resid.at[pl.ds(0, TOK)], 8)
    load_ow = load(ow_hbm, ow, 9)
    load_gain = load(gain_hbm, gain, 10)
    load_conv = load(conv_hbm, conv_w, 11)
    for copy in first_loads:
        copy.wait()

    position = (lax.broadcasted_iota(jnp.int32, (32, TOK), 1) + place * TOK).astype(F32)
    angles = position * freq[...]
    cosine, sine = jnp.cos(angles), jnp.sin(angles)

    def turned(a, b):
        a, b = a.astype(F32), b.astype(F32)
        return [a * cosine - b * sine, b * cosine + a * sine]

    def upright(pieces):
        return jnp.transpose(jnp.concatenate(pieces, axis=0), (1, 0))

    nothing = jnp.zeros((64, TOK), F32)
    expanded = jnp.dot(lat[...], ew[...], preferred_element_type=F32)
    key_rows = upright(turned(key_t[0:32, :], key_t[32:64, :]) + [nothing])
    low_lane = lax.broadcasted_iota(jnp.int32, (TOK, 128), 1) < 64
    swapped = pltpu.roll(expanded[:, 256:384], 64, 1)
    kvb[0, 0, :, 0:128] = expanded[:, 0:128].astype(BF)
    kvb[0, 0, :, 128:256] = jnp.where(low_lane, key_rows, swapped).astype(BF)
    kvb[0, 0, :, 256:384] = expanded[:, 128:256].astype(BF)
    kvb[0, 0, :, 384:512] = jnp.where(low_lane, swapped, 1.0).astype(BF)
    qb[3, :, 0:128] = upright([q_t[0:128, :].astype(F32)]).astype(BF)
    qb[3, :, 128:256] = upright(turned(q_t[192:224, :], q_t[224:256, :]) + [nothing]).astype(BF)
    qb[3, :, 256:384] = upright(
        turned(q_t[256:288, :], q_t[288:320, :]) + [q_t[128:192, :].astype(F32)]
    ).astype(BF)

    macc[...] = jnp.full((2, 512, 128), -3e38, F32)
    pl.semaphore_wait(barrier, len(greeted))

    def rows_of(slot, h):
        return kvb.at[slot, 0, pl.ds(32 * h, 32)]

    def slot_of(s, ahead):
        return 0 if s == 0 else 7 if s == 4 else 2 * s - 1 + ahead

    def kv_out(s, h):
        if s < 3 or h < 2:
            send(rows_of(slot_of(s, 0), h), rows_of(slot_of(s + 1, 0), h), kvz_s, kvz_r.at[0, s, h], right_z)
        if s < 3 or h >= 2:
            send(rows_of(slot_of(s, 1), h), rows_of(slot_of(s + 1, 1), h), kvz_s, kvz_r.at[1, s, h], left_z)

    def kv_across(slot):
        send(kvb.at[slot, 0], kvb.at[slot, 1], pk_s, pk_r.at[slot], partner)

    def kvz(s, h):
        if s < 4:
            wait_recv(rows_of(slot_of(s, 0), h), kvz_r.at[0, s - 1, h])
            wait_recv(rows_of(slot_of(s, 1), h), kvz_r.at[1, s - 1, h])
            kv_out(s, h)
            if h == 3:
                kv_across(2 * s - 1)
                kv_across(2 * s)
        else:
            for q in range(4):
                wait_recv(rows_of(7, q), kvz_r.at[q // 2, 3, q])
            kv_across(7)

    def q_relay(s):
        if s == 1:
            wait_recv(qb.at[1], q_r.at[0, 0])
            send(qb.at[1, pl.ds(0, 64)], qb.at[0, pl.ds(0, 64)], q_s, q_r.at[0, 1], right_y)
            wait_recv(qb.at[2], q_r.at[1, 0])
            send(qb.at[2, pl.ds(64, 64)], qb.at[0, pl.ds(64, 64)], q_s, q_r.at[1, 1], left_y)
        else:
            wait_recv(qb.at[0, pl.ds(0, 64)], q_r.at[0, 1])
            wait_recv(qb.at[0, pl.ds(64, 64)], q_r.at[1, 1])

    for q in range(4):
        kv_out(0, q)
    send(qb.at[3], qb.at[1], q_s, q_r.at[0, 0], right_y)
    send(qb.at[3], qb.at[2], q_s, q_r.at[1, 0], left_y)
    kv_across(0)

    for copy in weight_loads:
        copy.wait()

    offsets = [0, -1, 1, -2, 2, -3, 3, 4]

    def z_then_y(buf, z_s, z_r, y_s, y_r, p_s, p_r):
        def half(zz, yy, h):
            return buf.at[zz, yy, c, :, pl.ds(384 * h, 384)]

        def out(zz, j):
            block = buf.at[zz, y, c]
            send(block, block, y_s, y_r.at[0, 0, j], right_y)
            send(block, block, y_s, y_r.at[1, 0, j], left_y)
            send(block, block, p_s, p_r.at[j], partner)

        def on_z(s):
            lo, hi = zat(-s), zat(s)
            if s == 4:
                wait_recv(half(lo, y, 0), z_r.at[0, 3])
                wait_recv(half(lo, y, 1), z_r.at[1, 3])
                out(lo, 7)
                return
            for way, (zz, dev) in enumerate(((lo, right_z), (hi, left_z))):
                block = buf.at[zz, y, c]
                if s > 0:
                    wait_recv(block, z_r.at[way, s - 1])
                src = block if s < 3 else half(zz, y, way)
                send(src, src, z_s, z_r.at[way, s], dev)
            if s > 0:
                out(lo, 2 * s - 1)
                out(hi, 2 * s)

        def on_y(s, j):
            zz = zat(offsets[j])
            a, b, far = yat(-1), yat(1), yat(2)
            if s == 0:
                out(z, 0)
            elif s == 1:
                for way, (yy, dev) in enumerate(((a, right_y), (b, left_y))):
                    wait_recv(buf.at[zz, yy, c], y_r.at[way, 0, j])
                    src = half(zz, yy, way)
                    send(src, src, y_s, y_r.at[way, 1, j], dev)
                for yy in (a, b):
                    send(buf.at[zz, yy, c], buf.at[zz, yy, c], p_s, p_r.at[j], partner)
            else:
                wait_recv(half(zz, far, 0), y_r.at[0, 1, j])
                wait_recv(half(zz, far, 1), y_r.at[1, 1, j])
                send(buf.at[zz, far, c], buf.at[zz, far, c], p_s, p_r.at[j], partner)

        return on_z, on_y

    def y_then_z(buf, z_s, z_r, y_s, y_r, p_s, p_r):
        def half(zz, yy, h):
            return buf.at[zz, yy, c, :, pl.ds(384 * h, 384)]

        def on_y(s):
            a, b, far = yat(-1), yat(1), yat(2)
            if s == 2:
                wait_recv(half(z, far, 0), y_r.at[0, 1])
                wait_recv(half(z, far, 1), y_r.at[1, 1])
                return
            for way, (yy, dev) in enumerate(((a, right_y), (b, left_y))):
                if s == 0:
                    src = buf.at[z, y, c]
                else:
                    wait_recv(buf.at[z, yy, c], y_r.at[way, 0])
                    src = half(z, yy, way)
                send(src, src, y_s, y_r.at[way, s], dev)

        def on_z(s, r):
            yy = yat((0, -1, 1, 2)[r])
            lo, hi = zat(-s), zat(s)
            if s == 4:
                wait_recv(half(lo, yy, 0), z_r.at[0, 3, r])
                wait_recv(half(lo, yy, 1), z_r.at[1, 3, r])
            else:
                for way, (zz, dev) in enumerate(((lo, right_z), (hi, left_z))):
                    block = buf.at[zz, yy, c]
                    if s > 0:
                        wait_recv(block, z_r.at[way, s - 1, r])
                    src = block if s < 3 else half(zz, yy, way)
                    send(src, src, z_s, z_r.at[way, s, r], dev)
            for ahead, zz in enumerate((lo, hi) if 0 < s < 4 else (lo,)):
                send(buf.at[zz, yy, c], buf.at[zz, yy, c], p_s, p_r.at[slot_of(s, ahead)], partner)

        return on_y, on_z

    gb_z, gb_y = z_then_y(gb, *ring_sems[0:6])
    db_z, db_y = z_then_y(db, *ring_sems[6:12])
    va_y, va_z = y_then_z(va, *ring_sems[12:18])
    da_y, da_z = y_then_z(da, *ring_sems[18:24])

    heads = (
        (0, 256, 0, 256, 256, 512, (NOPE_A + ROPE) ** (-0.5) * LOG2E, accw),
        (256, 384, 128, 256, 384, 512, (NOPE_B + ROPE) ** (-0.5) * LOG2E, accn),
    )

    def scores(j):
        wait_recv(kvb.at[j, 1], pk_r.at[j])
        for head in range(2):
            q0, q1, k0, k1 = heads[head][:4]
            qs = qb[:, :, q0:q1].reshape(512, q1 - q0)
            ks = kvb[j, :, :, k0:k1].reshape(256, k1 - k0)
            s = lax.dot_general(qs, ks, (((1,), (1,)), ((), ())), preferred_element_type=F32)
            s_ref[head, j] = s
            macc[head] = jnp.maximum(macc[head], jnp.maximum(s[:, :128], s[:, 128:]))

    def weights(half, head, j0, j1):
        rows = slice(256 * half, 256 * half + 256)
        v0, v1, factor, acc = heads[head][4:]
        m = jnp.broadcast_to(jnp.max(macc[head, rows], axis=1, keepdims=True), (256, 128))
        for j in range(j0, j1):
            for side in range(2):
                s = s_ref[head, j, rows, side * 128 : side * 128 + 128]
                at = j * 256 + side * 128
                p_ref[head, :, at : at + 128] = jnp.exp2((s - m) * factor).astype(BF)
        vs = kvb[j0:j1, :, :, v0:v1].reshape(256 * (j1 - j0), v1 - v0)
        return m, jnp.dot(p_ref[head, :, j0 * 256 : j1 * 256], vs, preferred_element_type=F32)

    def weigh_early(half):
        rows = slice(256 * half, 256 * half + 256)
        for head in range(2):
            m, product = weights(half, head, 0, 5)
            mrow[head, rows] = m
            heads[head][7][rows] = product

    def weigh(half):
        rows = slice(256 * half, 256 * half + 256)
        for head in range(2):
            m, product = weights(half, head, 5, 8)
            factor, acc = heads[head][6:]
            shrink = jnp.exp2((mrow[head, rows] - m) * factor)
            shrink = jnp.concatenate([shrink] * (acc.shape[1] // 128), axis=1)
            mrow[head, rows] = m
            acc[rows] = acc[rows] * shrink + product

    lane = lax.broadcasted_iota(jnp.int32, (TOK, 128), 1)

    def pack(half):
        for b in (2 * half, 2 * half + 1):
            rows = slice(b * TOK, b * TOK + TOK)
            wide, narrow = accw[rows, :], accn[rows, :]
            tile = narrow
            stats = (
                mrow[0, rows, :], mrow[1, rows, :],
                jnp.broadcast_to(wide[:, 192:193], (TOK, 128)), jnp.broadcast_to(narrow[:, 64:65], (TOK, 128)),
            )
            at = 64
            for stat in stats:
                for piece in split3(stat):
                    tile = jnp.where(lane == at, piece, tile)
                    at += 1
            tile = jnp.where(lane >= at, 0.0, tile)
            part[b, :, 0:128] = wide[:, 0:128].astype(BF)
            part[b, :, 128:256] = tile.astype(BF)
        if half == 0:
            send(part.at[0], ob.at[0], o_s, o_r.at[0], {"sp_1": yat(2)})
            send(part.at[1], ob.at[2], o_s, o_r.at[2], left_y)
        else:
            send(part.at[2], ob.at[1], o_s, o_r.at[1], right_y)

    def merge():
        blocks = [part.at[3]] + [ob.at[g] for g in range(3)]
        tiles = [block[:, 128:256].astype(F32) for block in blocks]
        stats = [s + pltpu.roll(s, 127, 1) + pltpu.roll(s, 126, 1) for s in tiles]
        top = jnp.maximum(jnp.maximum(stats[0], stats[1]), jnp.maximum(stats[2], stats[3]))
        factor = jnp.where(lane == 64, heads[0][6], heads[1][6])
        shares = [jnp.exp2((s - top) * factor) for s in stats]
        total = sum(pltpu.roll(w, 6, 1) * s for w, s in zip(shares, stats))
        inverse = pltpu.roll(1.0 / total, 122, 1)
        shares = [w * inverse for w in shares]
        wide = sum(w[:, 64:65] * block[:, 0:128].astype(F32) for w, block in zip(shares, blocks))
        narrow = sum(w[:, 67:68] * s for w, s in zip(shares, tiles))
        att[x, 0:TOK, 0:128] = wide.astype(BF)
        att[x, 0:TOK, 128:256] = narrow.astype(BF)

    def part_in():
        for o in range(3):
            wait_recv(ob.at[o], o_r.at[o])

    def att_out():
        for o in (2, 1, 3):
            mine = att.at[x, pl.ds(0, TOK)]
            send(mine, mine, x_s, x_r.at[o - 1], {"tp": xat(o)})
        for o in range(NX):
            peer = {"tp": xat(o)}
            send(att.at[x, pl.ds(112, 16)], att.at[x, pl.ds(128, 16)], e_s, e_r.at[0, o], device_of(after) | peer)
            send(att.at[x, pl.ds(0, 16)], att.at[x, pl.ds(144, 16)], e_s, e_r.at[1, o], device_of(before) | peer)

    def edges_out():
        load_res.wait()
        send(resid.at[pl.ds(112, 16)], resid.at[pl.ds(128, 16)], h_s, h_r.at[0], device_of(after))
        send(resid.at[pl.ds(0, 16)], resid.at[pl.ds(144, 16)], h_s, h_r.at[1], device_of(before))

    edges_out()
    gb_z(0)
    gb_y(0, 0)
    va_y(0)
    kvz(1, 0)
    q_relay(1)
    kvz(1, 1)
    db_y(0, 0)
    kvz(1, 2)
    kvz(1, 3)
    da_y(0)
    gb_y(1, 0)
    va_y(1)
    gb_z(1)
    kvz(2, 0)
    q_relay(2)
    scores(0)
    scores(1)
    kvz(2, 1)
    db_y(1, 0)
    scores(2)
    kvz(2, 2)
    gb_y(2, 0)
    kvz(2, 3)
    va_y(2)
    gb_z(2)
    scores(3)
    scores(4)
    kvz(3, 0)
    va_z(0, 2)
    weigh_early(0)
    kvz(3, 1)
    db_y(2, 0)
    gb_y(1, 2)
    kvz(3, 2)
    weigh_early(1)
    kvz(3, 3)
    va_z(0, 3)
    va_z(0, 0)
    da_y(1)
    db_z(0)
    da_z(0, 2)
    va_z(0, 1)
    da_z(0, 0)
    gb_z(3)
    scores(5)
    gb_y(1, 4)
    scores(6)
    va_z(1, 2)
    gb_y(2, 2)
    da_y(2)
    da_z(0, 3)
    kvz(4, 0)
    va_z(1, 3)
    va_z(1, 0)
    db_z(1)
    scores(7)
    weigh(0)
    va_z(1, 1)
    pack(0)
    weigh(1)
    pack(1)
    da_z(1, 0)
    gb_y(2, 4)
    gb_z(4)
    gb_y(1, 3)
    da_z(0, 1)
    gb_y(1, 6)
    gb_y(1, 5)
    db_y(1, 1)
    va_z(2, 2)
    db_y(1, 2)
    va_z(2, 3)
    va_z(2, 0)
    db_z(2)
    va_z(2, 1)
    da_z(2, 0)
    part_in()
    merge()
    att_out()
    da_z(1, 1)
    gb_y(1, 1)
    da_z(1, 3)
    da_z(1, 2)
    va_z(3, 2)
    va_z(3, 3)
    gb_y(1, 7)
    va_z(3, 0)
    gb_y(2, 3)
    db_z(3)
    va_z(3, 1)
    gb_y(2, 6)
    da_z(3, 0)
    gb_y(2, 5)
    da_z(2, 1)
    db_y(2, 1)
    db_y(2, 2)
    da_z(2, 3)
    db_y(1, 3)
    da_z(2, 2)
    load_ow.wait()
    load_gain.wait()
    load_conv.wait()
    wait_recv(resid.at[pl.ds(128, 16)], h_r.at[0])
    wait_recv(resid.at[pl.ds(144, 16)], h_r.at[1])
    for o in (2, 1, 3):
        wait_recv(att.at[xat(-o), pl.ds(0, TOK)], x_r.at[o - 1])
    for o in range(NX):
        wait_recv(att.at[xat(-o), pl.ds(128, 16)], e_r.at[0, o])
        wait_recv(att.at[xat(-o), pl.ds(144, 16)], e_r.at[1, o])

    ss = jnp.zeros((ROWS, 1), F32)
    for n in range(8):
        cols = slice(n * 256, n * 256 + 256)
        total = resid[:, cols].astype(F32)
        for h in range(NX):
            total = total + jnp.dot(att[h, :, 0:192], ow[h * 192 : h * 192 + 192, cols], preferred_element_type=F32)
        rounded = total.astype(BF)
        stream[:, cols] = rounded
        wide = rounded.astype(F32)
        ss = ss + jnp.sum(wide * wide, axis=1, keepdims=True)
    scale = lax.rsqrt(ss * (1.0 / D) + 1e-06)
    for n in range(8):
        cols = slice(n * 256, n * 256 + 256)
        scaled = stream[:, cols].astype(F32) * scale
        normed[n] = (scaled * gain[cols].astype(F32).reshape(1, 256)).astype(BF)
    db_y(1, 4)
    db_z(4)
    va_z(4, 2)
    va_z(4, 0)
    va_z(4, 3)
    va_z(4, 1)
    gb_y(2, 1)
    gb_y(2, 7)

    def gate_rows(zz, cols):
        return gb[zz, :, :, 0:32, cols].reshape(256, 256)

    def value_rows(zz, cols):
        return jnp.concatenate([gb[zz, :, :, 32:48, cols], va[zz, :, :, :, cols]], axis=2).reshape(256, 256)

    def up(weights, rows, js, n):
        total = None
        for j in js:
            zz = zat(offsets[j])
            w = weights(zz, slice(n * 256, n * 256 + 256))
            term = jnp.dot(normed[zz, 0:rows], w, preferred_element_type=F32)
            total = term if total is None else total + term
        return total

    def arrived(buf, sems, j):
        wait_recv(buf.at[zat(offsets[j]), :, other], sems.at[j])

    for j in range(7):
        arrived(gb, ring_sems[5], j)
    for n in range(3):
        gacc[:, n * 256 : n * 256 + 256] = up(gate_rows, ROWS, range(7), n)
    da_z(3, 1)
    db_y(1, 5)
    for j in range(7):
        arrived(va, ring_sems[17], j)
    for n in range(3):
        vacc[:, n * 256 : n * 256 + 256] = up(value_rows, TOK, range(7), n)
    da_z(3, 3)
    db_y(1, 6)
    da_z(3, 2)
    arrived(gb, ring_sems[5], 7)
    arrived(va, ring_sems[17], 7)
    for n in range(3):
        cols = slice(n * 256, n * 256 + 256)
        gate[:, cols] = (gacc[:, cols] + up(gate_rows, ROWS, (7,), n)).astype(BF)
        value[:, cols] = (vacc[:, cols] + up(value_rows, TOK, (7,), n)).astype(BF)

    row = lax.broadcasted_iota(jnp.int32, (TOK, 256), 0)
    for n in range(3):
        cols = slice(n * 256, n * 256 + 256)
        g = gate[0:TOK, cols].astype(F32)
        edge = gate[TOK:ROWS, cols].astype(F32)
        first = jnp.where(place > 0, edge[15:16], 0.0)
        last = jnp.where(place < 63, edge[16:17], 0.0)
        low = jnp.where(row == 0, first, pltpu.roll(g, 1, 0))
        high = jnp.where(row == TOK - 1, last, pltpu.roll(g, TOK - 1, 0))
        cw = conv_w[:, cols].astype(F32)
        mixed = low * cw[0:1] + g * cw[1:2] + high * cw[2:3]
        silu = mixed / (1.0 + jnp.exp(-mixed))
        act[:, cols] = (silu * value[:, cols].astype(F32)).astype(BF)

    for j in range(NZ):
        zz = zat(offsets[j])
        arrived(da, ring_sems[23], j)
        arrived(db, ring_sems[11], j)
        w = jnp.concatenate([da[zz], db[zz]], axis=2).reshape(256, FFD)
        d = lax.dot_general(act[...], w, (((1,), (1,)), ((), ())), preferred_element_type=F32)
        fp[j] = d.astype(BF).reshape(NX, 32, 256)
        for o in (2, 1, 3):
            peer = xat(o)
            send(fp.at[j, peer], fr.at[j, x], f_s, f_r.at[j, o - 1], {"tp": peer})
        if j == 0:
            db_y(1, 7)
            db_y(2, 3)
        if j == 1:
            da_z(4, 0)
            db_y(2, 4)
        if j == 2:
            db_y(2, 5)
            da_z(4, 1)
        if j == 3:
            db_y(2, 6)
            da_z(4, 3)
        if j == 4:
            da_z(4, 2)
        if j == 6:
            db_y(2, 7)

    rows = pl.ds(pl.multiple_of(x * 32, 32), 32)
    for j in range(NZ):
        cols = pl.ds(pl.multiple_of(zat(offsets[j]) * 256, 256), 256)
        total = stream[rows, cols].astype(F32) + fp[j, x].astype(F32)
        for o in (1, 3, 2):
            wait_recv(fr.at[j, xat(-o)], f_r.at[j, o - 1])
            total = total + fr[j, xat(-o)].astype(F32)
        out_ref[:, cols] = total.astype(BF)

    wait_send(kvb.at[pl.ds(0, 7), 0], kvz_s)
    wait_send(qb.at[pl.ds(0, 3)], q_s)
    wait_send(kvb.at[:, 0], pk_s)
    for buf, (z_s, _, y_s, _, p_s, _) in ((gb, ring_sems[0:6]), (db, ring_sems[6:12])):
        wait_send(buf.at[pl.ds(0, 7), 0, 0], z_s)
        wait_send(buf.at[:, pl.ds(0, 3), 0], y_s)
        wait_send(buf.at[:, :, 0], p_s)
    for buf, (z_s, _, y_s, _, p_s, _) in ((va, ring_sems[12:18]), (da, ring_sems[18:24])):
        wait_send(buf.at[pl.ds(0, 7), :, 0], z_s)
        wait_send(buf.at[0, pl.ds(0, 3), 0], y_s)
        wait_send(buf.at[:, :, 0], p_s)
    wait_send(part.at[pl.ds(0, 3)], o_s)
    wait_send(att.at[pl.ds(0, 3), pl.ds(0, TOK)], x_s)
    wait_send(att.at[:, pl.ds(0, 32)], e_s)
    wait_send(resid.at[pl.ds(0, 32)], h_s)
    wait_send(fp.at[:, pl.ds(0, 3)], f_s)


def layer(*operands):
    vmem = pl.BlockSpec(memory_space=pltpu.VMEM)
    hbm = pl.BlockSpec(memory_space=pltpu.HBM)
    dma = pltpu.SemaphoreType.DMA
    scratch = [
        pltpu.VMEM((D,), BF),
        pltpu.VMEM((3, FFD), BF),
        pltpu.VMEM((320, TOK), BF),
        pltpu.VMEM((TOK, 512), BF),
        pltpu.VMEM((64, TOK), BF),
        pltpu.VMEM((512, 384), BF),
        pltpu.VMEM((32, TOK), F32),
        pltpu.VMEM((NZ, 2, TOK, 512), BF),
        pltpu.VMEM((NY, TOK, 384), BF),
        pltpu.VMEM((NZ, NY, 2, 48, FFD), BF),
        pltpu.VMEM((NZ, NY, 2, 16, FFD), BF),
        pltpu.VMEM((NZ, NY, 2, 16, FFD), BF),
        pltpu.VMEM((NZ, NY, 2, 16, FFD), BF),
        pltpu.VMEM((768, D), BF),
        pltpu.VMEM((ROWS, D), BF),
        pltpu.VMEM((2, NZ, 512, 256), F32),
        pltpu.VMEM((2, 256, 2048), BF),
        pltpu.VMEM((2, 512, 128), F32),
        pltpu.VMEM((2, 512, 128), F32),
        pltpu.VMEM((512, 256), F32),
        pltpu.VMEM((512, 128), F32),
        pltpu.VMEM((NY, TOK, 256), BF),
        pltpu.VMEM((NY, TOK, 256), BF),
        pltpu.VMEM((NX, ROWS, 256), BF),
        pltpu.VMEM((ROWS, D), BF),
        pltpu.VMEM((NZ, ROWS, 256), BF),
        pltpu.VMEM((ROWS, FFD), F32),
        pltpu.VMEM((TOK, FFD), F32),
        pltpu.VMEM((ROWS, FFD), BF),
        pltpu.VMEM((TOK, FFD), BF),
        pltpu.VMEM((TOK, FFD), BF),
        pltpu.VMEM((NZ, NX, 32, 256), BF),
        pltpu.VMEM((NZ, NX, 32, 256), BF),
        dma, dma((2, 4, 4)), dma, dma((2, 2)), dma, dma((8,)), dma, dma((3,)), dma, dma((3,)),
        dma, dma((2, 4)), dma, dma((2,)), dma, dma((NZ, 3)), dma((14,)),
    ]
    scratch += 2 * [dma, dma((2, 4)), dma, dma((2, 2, 8)), dma, dma((8,))]
    scratch += 2 * [dma, dma((2, 4, 4)), dma, dma((2, 2)), dma, dma((8,))]
    return pl.pallas_call(
        kernel,
        out_shape=pltpu.VMEM((32, D), BF),
        in_specs=[hbm] * 12,
        out_specs=vmem,
        scratch_shapes=scratch,
        compiler_params=pltpu.CompilerParams(collective_id=0, has_side_effects=True),
    )(*operands)


def body(
    queries, latents, shared_key, expand_weight, residual, out_weight,
    norm_gain, gate_weight, value_weight, conv_weight, down_weight,
):
    frequency = (10000.0 ** (-np.arange(ROPE // 2) / (ROPE // 2))).astype(np.float32)
    return layer(
        norm_gain, conv_weight, queries.T, latents, shared_key.T, expand_weight, gate_weight, value_weight,
        down_weight.T, np.ascontiguousarray(np.broadcast_to(frequency[:, None], (ROPE // 2, TOK))),
        residual, out_weight,
    )


def solution(mesh):
    split = Mesh(mesh.devices.reshape(NZ, NY, 2, mesh.shape["tp"]), ("sp_0", "sp_1", "sp_2", "tp"))
    placed = (
        P(SP, "tp"),
        P(SP, None),
        P(SP, None),
        P(None, "tp"),
        P(SP, None),
        P(),
        P(),
        P(SP, "tp"),
        P(SP, "tp"),
        P(None, "tp"),
        P("tp", SP),
    )
    return jax.shard_map(
        body, mesh=split, in_specs=placed, out_specs=P(SP_TP, None), check_vma=False
    )
```

```python
import functools

import jax
import jax.numpy as jnp
import numpy as np
from jax import lax
from jax.experimental import pallas as pl
from jax.experimental.pallas import tpu as pltpu
from jax.sharding import Mesh
from jax.sharding import PartitionSpec as P

NOPE_A = 128
VAL_A = 128
NOPE_B = 64
VAL_B = 64
ROPE = 64
SP = ("sp_0", "sp_1", "sp_2")
SP_TP = ("sp_0", "sp_1", "sp_2", "tp")
NZ, NY, NX = 8, 4, 4
TOK = 128
ROWS = TOK + 32
D = 2048
FFD = 768
MESH = pl.DeviceIdType.MESH
LOG2E = 1.4426950408889634
F32 = jnp.float32
BF = jnp.bfloat16


def split3(v):
    hi = v.astype(BF).astype(F32)
    rest = v - hi
    mid = rest.astype(BF).astype(F32)
    return hi, mid, rest - mid


def kernel(
    gain_hbm, conv_hbm, q_hbm, lat_hbm, key_hbm, ew_hbm, gate_hbm, value_hbm, dn_hbm, freq_hbm, resid_hbm, ow_hbm,
    out_ref,
    gain, conv_w, q_t, lat, key_t, ew, freq, kvb, qb, gb, va, da, db, ow, resid, s_ref, p_ref, macc, mrow, accw, accn,
    part, ob, att, attp, stream, normed, gacc, vacc, gate, value, act, fp, fr,
    kvz_s, kvz_r, q_s, q_r, pk_s, pk_r, o_s, o_r, x_s, x_r, e_s, e_r, h_s, h_r, f_s, f_r, loc, *ring_sems,
):
    z = lax.axis_index("sp_0")
    y = lax.axis_index("sp_1")
    c = lax.axis_index("sp_2")
    x = lax.axis_index("tp")
    other = 1 - c

    def zat(k):
        return lax.rem(z + (k + NZ), NZ)

    def yat(k):
        return lax.rem(y + (k + NY), NY)

    def xat(k):
        return lax.rem(x + (k + NX), NX)

    right_z, left_z = {"sp_0": zat(1)}, {"sp_0": zat(-1)}
    right_y, left_y = {"sp_1": yat(1)}, {"sp_1": yat(-1)}
    partner = {"sp_2": other}
    place = (z * NY + y) * 2 + c
    after = lax.rem(place + 1, 64)
    before = lax.rem(place + 63, 64)

    def device_of(i):
        return {"sp_0": i // 8, "sp_1": lax.rem(i // 2, 4), "sp_2": lax.rem(i, 2)}

    def send(src, dst, ssem, rsem, dev):
        pltpu.make_async_remote_copy(
            src_ref=src, dst_ref=dst, send_sem=ssem, recv_sem=rsem, device_id=dev, device_id_type=MESH
        ).start()

    def wait_recv(ref, sem):
        pltpu.make_async_remote_copy(
            src_ref=ref, dst_ref=ref, send_sem=sem, recv_sem=sem, device_id=partner, device_id_type=MESH
        ).wait_recv()

    def wait_send(ref, sem):
        pltpu.make_async_remote_copy(
            src_ref=ref, dst_ref=ref, send_sem=sem, recv_sem=sem, device_id=partner, device_id_type=MESH
        ).wait_send()

    barrier = pltpu.get_barrier_semaphore()
    greeted = [
        partner, right_z, left_z, right_y, left_y, {"sp_1": yat(2)},
        {"tp": xat(1)}, {"tp": xat(2)}, {"tp": xat(3)},
    ]
    greeted += [device_of(i) | {"tp": xat(o)} for i in (after, before) for o in range(NX)]
    for dev in greeted:
        pl.semaphore_signal(barrier, inc=1, device_id=dev, device_id_type=MESH)

    def load(src, dst, i):
        copy = pltpu.make_async_copy(src, dst, loc.at[i])
        copy.start()
        return copy

    first_loads = [
        load(lat_hbm, lat, 0), load(ew_hbm, ew, 1), load(key_hbm, key_t, 2), load(freq_hbm, freq, 3),
        load(q_hbm, q_t, 4),
    ]
    weight_loads = [
        load(gate_hbm, gb.at[z, y, c, pl.ds(0, 32)], 5),
        load(value_hbm.at[pl.ds(0, 16)], gb.at[z, y, c, pl.ds(32, 16)], 6),
        load(value_hbm.at[pl.ds(16, 16)], va.at[z, y, c], 7),
        load(dn_hbm.at[pl.ds(0, 16)], da.at[z, y, c], 12), load(dn_hbm.at[pl.ds(16, 16)], db.at[z, y, c], 13),
    ]
    load_res = load(resid_hbm, resid.at[pl.ds(0, TOK)], 8)
    load_ow = load(ow_hbm, ow, 9)
    load_gain = load(gain_hbm, gain, 10)
    load_conv = load(conv_hbm, conv_w, 11)
    for copy in first_loads:
        copy.wait()

    position = (lax.broadcasted_iota(jnp.int32, (32, TOK), 1) + place * TOK).astype(F32)
    angles = position * freq[...]
    cosine, sine = jnp.cos(angles), jnp.sin(angles)

    def turned(a, b):
        a, b = a.astype(F32), b.astype(F32)
        return [a * cosine - b * sine, b * cosine + a * sine]

    def upright(pieces):
        return jnp.transpose(jnp.concatenate(pieces, axis=0), (1, 0))

    nothing = jnp.zeros((64, TOK), F32)
    expanded = jnp.dot(lat[...], ew[...], preferred_element_type=F32)
    key_rows = upright(turned(key_t[0:32, :], key_t[32:64, :]) + [nothing])
    low_lane = lax.broadcasted_iota(jnp.int32, (TOK, 128), 1) < 64
    swapped = pltpu.roll(expanded[:, 256:384], 64, 1)
    kvb[0, 0, :, 0:128] = expanded[:, 0:128].astype(BF)
    kvb[0, 0, :, 128:256] = jnp.where(low_lane, key_rows, swapped).astype(BF)
    kvb[0, 0, :, 256:384] = expanded[:, 128:256].astype(BF)
    kvb[0, 0, :, 384:512] = jnp.where(low_lane, swapped, 1.0).astype(BF)
    qb[3, :, 0:128] = upright([q_t[0:128, :].astype(F32)]).astype(BF)
    qb[3, :, 128:256] = upright(turned(q_t[192:224, :], q_t[224:256, :]) + [nothing]).astype(BF)
    qb[3, :, 256:384] = upright(
        turned(q_t[256:288, :], q_t[288:320, :]) + [q_t[128:192, :].astype(F32)]
    ).astype(BF)

    macc[...] = jnp.full((2, 512, 128), -3e38, F32)
    pl.semaphore_wait(barrier, len(greeted))

    def rows_of(slot, h):
        return kvb.at[slot, 0, pl.ds(32 * h, 32)]

    def slot_of(s, ahead):
        return 0 if s == 0 else 7 if s == 4 else 2 * s - 1 + ahead

    def kv_out(s, h):
        if s < 3 or h < 2:
            send(rows_of(slot_of(s, 0), h), rows_of(slot_of(s + 1, 0), h), kvz_s, kvz_r.at[0, s, h], right_z)
        if s < 3 or h >= 2:
            send(rows_of(slot_of(s, 1), h), rows_of(slot_of(s + 1, 1), h), kvz_s, kvz_r.at[1, s, h], left_z)

    def kv_across(slot):
        send(kvb.at[slot, 0], kvb.at[slot, 1], pk_s, pk_r.at[slot], partner)

    def kvz(s, h):
        if s < 4:
            wait_recv(rows_of(slot_of(s, 0), h), kvz_r.at[0, s - 1, h])
            wait_recv(rows_of(slot_of(s, 1), h), kvz_r.at[1, s - 1, h])
            kv_out(s, h)
            if h == 3:
                kv_across(2 * s - 1)
                kv_across(2 * s)
        else:
            for q in range(4):
                wait_recv(rows_of(7, q), kvz_r.at[q // 2, 3, q])
            kv_across(7)

    def q_relay(s):
        if s == 1:
            wait_recv(qb.at[1], q_r.at[0, 0])
            send(qb.at[1, pl.ds(0, 64)], qb.at[0, pl.ds(0, 64)], q_s, q_r.at[0, 1], right_y)
            wait_recv(qb.at[2], q_r.at[1, 0])
            send(qb.at[2, pl.ds(64, 64)], qb.at[0, pl.ds(64, 64)], q_s, q_r.at[1, 1], left_y)
        else:
            wait_recv(qb.at[0, pl.ds(0, 64)], q_r.at[0, 1])
            wait_recv(qb.at[0, pl.ds(64, 64)], q_r.at[1, 1])

    for q in range(4):
        kv_out(0, q)
    send(qb.at[3], qb.at[1], q_s, q_r.at[0, 0], right_y)
    send(qb.at[3], qb.at[2], q_s, q_r.at[1, 0], left_y)
    kv_across(0)

    for copy in weight_loads:
        copy.wait()

    offsets = [0, -1, 1, -2, 2, -3, 3, 4]

    def z_then_y(buf, z_s, z_r, y_s, y_r, p_s, p_r):
        def half(zz, yy, h):
            return buf.at[zz, yy, c, :, pl.ds(384 * h, 384)]

        def out(zz, j):
            block = buf.at[zz, y, c]
            send(block, block, y_s, y_r.at[0, 0, j], right_y)
            send(block, block, y_s, y_r.at[1, 0, j], left_y)
            send(block, block, p_s, p_r.at[j], partner)

        def on_z(s):
            lo, hi = zat(-s), zat(s)
            if s == 4:
                wait_recv(half(lo, y, 0), z_r.at[0, 3])
                wait_recv(half(lo, y, 1), z_r.at[1, 3])
                out(lo, 7)
                return
            for way, (zz, dev) in enumerate(((lo, right_z), (hi, left_z))):
                block = buf.at[zz, y, c]
                if s > 0:
                    wait_recv(block, z_r.at[way, s - 1])
                src = block if s < 3 else half(zz, y, way)
                send(src, src, z_s, z_r.at[way, s], dev)
            if s > 0:
                out(lo, 2 * s - 1)
                out(hi, 2 * s)

        def on_y(s, j):
            zz = zat(offsets[j])
            a, b, far = yat(-1), yat(1), yat(2)
            if s == 0:
                out(z, 0)
            elif s == 1:
                for way, (yy, dev) in enumerate(((a, right_y), (b, left_y))):
                    wait_recv(buf.at[zz, yy, c], y_r.at[way, 0, j])
                    src = half(zz, yy, way)
                    send(src, src, y_s, y_r.at[way, 1, j], dev)
                for yy in (a, b):
                    send(buf.at[zz, yy, c], buf.at[zz, yy, c], p_s, p_r.at[j], partner)
            else:
                wait_recv(half(zz, far, 0), y_r.at[0, 1, j])
                wait_recv(half(zz, far, 1), y_r.at[1, 1, j])
                send(buf.at[zz, far, c], buf.at[zz, far, c], p_s, p_r.at[j], partner)

        return on_z, on_y

    def y_then_z(buf, z_s, z_r, y_s, y_r, p_s, p_r):
        def half(zz, yy, h):
            return buf.at[zz, yy, c, :, pl.ds(384 * h, 384)]

        def on_y(s):
            a, b, far = yat(-1), yat(1), yat(2)
            if s == 2:
                wait_recv(half(z, far, 0), y_r.at[0, 1])
                wait_recv(half(z, far, 1), y_r.at[1, 1])
                return
            for way, (yy, dev) in enumerate(((a, right_y), (b, left_y))):
                if s == 0:
                    src = buf.at[z, y, c]
                else:
                    wait_recv(buf.at[z, yy, c], y_r.at[way, 0])
                    src = half(z, yy, way)
                send(src, src, y_s, y_r.at[way, s], dev)

        def on_z(s, r):
            yy = yat((0, -1, 1, 2)[r])
            lo, hi = zat(-s), zat(s)
            if s == 4:
                wait_recv(half(lo, yy, 0), z_r.at[0, 3, r])
                wait_recv(half(lo, yy, 1), z_r.at[1, 3, r])
            else:
                for way, (zz, dev) in enumerate(((lo, right_z), (hi, left_z))):
                    block = buf.at[zz, yy, c]
                    if s > 0:
                        wait_recv(block, z_r.at[way, s - 1, r])
                    src = block if s < 3 else half(zz, yy, way)
                    send(src, src, z_s, z_r.at[way, s, r], dev)
            for ahead, zz in enumerate((lo, hi) if 0 < s < 4 else (lo,)):
                send(buf.at[zz, yy, c], buf.at[zz, yy, c], p_s, p_r.at[slot_of(s, ahead)], partner)

        return on_y, on_z

    gb_z, gb_y = z_then_y(gb, *ring_sems[0:6])
    db_z, db_y = z_then_y(db, *ring_sems[6:12])
    va_y, va_z = y_then_z(va, *ring_sems[12:18])
    da_y, da_z = y_then_z(da, *ring_sems[18:24])

    heads = (
        (0, 256, 0, 256, 256, 512, (NOPE_A + ROPE) ** (-0.5) * LOG2E, accw),
        (256, 384, 128, 256, 384, 512, (NOPE_B + ROPE) ** (-0.5) * LOG2E, accn),
    )

    def scores(j):
        wait_recv(kvb.at[j, 1], pk_r.at[j])
        for head in range(2):
            q0, q1, k0, k1 = heads[head][:4]
            qs = qb[:, :, q0:q1].reshape(512, q1 - q0)
            ks = kvb[j, :, :, k0:k1].reshape(256, k1 - k0)
            s = lax.dot_general(qs, ks, (((1,), (1,)), ((), ())), preferred_element_type=F32)
            s_ref[head, j] = s
            macc[head] = jnp.maximum(macc[head], jnp.maximum(s[:, :128], s[:, 128:]))

    def weights(half, head, j0, j1):
        rows = slice(256 * half, 256 * half + 256)
        v0, v1, factor, acc = heads[head][4:]
        m = jnp.broadcast_to(jnp.max(macc[head, rows], axis=1, keepdims=True), (256, 128))
        for j in range(j0, j1):
            for side in range(2):
                s = s_ref[head, j, rows, side * 128 : side * 128 + 128]
                at = j * 256 + side * 128
                p_ref[head, :, at : at + 128] = jnp.exp2((s - m) * factor).astype(BF)
        vs = kvb[j0:j1, :, :, v0:v1].reshape(256 * (j1 - j0), v1 - v0)
        return m, jnp.dot(p_ref[head, :, j0 * 256 : j1 * 256], vs, preferred_element_type=F32)

    def weigh_early(half):
        rows = slice(256 * half, 256 * half + 256)
        for head in range(2):
            m, product = weights(half, head, 0, 5)
            mrow[head, rows] = m
            heads[head][7][rows] = product

    def weigh(half):
        rows = slice(256 * half, 256 * half + 256)
        for head in range(2):
            m, product = weights(half, head, 5, 8)
            factor, acc = heads[head][6:]
            shrink = jnp.exp2((mrow[head, rows] - m) * factor)
            shrink = jnp.concatenate([shrink] * (acc.shape[1] // 128), axis=1)
            mrow[head, rows] = m
            acc[rows] = acc[rows] * shrink + product

    lane = lax.broadcasted_iota(jnp.int32, (TOK, 128), 1)

    def pack(half):
        for b in (2 * half, 2 * half + 1):
            rows = slice(b * TOK, b * TOK + TOK)
            wide, narrow = accw[rows, :], accn[rows, :]
            tile = narrow
            stats = (
                mrow[0, rows, :], mrow[1, rows, :],
                jnp.broadcast_to(wide[:, 192:193], (TOK, 128)), jnp.broadcast_to(narrow[:, 64:65], (TOK, 128)),
            )
            at = 64
            for stat in stats:
                for piece in split3(stat):
                    tile = jnp.where(lane == at, piece, tile)
                    at += 1
            tile = jnp.where(lane >= at, 0.0, tile)
            part[b, :, 0:128] = wide[:, 0:128].astype(BF)
            part[b, :, 128:256] = tile.astype(BF)
        if half == 0:
            send(part.at[0], ob.at[0], o_s, o_r.at[0], {"sp_1": yat(2)})
            send(part.at[1], ob.at[2], o_s, o_r.at[2], left_y)
        else:
            send(part.at[2], ob.at[1], o_s, o_r.at[1], right_y)

    def merge():
        blocks = [part.at[3]] + [ob.at[g] for g in range(3)]
        tiles = [block[:, 128:256].astype(F32) for block in blocks]
        stats = [s + pltpu.roll(s, 127, 1) + pltpu.roll(s, 126, 1) for s in tiles]
        top = jnp.maximum(jnp.maximum(stats[0], stats[1]), jnp.maximum(stats[2], stats[3]))
        factor = jnp.where(lane == 64, heads[0][6], heads[1][6])
        shares = [jnp.exp2((s - top) * factor) for s in stats]
        total = sum(pltpu.roll(w, 6, 1) * s for w, s in zip(shares, stats))
        inverse = pltpu.roll(1.0 / total, 122, 1)
        shares = [w * inverse for w in shares]
        wide = sum(w[:, 64:65] * block[:, 0:128].astype(F32) for w, block in zip(shares, blocks))
        narrow = sum(w[:, 67:68] * s for w, s in zip(shares, tiles))
        att[x, 0:TOK, 0:128] = wide.astype(BF)
        att[x, 0:TOK, 128:256] = narrow.astype(BF)
        attp[x, 0:TOK] = wide.astype(BF)
        attp[x, TOK:192] = jnp.where(lane[0:64] < 64, narrow[0:64], pltpu.roll(narrow[64:128], 64, 1)).astype(BF)

    def part_in():
        for o in range(3):
            wait_recv(ob.at[o], o_r.at[o])

    def att_out():
        for o in (2, 1, 3):
            send(attp.at[x], attp.at[x], x_s, x_r.at[o - 1], {"tp": xat(o)})
        for o in range(NX):
            peer = {"tp": xat(o)}
            send(att.at[x, pl.ds(112, 16)], att.at[x, pl.ds(128, 16)], e_s, e_r.at[0, o], device_of(after) | peer)
            send(att.at[x, pl.ds(0, 16)], att.at[x, pl.ds(144, 16)], e_s, e_r.at[1, o], device_of(before) | peer)

    def edges_out():
        load_res.wait()
        send(resid.at[pl.ds(112, 16)], resid.at[pl.ds(128, 16)], h_s, h_r.at[0], device_of(after))
        send(resid.at[pl.ds(0, 16)], resid.at[pl.ds(144, 16)], h_s, h_r.at[1], device_of(before))

    edges_out()
    gb_z(0)
    gb_y(0, 0)
    va_y(0)
    db_y(0, 0)
    kvz(1, 0)
    q_relay(1)
    kvz(1, 1)
    kvz(1, 2)
    kvz(1, 3)
    gb_y(1, 0)
    gb_z(1)
    db_y(1, 0)
    kvz(2, 0)
    q_relay(2)
    scores(0)
    kvz(2, 1)
    scores(1)
    kvz(2, 2)
    da_y(0)
    scores(2)
    kvz(2, 3)
    va_y(1)
    va_z(0, 1)
    gb_z(2)
    scores(3)
    scores(4)
    kvz(3, 0)
    weigh_early(0)
    kvz(3, 1)
    va_y(2)
    va_z(0, 3)
    weigh_early(1)
    kvz(3, 2)
    kvz(3, 3)
    va_z(0, 0)
    va_z(0, 2)
    db_z(0)
    db_y(2, 0)
    gb_y(1, 2)
    va_z(1, 1)
    da_y(1)
    da_z(0, 1)
    gb_y(1, 3)
    scores(5)
    gb_z(3)
    scores(6)
    gb_y(1, 4)
    gb_y(2, 2)
    va_z(1, 3)
    kvz(4, 0)
    va_z(1, 0)
    va_z(1, 2)
    db_z(1)
    scores(7)
    weigh(0)
    va_z(2, 1)
    da_y(2)
    da_z(0, 0)
    da_z(0, 2)
    da_z(0, 3)
    pack(0)
    weigh(1)
    pack(1)
    gb_z(4)
    gb_y(1, 1)
    gb_y(1, 5)
    gb_y(2, 4)
    gb_y(2, 3)
    va_z(2, 3)
    va_z(2, 0)
    db_y(1, 1)
    va_z(2, 2)
    db_y(1, 2)
    db_z(2)
    va_z(3, 1)
    da_z(1, 0)
    da_z(1, 2)
    da_z(1, 3)
    part_in()
    merge()
    att_out()
    da_z(1, 1)
    va_z(3, 3)
    gb_y(2, 0)
    va_z(3, 0)
    gb_y(1, 6)
    va_z(3, 2)
    gb_y(1, 7)
    db_z(3)
    va_z(4, 1)
    gb_y(2, 1)
    da_z(2, 0)
    da_z(2, 2)
    gb_y(2, 5)
    db_y(2, 1)
    da_z(2, 3)
    db_y(2, 2)
    da_z(2, 1)
    db_y(1, 3)
    va_z(4, 3)
    load_ow.wait()
    load_gain.wait()
    load_conv.wait()
    wait_recv(resid.at[pl.ds(128, 16)], h_r.at[0])
    wait_recv(resid.at[pl.ds(144, 16)], h_r.at[1])
    for o in (2, 1, 3):
        wait_recv(attp.at[xat(-o)], x_r.at[o - 1])
        packed = attp[xat(-o), TOK:192]
        att[xat(-o), 0:TOK, 0:128] = attp[xat(-o), 0:TOK]
        att[xat(-o), 0:64, 128:256] = packed
        att[xat(-o), 64:128, 128:256] = pltpu.roll(packed.astype(F32), 64, 1).astype(BF)
    for o in range(NX):
        wait_recv(att.at[xat(-o), pl.ds(128, 16)], e_r.at[0, o])
        wait_recv(att.at[xat(-o), pl.ds(144, 16)], e_r.at[1, o])

    ss = jnp.zeros((ROWS, 1), F32)
    for n in range(8):
        cols = slice(n * 256, n * 256 + 256)
        total = resid[:, cols].astype(F32)
        for h in range(NX):
            total = total + jnp.dot(att[h, :, 0:192], ow[h * 192 : h * 192 + 192, cols], preferred_element_type=F32)
        rounded = total.astype(BF)
        stream[:, cols] = rounded
        wide = rounded.astype(F32)
        ss = ss + jnp.sum(wide * wide, axis=1, keepdims=True)
    scale = lax.rsqrt(ss * (1.0 / D) + 1e-06)
    for n in range(8):
        cols = slice(n * 256, n * 256 + 256)
        scaled = stream[:, cols].astype(F32) * scale
        normed[n] = (scaled * gain[cols].astype(F32).reshape(1, 256)).astype(BF)
    db_z(4)
    db_y(1, 4)
    da_z(3, 0)
    va_z(4, 2)
    va_z(4, 0)
    gb_y(2, 6)
    gb_y(2, 7)

    def gate_rows(zz, cols):
        return gb[zz, :, :, 0:32, cols].reshape(256, 256)

    def value_rows(zz, cols):
        return jnp.concatenate([gb[zz, :, :, 32:48, cols], va[zz, :, :, :, cols]], axis=2).reshape(256, 256)

    def up(weights, rows, js, n):
        total = None
        for j in js:
            zz = zat(offsets[j])
            w = weights(zz, slice(n * 256, n * 256 + 256))
            term = jnp.dot(normed[zz, 0:rows], w, preferred_element_type=F32)
            total = term if total is None else total + term
        return total

    def arrived(buf, sems, j):
        wait_recv(buf.at[zat(offsets[j]), :, other], sems.at[j])

    for j in range(7):
        arrived(gb, ring_sems[5], j)
    gacc[:, 0:256] = up(gate_rows, ROWS, range(7), 0)
    da_z(3, 2)
    gacc[:, 256:512] = up(gate_rows, ROWS, range(7), 1)
    gacc[:, 512:768] = up(gate_rows, ROWS, range(7), 2)
    db_y(1, 5)
    da_z(3, 3)
    for j in range(7):
        arrived(va, ring_sems[17], j)
    vacc[:, 0:256] = up(value_rows, TOK, range(7), 0)
    vacc[:, 256:512] = up(value_rows, TOK, range(7), 1)
    db_y(1, 6)
    da_z(3, 1)
    vacc[:, 512:768] = up(value_rows, TOK, range(7), 2)
    arrived(gb, ring_sems[5], 7)
    arrived(va, ring_sems[17], 7)
    for n in range(3):
        cols = slice(n * 256, n * 256 + 256)
        gate[:, cols] = (gacc[:, cols] + up(gate_rows, ROWS, (7,), n)).astype(BF)
        value[:, cols] = (vacc[:, cols] + up(value_rows, TOK, (7,), n)).astype(BF)

    row = lax.broadcasted_iota(jnp.int32, (TOK, 256), 0)
    for n in range(3):
        cols = slice(n * 256, n * 256 + 256)
        g = gate[0:TOK, cols].astype(F32)
        edge = gate[TOK:ROWS, cols].astype(F32)
        first = jnp.where(place > 0, edge[15:16], 0.0)
        last = jnp.where(place < 63, edge[16:17], 0.0)
        low = jnp.where(row == 0, first, pltpu.roll(g, 1, 0))
        high = jnp.where(row == TOK - 1, last, pltpu.roll(g, TOK - 1, 0))
        cw = conv_w[:, cols].astype(F32)
        mixed = low * cw[0:1] + g * cw[1:2] + high * cw[2:3]
        silu = mixed / (1.0 + jnp.exp(-mixed))
        act[:, cols] = (silu * value[:, cols].astype(F32)).astype(BF)

    for j in range(NZ):
        zz = zat(offsets[j])
        arrived(da, ring_sems[23], j)
        arrived(db, ring_sems[11], j)
        w = jnp.concatenate([da[zz], db[zz]], axis=2).reshape(256, FFD)
        d = lax.dot_general(act[...], w, (((1,), (1,)), ((), ())), preferred_element_type=F32)
        fp[j] = d.astype(BF).reshape(NX, 32, 256)
        for o in (2, 1, 3):
            peer = xat(o)
            send(fp.at[j, peer], fr.at[j, x], f_s, f_r.at[j, o - 1], {"tp": peer})
        if j == 0:
            db_y(1, 7)
            db_y(2, 3)
        if j == 1:
            db_y(2, 4)
            da_z(4, 0)
        if j == 2:
            db_y(2, 5)
            da_z(4, 2)
        if j == 3:
            db_y(2, 6)
            da_z(4, 3)
        if j == 4:
            da_z(4, 1)
        if j == 6:
            db_y(2, 7)

    rows = pl.ds(pl.multiple_of(x * 32, 32), 32)
    for j in range(NZ):
        cols = pl.ds(pl.multiple_of(zat(offsets[j]) * 256, 256), 256)
        total = stream[rows, cols].astype(F32) + fp[j, x].astype(F32)
        for o in (1, 3, 2):
            wait_recv(fr.at[j, xat(-o)], f_r.at[j, o - 1])
            total = total + fr[j, xat(-o)].astype(F32)
        out_ref[:, cols] = total.astype(BF)

    wait_send(kvb.at[pl.ds(0, 7), 0], kvz_s)
    wait_send(qb.at[pl.ds(0, 3)], q_s)
    wait_send(kvb.at[:, 0], pk_s)
    for buf, (z_s, _, y_s, _, p_s, _) in ((gb, ring_sems[0:6]), (db, ring_sems[6:12])):
        wait_send(buf.at[pl.ds(0, 7), 0, 0], z_s)
        wait_send(buf.at[:, pl.ds(0, 3), 0], y_s)
        wait_send(buf.at[:, :, 0], p_s)
    for buf, (z_s, _, y_s, _, p_s, _) in ((va, ring_sems[12:18]), (da, ring_sems[18:24])):
        wait_send(buf.at[pl.ds(0, 7), :, 0], z_s)
        wait_send(buf.at[0, pl.ds(0, 3), 0], y_s)
        wait_send(buf.at[:, :, 0], p_s)
    wait_send(part.at[pl.ds(0, 3)], o_s)
    wait_send(attp.at[pl.ds(0, 3)], x_s)
    wait_send(att.at[:, pl.ds(0, 32)], e_s)
    wait_send(resid.at[pl.ds(0, 32)], h_s)
    wait_send(fp.at[:, pl.ds(0, 3)], f_s)


def layer(*operands):
    vmem = pl.BlockSpec(memory_space=pltpu.VMEM)
    hbm = pl.BlockSpec(memory_space=pltpu.HBM)
    dma = pltpu.SemaphoreType.DMA
    scratch = [
        pltpu.VMEM((D,), BF),
        pltpu.VMEM((3, FFD), BF),
        pltpu.VMEM((320, TOK), BF),
        pltpu.VMEM((TOK, 512), BF),
        pltpu.VMEM((64, TOK), BF),
        pltpu.VMEM((512, 384), BF),
        pltpu.VMEM((32, TOK), F32),
        pltpu.VMEM((NZ, 2, TOK, 512), BF),
        pltpu.VMEM((NY, TOK, 384), BF),
        pltpu.VMEM((NZ, NY, 2, 48, FFD), BF),
        pltpu.VMEM((NZ, NY, 2, 16, FFD), BF),
        pltpu.VMEM((NZ, NY, 2, 16, FFD), BF),
        pltpu.VMEM((NZ, NY, 2, 16, FFD), BF),
        pltpu.VMEM((768, D), BF),
        pltpu.VMEM((ROWS, D), BF),
        pltpu.VMEM((2, NZ, 512, 256), F32),
        pltpu.VMEM((2, 256, 2048), BF),
        pltpu.VMEM((2, 512, 128), F32),
        pltpu.VMEM((2, 512, 128), F32),
        pltpu.VMEM((512, 256), F32),
        pltpu.VMEM((512, 128), F32),
        pltpu.VMEM((NY, TOK, 256), BF),
        pltpu.VMEM((NY, TOK, 256), BF),
        pltpu.VMEM((NX, ROWS, 256), BF),
        pltpu.VMEM((NX, 192, 128), BF),
        pltpu.VMEM((ROWS, D), BF),
        pltpu.VMEM((NZ, ROWS, 256), BF),
        pltpu.VMEM((ROWS, FFD), F32),
        pltpu.VMEM((TOK, FFD), F32),
        pltpu.VMEM((ROWS, FFD), BF),
        pltpu.VMEM((TOK, FFD), BF),
        pltpu.VMEM((TOK, FFD), BF),
        pltpu.VMEM((NZ, NX, 32, 256), BF),
        pltpu.VMEM((NZ, NX, 32, 256), BF),
        dma, dma((2, 4, 4)), dma, dma((2, 2)), dma, dma((8,)), dma, dma((3,)), dma, dma((3,)),
        dma, dma((2, 4)), dma, dma((2,)), dma, dma((NZ, 3)), dma((14,)),
    ]
    scratch += 2 * [dma, dma((2, 4)), dma, dma((2, 2, 8)), dma, dma((8,))]
    scratch += 2 * [dma, dma((2, 4, 4)), dma, dma((2, 2)), dma, dma((8,))]
    return pl.pallas_call(
        kernel,
        out_shape=pltpu.VMEM((32, D), BF),
        in_specs=[hbm] * 12,
        out_specs=vmem,
        scratch_shapes=scratch,
        compiler_params=pltpu.CompilerParams(collective_id=0, has_side_effects=True),
    )(*operands)


def body(
    queries, latents, shared_key, expand_weight, residual, out_weight,
    norm_gain, gate_weight, value_weight, conv_weight, down_weight,
):
    frequency = (10000.0 ** (-np.arange(ROPE // 2) / (ROPE // 2))).astype(np.float32)
    return layer(
        norm_gain, conv_weight, queries.T, latents, shared_key.T, expand_weight, gate_weight, value_weight,
        down_weight.T, np.ascontiguousarray(np.broadcast_to(frequency[:, None], (ROPE // 2, TOK))),
        residual, out_weight,
    )


def solution(mesh):
    split = Mesh(mesh.devices.reshape(NZ, NY, 2, mesh.shape["tp"]), ("sp_0", "sp_1", "sp_2", "tp"))
    placed = (
        P(SP, "tp"),
        P(SP, None),
        P(SP, None),
        P(None, "tp"),
        P(SP, None),
        P(),
        P(),
        P(SP, "tp"),
        P(SP, "tp"),
        P(None, "tp"),
        P("tp", SP),
    )
    return jax.shard_map(
        body, mesh=split, in_specs=placed, out_specs=P(SP_TP, None), check_vma=False
    )
```

```python
import functools

import jax
import jax.numpy as jnp
import numpy as np
from jax import lax
from jax.experimental import pallas as pl
from jax.experimental.pallas import tpu as pltpu
from jax.sharding import Mesh
from jax.sharding import PartitionSpec as P

NOPE_A = 128
VAL_A = 128
NOPE_B = 64
VAL_B = 64
ROPE = 64
SP = ("sp_0", "sp_1", "sp_2")
SP_TP = ("sp_0", "sp_1", "sp_2", "tp")
NZ, NY, NX = 8, 4, 4
TOK = 128
ROWS = TOK + 32
D = 2048
FFD = 768
MESH = pl.DeviceIdType.MESH
LOG2E = 1.4426950408889634
F32 = jnp.float32
BF = jnp.bfloat16


def split3(v):
    hi = v.astype(BF).astype(F32)
    rest = v - hi
    mid = rest.astype(BF).astype(F32)
    return hi, mid, rest - mid


def kernel(
    gain_hbm, conv_hbm, q_hbm, lat_hbm, key_hbm, ew_hbm, gate_hbm, value_hbm, dn_hbm, freq_hbm, resid_hbm, ow_hbm,
    out_ref,
    gain, conv_w, q_t, lat, key_t, ew, freq, kvb, qb, gb, va, da, db, ow, resid, s_ref, p_ref, macc, mrow, accw, accn,
    part, ob, att, stream, normed, gacc, vacc, gate, value, act, fp, fr,
    kvz_s, kvz_r, q_s, q_r, pk_s, pk_r, o_s, o_r, x_s, x_r, e_s, e_r, h_s, h_r, f_s, f_r, loc, *ring_sems,
):
    z = lax.axis_index("sp_0")
    y = lax.axis_index("sp_1")
    c = lax.axis_index("sp_2")
    x = lax.axis_index("tp")
    other = 1 - c

    def zat(k):
        return lax.rem(z + (k + NZ), NZ)

    def yat(k):
        return lax.rem(y + (k + NY), NY)

    def xat(k):
        return lax.rem(x + (k + NX), NX)

    right_z, left_z = {"sp_0": zat(1)}, {"sp_0": zat(-1)}
    right_y, left_y = {"sp_1": yat(1)}, {"sp_1": yat(-1)}
    partner = {"sp_2": other}
    place = (z * NY + y) * 2 + c
    after = lax.rem(place + 1, 64)
    before = lax.rem(place + 63, 64)

    def device_of(i):
        return {"sp_0": i // 8, "sp_1": lax.rem(i // 2, 4), "sp_2": lax.rem(i, 2)}

    def send(src, dst, ssem, rsem, dev):
        pltpu.make_async_remote_copy(
            src_ref=src, dst_ref=dst, send_sem=ssem, recv_sem=rsem, device_id=dev, device_id_type=MESH
        ).start()

    def wait_recv(ref, sem):
        pltpu.make_async_remote_copy(
            src_ref=ref, dst_ref=ref, send_sem=sem, recv_sem=sem, device_id=partner, device_id_type=MESH
        ).wait_recv()

    def wait_send(ref, sem):
        pltpu.make_async_remote_copy(
            src_ref=ref, dst_ref=ref, send_sem=sem, recv_sem=sem, device_id=partner, device_id_type=MESH
        ).wait_send()

    barrier = pltpu.get_barrier_semaphore()
    greeted = [
        partner, right_z, left_z, right_y, left_y, {"sp_1": yat(2)},
        {"tp": xat(1)}, {"tp": xat(2)}, {"tp": xat(3)},
    ]
    greeted += [device_of(i) | {"tp": xat(o)} for i in (after, before) for o in range(NX)]
    for dev in greeted:
        pl.semaphore_signal(barrier, inc=1, device_id=dev, device_id_type=MESH)

    def load(src, dst, i):
        copy = pltpu.make_async_copy(src, dst, loc.at[i])
        copy.start()
        return copy

    first_loads = [
        load(lat_hbm, lat, 0), load(ew_hbm, ew, 1), load(key_hbm, key_t, 2), load(freq_hbm, freq, 3),
        load(q_hbm, q_t, 4),
    ]
    weight_loads = [
        load(gate_hbm, gb.at[z, y, c, pl.ds(0, 32)], 5),
        load(value_hbm.at[pl.ds(0, 16)], gb.at[z, y, c, pl.ds(32, 16)], 6),
        load(value_hbm.at[pl.ds(16, 16)], va.at[z, y, c], 7),
        load(dn_hbm.at[pl.ds(0, 16)], da.at[z, y, c], 12), load(dn_hbm.at[pl.ds(16, 16)], db.at[z, y, c], 13),
    ]
    load_res = load(resid_hbm, resid.at[pl.ds(0, TOK)], 8)
    load_ow = load(ow_hbm, ow, 9)
    load_gain = load(gain_hbm, gain, 10)
    load_conv = load(conv_hbm, conv_w, 11)
    for copy in first_loads:
        copy.wait()

    position = (lax.broadcasted_iota(jnp.int32, (32, TOK), 1) + place * TOK).astype(F32)
    angles = position * freq[...]
    cosine, sine = jnp.cos(angles), jnp.sin(angles)

    def turned(a, b):
        a, b = a.astype(F32), b.astype(F32)
        return [a * cosine - b * sine, b * cosine + a * sine]

    def upright(pieces):
        return jnp.transpose(jnp.concatenate(pieces, axis=0), (1, 0))

    nothing = jnp.zeros((64, TOK), F32)
    expanded = jnp.dot(lat[...], ew[...], preferred_element_type=F32)
    key_rows = upright(turned(key_t[0:32, :], key_t[32:64, :]) + [nothing])
    low_lane = lax.broadcasted_iota(jnp.int32, (TOK, 128), 1) < 64
    swapped = pltpu.roll(expanded[:, 256:384], 64, 1)
    kvb[0, 0, :, 0:128] = expanded[:, 0:128].astype(BF)
    kvb[0, 0, :, 128:256] = jnp.where(low_lane, key_rows, swapped).astype(BF)
    kvb[0, 0, :, 256:384] = expanded[:, 128:256].astype(BF)
    kvb[0, 0, :, 384:512] = jnp.where(low_lane, swapped, 1.0).astype(BF)
    qb[3, :, 0:128] = upright([q_t[0:128, :].astype(F32)]).astype(BF)
    qb[3, :, 128:256] = upright(turned(q_t[192:224, :], q_t[224:256, :]) + [nothing]).astype(BF)
    qb[3, :, 256:384] = upright(
        turned(q_t[256:288, :], q_t[288:320, :]) + [q_t[128:192, :].astype(F32)]
    ).astype(BF)

    macc[...] = jnp.full((2, 512, 128), -3e38, F32)
    pl.semaphore_wait(barrier, len(greeted))

    def rows_of(slot, h):
        return kvb.at[slot, 0, pl.ds(32 * h, 32)]

    def slot_of(s, ahead):
        return 0 if s == 0 else 7 if s == 4 else 2 * s - 1 + ahead

    def kv_out(s, h):
        if s < 3 or h < 2:
            send(rows_of(slot_of(s, 0), h), rows_of(slot_of(s + 1, 0), h), kvz_s, kvz_r.at[0, s, h], right_z)
        if s < 3 or h >= 2:
            send(rows_of(slot_of(s, 1), h), rows_of(slot_of(s + 1, 1), h), kvz_s, kvz_r.at[1, s, h], left_z)

    def kv_across(slot):
        send(kvb.at[slot, 0], kvb.at[slot, 1], pk_s, pk_r.at[slot], partner)

    def kvz(s, h):
        if s < 4:
            wait_recv(rows_of(slot_of(s, 0), h), kvz_r.at[0, s - 1, h])
            wait_recv(rows_of(slot_of(s, 1), h), kvz_r.at[1, s - 1, h])
            kv_out(s, h)
            if h == 3:
                kv_across(2 * s - 1)
                kv_across(2 * s)
        else:
            for q in range(4):
                wait_recv(rows_of(7, q), kvz_r.at[q // 2, 3, q])
            kv_across(7)

    def q_relay(s):
        if s == 1:
            wait_recv(qb.at[1], q_r.at[0, 0])
            send(qb.at[1, pl.ds(0, 64)], qb.at[0, pl.ds(0, 64)], q_s, q_r.at[0, 1], right_y)
            wait_recv(qb.at[2], q_r.at[1, 0])
            send(qb.at[2, pl.ds(64, 64)], qb.at[0, pl.ds(64, 64)], q_s, q_r.at[1, 1], left_y)
        else:
            wait_recv(qb.at[0, pl.ds(0, 64)], q_r.at[0, 1])
            wait_recv(qb.at[0, pl.ds(64, 64)], q_r.at[1, 1])

    for q in range(4):
        kv_out(0, q)
    send(qb.at[3], qb.at[1], q_s, q_r.at[0, 0], right_y)
    send(qb.at[3], qb.at[2], q_s, q_r.at[1, 0], left_y)
    kv_across(0)

    for copy in weight_loads:
        copy.wait()

    offsets = [0, -1, 1, -2, 2, -3, 3, 4]

    def z_then_y(buf, z_s, z_r, y_s, y_r, p_s, p_r):
        def half(zz, yy, h):
            return buf.at[zz, yy, c, :, pl.ds(384 * h, 384)]

        def out(zz, j):
            block = buf.at[zz, y, c]
            send(block, block, y_s, y_r.at[0, 0, j], right_y)
            send(block, block, y_s, y_r.at[1, 0, j], left_y)
            send(block, block, p_s, p_r.at[j], partner)

        def on_z(s):
            lo, hi = zat(-s), zat(s)
            if s == 4:
                wait_recv(half(lo, y, 0), z_r.at[0, 3])
                wait_recv(half(lo, y, 1), z_r.at[1, 3])
                out(lo, 7)
                return
            for way, (zz, dev) in enumerate(((lo, right_z), (hi, left_z))):
                block = buf.at[zz, y, c]
                if s > 0:
                    wait_recv(block, z_r.at[way, s - 1])
                src = block if s < 3 else half(zz, y, way)
                send(src, src, z_s, z_r.at[way, s], dev)
            if s > 0:
                out(lo, 2 * s - 1)
                out(hi, 2 * s)

        def on_y(s, j):
            zz = zat(offsets[j])
            a, b, far = yat(-1), yat(1), yat(2)
            if s == 0:
                out(z, 0)
            elif s == 1:
                for way, (yy, dev) in enumerate(((a, right_y), (b, left_y))):
                    wait_recv(buf.at[zz, yy, c], y_r.at[way, 0, j])
                    src = half(zz, yy, way)
                    send(src, src, y_s, y_r.at[way, 1, j], dev)
                for yy in (a, b):
                    send(buf.at[zz, yy, c], buf.at[zz, yy, c], p_s, p_r.at[j], partner)
            else:
                wait_recv(half(zz, far, 0), y_r.at[0, 1, j])
                wait_recv(half(zz, far, 1), y_r.at[1, 1, j])
                send(buf.at[zz, far, c], buf.at[zz, far, c], p_s, p_r.at[j], partner)

        return on_z, on_y

    def y_then_z(buf, z_s, z_r, y_s, y_r, p_s, p_r):
        def half(zz, yy, h):
            return buf.at[zz, yy, c, :, pl.ds(384 * h, 384)]

        def on_y(s):
            a, b, far = yat(-1), yat(1), yat(2)
            if s == 2:
                wait_recv(half(z, far, 0), y_r.at[0, 1])
                wait_recv(half(z, far, 1), y_r.at[1, 1])
                return
            for way, (yy, dev) in enumerate(((a, right_y), (b, left_y))):
                if s == 0:
                    src = buf.at[z, y, c]
                else:
                    wait_recv(buf.at[z, yy, c], y_r.at[way, 0])
                    src = half(z, yy, way)
                send(src, src, y_s, y_r.at[way, s], dev)

        def on_z(s, r):
            yy = yat((0, -1, 1, 2)[r])
            lo, hi = zat(-s), zat(s)
            if s == 4:
                wait_recv(half(lo, yy, 0), z_r.at[0, 3, r])
                wait_recv(half(lo, yy, 1), z_r.at[1, 3, r])
            else:
                for way, (zz, dev) in enumerate(((lo, right_z), (hi, left_z))):
                    block = buf.at[zz, yy, c]
                    if s > 0:
                        wait_recv(block, z_r.at[way, s - 1, r])
                    src = block if s < 3 else half(zz, yy, way)
                    send(src, src, z_s, z_r.at[way, s, r], dev)
            for ahead, zz in enumerate((lo, hi) if 0 < s < 4 else (lo,)):
                send(buf.at[zz, yy, c], buf.at[zz, yy, c], p_s, p_r.at[slot_of(s, ahead)], partner)

        return on_y, on_z

    gb_z, gb_y = z_then_y(gb, *ring_sems[0:6])
    db_z, db_y = z_then_y(db, *ring_sems[6:12])
    va_y, va_z = y_then_z(va, *ring_sems[12:18])
    da_y, da_z = y_then_z(da, *ring_sems[18:24])

    heads = (
        (0, 256, 0, 256, 256, 512, (NOPE_A + ROPE) ** (-0.5) * LOG2E, accw),
        (256, 384, 128, 256, 384, 512, (NOPE_B + ROPE) ** (-0.5) * LOG2E, accn),
    )

    def scores(j):
        wait_recv(kvb.at[j, 1], pk_r.at[j])
        for head in range(2):
            q0, q1, k0, k1 = heads[head][:4]
            qs = qb[:, :, q0:q1].reshape(512, q1 - q0)
            ks = kvb[j, :, :, k0:k1].reshape(256, k1 - k0)
            s = lax.dot_general(qs, ks, (((1,), (1,)), ((), ())), preferred_element_type=F32)
            s_ref[head, j] = s
            macc[head] = jnp.maximum(macc[head], jnp.maximum(s[:, :128], s[:, 128:]))

    def weights(half, head, j0, j1):
        rows = slice(256 * half, 256 * half + 256)
        v0, v1, factor, acc = heads[head][4:]
        m = jnp.broadcast_to(jnp.max(macc[head, rows], axis=1, keepdims=True), (256, 128))
        for j in range(j0, j1):
            for side in range(2):
                s = s_ref[head, j, rows, side * 128 : side * 128 + 128]
                at = j * 256 + side * 128
                p_ref[head, :, at : at + 128] = jnp.exp2((s - m) * factor).astype(BF)
        vs = kvb[j0:j1, :, :, v0:v1].reshape(256 * (j1 - j0), v1 - v0)
        return m, jnp.dot(p_ref[head, :, j0 * 256 : j1 * 256], vs, preferred_element_type=F32)

    def weigh_early(half):
        rows = slice(256 * half, 256 * half + 256)
        for head in range(2):
            m, product = weights(half, head, 0, 5)
            mrow[head, rows] = m
            heads[head][7][rows] = product

    def weigh(half):
        rows = slice(256 * half, 256 * half + 256)
        for head in range(2):
            m, product = weights(half, head, 5, 8)
            factor, acc = heads[head][6:]
            shrink = jnp.exp2((mrow[head, rows] - m) * factor)
            shrink = jnp.concatenate([shrink] * (acc.shape[1] // 128), axis=1)
            mrow[head, rows] = m
            acc[rows] = acc[rows] * shrink + product

    lane = lax.broadcasted_iota(jnp.int32, (TOK, 128), 1)

    def pack(half):
        for b in (2 * half, 2 * half + 1):
            rows = slice(b * TOK, b * TOK + TOK)
            wide, narrow = accw[rows, :], accn[rows, :]
            tile = narrow
            stats = (
                mrow[0, rows, :], mrow[1, rows, :],
                jnp.broadcast_to(wide[:, 192:193], (TOK, 128)), jnp.broadcast_to(narrow[:, 64:65], (TOK, 128)),
            )
            at = 64
            for stat in stats:
                for piece in split3(stat):
                    tile = jnp.where(lane == at, piece, tile)
                    at += 1
            tile = jnp.where(lane >= at, 0.0, tile)
            part[b, :, 0:128] = wide[:, 0:128].astype(BF)
            part[b, :, 128:256] = tile.astype(BF)
        if half == 0:
            send(part.at[0], ob.at[0], o_s, o_r.at[0], {"sp_1": yat(2)})
            send(part.at[1], ob.at[2], o_s, o_r.at[2], left_y)
        else:
            send(part.at[2], ob.at[1], o_s, o_r.at[1], right_y)

    def merge():
        blocks = [part.at[3]] + [ob.at[g] for g in range(3)]
        tiles = [block[:, 128:256].astype(F32) for block in blocks]
        stats = [s + pltpu.roll(s, 127, 1) + pltpu.roll(s, 126, 1) for s in tiles]
        top = jnp.maximum(jnp.maximum(stats[0], stats[1]), jnp.maximum(stats[2], stats[3]))
        factor = jnp.where(lane == 64, heads[0][6], heads[1][6])
        shares = [jnp.exp2((s - top) * factor) for s in stats]
        total = sum(pltpu.roll(w, 6, 1) * s for w, s in zip(shares, stats))
        inverse = pltpu.roll(1.0 / total, 122, 1)
        shares = [w * inverse for w in shares]
        wide = sum(w[:, 64:65] * block[:, 0:128].astype(F32) for w, block in zip(shares, blocks))
        narrow = sum(w[:, 67:68] * s for w, s in zip(shares, tiles))
        att[x, 0:TOK, 0:128] = wide.astype(BF)
        att[x, 0:TOK, 128:256] = narrow.astype(BF)

    def part_in():
        for o in range(3):
            wait_recv(ob.at[o], o_r.at[o])

    def att_out():
        for o in (2, 1, 3):
            mine = att.at[x, pl.ds(0, TOK)]
            send(mine, mine, x_s, x_r.at[o - 1], {"tp": xat(o)})
        for o in range(NX):
            peer = {"tp": xat(o)}
            send(att.at[x, pl.ds(112, 16)], att.at[x, pl.ds(128, 16)], e_s, e_r.at[0, o], device_of(after) | peer)
            send(att.at[x, pl.ds(0, 16)], att.at[x, pl.ds(144, 16)], e_s, e_r.at[1, o], device_of(before) | peer)

    def edges_out():
        load_res.wait()
        send(resid.at[pl.ds(112, 16)], resid.at[pl.ds(128, 16)], h_s, h_r.at[0], device_of(after))
        send(resid.at[pl.ds(0, 16)], resid.at[pl.ds(144, 16)], h_s, h_r.at[1], device_of(before))

    gb_z(0)
    gb_y(0, 0)
    va_y(0)
    kvz(1, 0)
    q_relay(1)
    kvz(1, 1)
    db_y(0, 0)
    kvz(1, 2)
    kvz(1, 3)
    da_y(0)
    edges_out()
    gb_y(1, 0)
    va_y(1)
    gb_z(1)
    kvz(2, 0)
    q_relay(2)
    scores(0)
    scores(1)
    kvz(2, 1)
    db_y(1, 0)
    scores(2)
    kvz(2, 2)
    gb_y(2, 0)
    kvz(2, 3)
    va_y(2)
    gb_z(2)
    scores(3)
    scores(4)
    kvz(3, 0)
    va_z(0, 2)
    weigh_early(0)
    kvz(3, 1)
    db_y(2, 0)
    gb_y(1, 2)
    kvz(3, 2)
    weigh_early(1)
    kvz(3, 3)
    va_z(0, 3)
    va_z(0, 0)
    da_y(1)
    db_z(0)
    da_z(0, 2)
    va_z(0, 1)
    da_z(0, 0)
    gb_z(3)
    scores(5)
    gb_y(1, 4)
    scores(6)
    va_z(1, 2)
    gb_y(2, 2)
    da_y(2)
    da_z(0, 3)
    kvz(4, 0)
    va_z(1, 3)
    va_z(1, 0)
    db_z(1)
    scores(7)
    weigh(0)
    va_z(1, 1)
    pack(0)
    weigh(1)
    pack(1)
    da_z(1, 0)
    gb_y(2, 4)
    gb_z(4)
    gb_y(1, 3)
    da_z(0, 1)
    gb_y(1, 6)
    gb_y(1, 5)
    db_y(1, 1)
    va_z(2, 2)
    db_y(1, 2)
    va_z(2, 3)
    va_z(2, 0)
    db_z(2)
    va_z(2, 1)
    da_z(2, 0)
    part_in()
    merge()
    att_out()
    da_z(1, 1)
    gb_y(1, 1)
    da_z(1, 3)
    da_z(1, 2)
    va_z(3, 2)
    va_z(3, 3)
    gb_y(1, 7)
    va_z(3, 0)
    gb_y(2, 3)
    db_z(3)
    va_z(3, 1)
    gb_y(2, 6)
    da_z(3, 0)
    gb_y(2, 5)
    da_z(2, 1)
    db_y(2, 1)
    db_y(2, 2)
    da_z(2, 3)
    db_y(1, 3)
    da_z(2, 2)
    load_ow.wait()
    load_gain.wait()
    load_conv.wait()
    wait_recv(resid.at[pl.ds(128, 16)], h_r.at[0])
    wait_recv(resid.at[pl.ds(144, 16)], h_r.at[1])
    for o in (2, 1, 3):
        wait_recv(att.at[xat(-o), pl.ds(0, TOK)], x_r.at[o - 1])
    for o in range(NX):
        wait_recv(att.at[xat(-o), pl.ds(128, 16)], e_r.at[0, o])
        wait_recv(att.at[xat(-o), pl.ds(144, 16)], e_r.at[1, o])

    ss = jnp.zeros((ROWS, 1), F32)
    for n in range(8):
        cols = slice(n * 256, n * 256 + 256)
        total = resid[:, cols].astype(F32)
        for h in range(NX):
            total = total + jnp.dot(att[h, :, 0:192], ow[h * 192 : h * 192 + 192, cols], preferred_element_type=F32)
        rounded = total.astype(BF)
        stream[:, cols] = rounded
        wide = rounded.astype(F32)
        ss = ss + jnp.sum(wide * wide, axis=1, keepdims=True)
    scale = lax.rsqrt(ss * (1.0 / D) + 1e-06)
    for n in range(8):
        cols = slice(n * 256, n * 256 + 256)
        scaled = stream[:, cols].astype(F32) * scale
        normed[n] = (scaled * gain[cols].astype(F32).reshape(1, 256)).astype(BF)
    db_y(1, 4)
    db_z(4)
    va_z(4, 2)
    va_z(4, 0)
    va_z(4, 3)
    va_z(4, 1)
    gb_y(2, 1)
    gb_y(2, 7)

    def gate_rows(zz, cols):
        return gb[zz, :, :, 0:32, cols].reshape(256, 256)

    def value_rows(zz, cols):
        return jnp.concatenate([gb[zz, :, :, 32:48, cols], va[zz, :, :, :, cols]], axis=2).reshape(256, 256)

    def up(weights, rows, js, n):
        total = None
        for j in js:
            zz = zat(offsets[j])
            w = weights(zz, slice(n * 256, n * 256 + 256))
            term = jnp.dot(normed[zz, 0:rows], w, preferred_element_type=F32)
            total = term if total is None else total + term
        return total

    def arrived(buf, sems, j):
        wait_recv(buf.at[zat(offsets[j]), :, other], sems.at[j])

    for j in range(7):
        arrived(gb, ring_sems[5], j)
    for n in range(3):
        gacc[:, n * 256 : n * 256 + 256] = up(gate_rows, ROWS, range(7), n)
    da_z(3, 1)
    db_y(1, 5)
    for j in range(7):
        arrived(va, ring_sems[17], j)
    for n in range(3):
        vacc[:, n * 256 : n * 256 + 256] = up(value_rows, TOK, range(7), n)
    da_z(3, 3)
    db_y(1, 6)
    da_z(3, 2)
    arrived(gb, ring_sems[5], 7)
    arrived(va, ring_sems[17], 7)
    for n in range(3):
        cols = slice(n * 256, n * 256 + 256)
        gate[:, cols] = (gacc[:, cols] + up(gate_rows, ROWS, (7,), n)).astype(BF)
        value[:, cols] = (vacc[:, cols] + up(value_rows, TOK, (7,), n)).astype(BF)

    row = lax.broadcasted_iota(jnp.int32, (TOK, 256), 0)
    for n in range(3):
        cols = slice(n * 256, n * 256 + 256)
        g = gate[0:TOK, cols].astype(F32)
        edge = gate[TOK:ROWS, cols].astype(F32)
        first = jnp.where(place > 0, edge[15:16], 0.0)
        last = jnp.where(place < 63, edge[16:17], 0.0)
        low = jnp.where(row == 0, first, pltpu.roll(g, 1, 0))
        high = jnp.where(row == TOK - 1, last, pltpu.roll(g, TOK - 1, 0))
        cw = conv_w[:, cols].astype(F32)
        mixed = low * cw[0:1] + g * cw[1:2] + high * cw[2:3]
        silu = mixed / (1.0 + jnp.exp(-mixed))
        act[:, cols] = (silu * value[:, cols].astype(F32)).astype(BF)

    for j in range(NZ):
        zz = zat(offsets[j])
        arrived(da, ring_sems[23], j)
        arrived(db, ring_sems[11], j)
        w = jnp.concatenate([da[zz], db[zz]], axis=2).reshape(256, FFD)
        d = lax.dot_general(act[...], w, (((1,), (1,)), ((), ())), preferred_element_type=F32)
        fp[j] = d.astype(BF).reshape(NX, 32, 256)
        for o in (2, 1, 3):
            peer = xat(o)
            send(fp.at[j, peer], fr.at[j, x], f_s, f_r.at[j, o - 1], {"tp": peer})
        if j == 0:
            db_y(1, 7)
            db_y(2, 3)
        if j == 1:
            da_z(4, 0)
            db_y(2, 4)
        if j == 2:
            db_y(2, 5)
            da_z(4, 1)
        if j == 3:
            db_y(2, 6)
            da_z(4, 3)
        if j == 4:
            da_z(4, 2)
        if j == 6:
            db_y(2, 7)

    rows = pl.ds(pl.multiple_of(x * 32, 32), 32)
    for j in range(NZ):
        cols = pl.ds(pl.multiple_of(zat(offsets[j]) * 256, 256), 256)
        total = stream[rows, cols].astype(F32) + fp[j, x].astype(F32)
        for o in (1, 3, 2):
            wait_recv(fr.at[j, xat(-o)], f_r.at[j, o - 1])
            total = total + fr[j, xat(-o)].astype(F32)
        out_ref[:, cols] = total.astype(BF)

    wait_send(kvb.at[pl.ds(0, 7), 0], kvz_s)
    wait_send(qb.at[pl.ds(0, 3)], q_s)
    wait_send(kvb.at[:, 0], pk_s)
    for buf, (z_s, _, y_s, _, p_s, _) in ((gb, ring_sems[0:6]), (db, ring_sems[6:12])):
        wait_send(buf.at[pl.ds(0, 7), 0, 0], z_s)
        wait_send(buf.at[:, pl.ds(0, 3), 0], y_s)
        wait_send(buf.at[:, :, 0], p_s)
    for buf, (z_s, _, y_s, _, p_s, _) in ((va, ring_sems[12:18]), (da, ring_sems[18:24])):
        wait_send(buf.at[pl.ds(0, 7), :, 0], z_s)
        wait_send(buf.at[0, pl.ds(0, 3), 0], y_s)
        wait_send(buf.at[:, :, 0], p_s)
    wait_send(part.at[pl.ds(0, 3)], o_s)
    wait_send(att.at[pl.ds(0, 3), pl.ds(0, TOK)], x_s)
    wait_send(att.at[:, pl.ds(0, 32)], e_s)
    wait_send(resid.at[pl.ds(0, 32)], h_s)
    wait_send(fp.at[:, pl.ds(0, 3)], f_s)


def layer(*operands):
    vmem = pl.BlockSpec(memory_space=pltpu.VMEM)
    hbm = pl.BlockSpec(memory_space=pltpu.HBM)
    dma = pltpu.SemaphoreType.DMA
    scratch = [
        pltpu.VMEM((D,), BF),
        pltpu.VMEM((3, FFD), BF),
        pltpu.VMEM((320, TOK), BF),
        pltpu.VMEM((TOK, 512), BF),
        pltpu.VMEM((64, TOK), BF),
        pltpu.VMEM((512, 384), BF),
        pltpu.VMEM((32, TOK), F32),
        pltpu.VMEM((NZ, 2, TOK, 512), BF),
        pltpu.VMEM((NY, TOK, 384), BF),
        pltpu.VMEM((NZ, NY, 2, 48, FFD), BF),
        pltpu.VMEM((NZ, NY, 2, 16, FFD), BF),
        pltpu.VMEM((NZ, NY, 2, 16, FFD), BF),
        pltpu.VMEM((NZ, NY, 2, 16, FFD), BF),
        pltpu.VMEM((768, D), BF),
        pltpu.VMEM((ROWS, D), BF),
        pltpu.VMEM((2, NZ, 512, 256), F32),
        pltpu.VMEM((2, 256, 2048), BF),
        pltpu.VMEM((2, 512, 128), F32),
        pltpu.VMEM((2, 512, 128), F32),
        pltpu.VMEM((512, 256), F32),
        pltpu.VMEM((512, 128), F32),
        pltpu.VMEM((NY, TOK, 256), BF),
        pltpu.VMEM((NY, TOK, 256), BF),
        pltpu.VMEM((NX, ROWS, 256), BF),
        pltpu.VMEM((ROWS, D), BF),
        pltpu.VMEM((NZ, ROWS, 256), BF),
        pltpu.VMEM((ROWS, FFD), F32),
        pltpu.VMEM((TOK, FFD), F32),
        pltpu.VMEM((ROWS, FFD), BF),
        pltpu.VMEM((TOK, FFD), BF),
        pltpu.VMEM((TOK, FFD), BF),
        pltpu.VMEM((NZ, NX, 32, 256), BF),
        pltpu.VMEM((NZ, NX, 32, 256), BF),
        dma, dma((2, 4, 4)), dma, dma((2, 2)), dma, dma((8,)), dma, dma((3,)), dma, dma((3,)),
        dma, dma((2, 4)), dma, dma((2,)), dma, dma((NZ, 3)), dma((14,)),
    ]
    scratch += 2 * [dma, dma((2, 4)), dma, dma((2, 2, 8)), dma, dma((8,))]
    scratch += 2 * [dma, dma((2, 4, 4)), dma, dma((2, 2)), dma, dma((8,))]
    return pl.pallas_call(
        kernel,
        out_shape=pltpu.VMEM((32, D), BF),
        in_specs=[hbm] * 12,
        out_specs=vmem,
        scratch_shapes=scratch,
        compiler_params=pltpu.CompilerParams(collective_id=0, has_side_effects=True),
    )(*operands)


def body(
    queries, latents, shared_key, expand_weight, residual, out_weight,
    norm_gain, gate_weight, value_weight, conv_weight, down_weight,
):
    frequency = (10000.0 ** (-np.arange(ROPE // 2) / (ROPE // 2))).astype(np.float32)
    return layer(
        norm_gain, conv_weight, queries.T, latents, shared_key.T, expand_weight, gate_weight, value_weight,
        down_weight.T, np.ascontiguousarray(np.broadcast_to(frequency[:, None], (ROPE // 2, TOK))),
        residual, out_weight,
    )


def solution(mesh):
    split = Mesh(mesh.devices.reshape(NZ, NY, 2, mesh.shape["tp"]), ("sp_0", "sp_1", "sp_2", "tp"))
    placed = (
        P(SP, "tp"),
        P(SP, None),
        P(SP, None),
        P(None, "tp"),
        P(SP, None),
        P(),
        P(),
        P(SP, "tp"),
        P(SP, "tp"),
        P(None, "tp"),
        P("tp", SP),
    )
    return jax.shard_map(
        body, mesh=split, in_specs=placed, out_specs=P(SP_TP, None), check_vma=False
    )
```
